128 devices in a mesh: sp: 16 (over z, x), tp: 8 (over y, core).
Axes of the slice: x: 4, y: 4, z: 4, core: 2. Of those that a mesh axis runs over, the one named last changes fastest.
Arguments:
- query_small: bfloat16 [12288, 1024], P('sp', 'tp'), may hold values from -6 to 6
- key_small: bfloat16 [12288, 1024], P('sp', 'tp'), may hold values from -6 to 6
- value_small: bfloat16 [12288, 1024], P('sp', 'tp'), may hold values from -6 to 6
- gates_small: float32 [12288, 16], P('sp', 'tp'), as said below
- query_large: bfloat16 [12288, 1024], P('sp', 'tp'), may hold values from -6 to 6
- key_large: bfloat16 [12288, 1024], P('sp', 'tp'), may hold values from -6 to 6
- value_large: bfloat16 [12288, 1024], P('sp', 'tp'), may hold values from -6 to 6
- gates_large: float32 [12288, 8], P('sp', 'tp'), as said below
- residual: bfloat16 [12288, 2048], P(('sp', 'tp')), may hold values from -6 to 6
- mixer_small: bfloat16 [1024, 2048], P('tp'), may hold values from -1 to 1
- mixer_large: bfloat16 [1024, 2048], P('tp'), may hold values from -1 to 1
- mix_gain: float32 [2048], replicated, may hold values from 0.1 to 1.9
- value_weight: bfloat16 [2048, 5632], P('sp', 'tp'), may hold values from -0.125 to 0.125
- gate_weight: bfloat16 [2048, 5632], P('sp', 'tp'), may hold values from -0.125 to 0.125
- value_taps: float32 [3, 5632], P(None, 'tp'), may hold values from -3 to 3
- gate_taps: float32 [3, 5632], P(None, 'tp'), may hold values from -3 to 3
- down_weight: bfloat16 [5632, 2048], P('tp', 'sp'), may hold values from -0.078125 to 0.078125
- final_gain: float32 [2048], replicated, may hold values from 0.1 to 1.9
Outputs:
- layer_out: bfloat16 [12288, 2048], P(('sp', 'tp'))
The draws below stay inside these ranges and needn't reach their ends.
Inputs may be any that keep to these rules, and one draw needn't show every extreme that they name: `gates_small`: each column never rises from one position to the next, and its first entry is negative. `gates_large`: each column never rises from one position to the next, and its first entry is negative.
All inputs are finite; a program needn't handle non-finite values.
Results may differ from the reference program's by a relative error of at most 0.018.
Values may be sent and summed in bfloat16 or wider, within the bound.
No kernel may reach another device: no remote copies, remote signals or barrier semaphores. Data moves between devices by JAX's collectives and lax.ppermute only.
A program may use at most 128 MiB of HBM per device.

```python
import math
import jax
import jax.numpy as jnp
from jax import lax

D = 2048
FF = 5632
HS = 16
DS = 64
HL = 8
DL = 128
TOK_DEV = 768
SEQUENCE_TOKENS = 12288


def plant_pair(key, head_group, head_dim, salt):
    base_level = jax.random.fold_in(key, salt)
    width = head_group * head_dim
    queries = jnp.clip(jax.random.normal(jax.random.fold_in(base_level, 1), (SEQUENCE_TOKENS, width), jnp.float32), -6.0, 6.0)
    key_rows = jnp.clip(jax.random.normal(jax.random.fold_in(base_level, 2), (SEQUENCE_TOKENS, width), jnp.float32), -6.0, 6.0)
    return (queries, key_rows)


def gate_totals(key, head_group, salt):
    base_level = jax.random.fold_in(key, salt)
    share_fast = 0.5
    rapid_decay = jax.random.uniform(jax.random.fold_in(base_level, 1), (head_group,), jnp.float32) < share_fast
    rate = jnp.where(rapid_decay, 1.0 / 40.0, 0.5 / SEQUENCE_TOKENS)
    block_count = SEQUENCE_TOKENS // TOK_DEV
    factor = jnp.exp(jax.random.uniform(jax.random.fold_in(base_level, 2), (block_count, head_group), jnp.float32, -0.7, 0.7))
    factor = jnp.repeat(factor, TOK_DEV, axis=0)
    jitter = jax.random.uniform(jax.random.fold_in(base_level, 3), (SEQUENCE_TOKENS, head_group), jnp.float32, 0.3, 1.7)
    forget_decrements = rate[None, :] * factor * jitter
    spike_locations = jax.random.randint(jax.random.fold_in(base_level, 4), (3, head_group), 0, SEQUENCE_TOKENS)
    spike_magnitudes = jax.random.uniform(jax.random.fold_in(base_level, 5), (3, head_group), jnp.float32, 0.22, 0.69)
    token_positions = jnp.arange(SEQUENCE_TOKENS)
    match_events = jnp.where(token_positions[:, None, None] == spike_locations[None, :, :], spike_magnitudes[None, :, :], 0.0)
    spike_events = jnp.sum(match_events, axis=1) * jnp.where(rapid_decay, 0.0, 1.0)[None, :]
    return jnp.cumsum(-(forget_decrements + spike_events), axis=0)


def draw_query_small(key, part):
    return plant_pair(key, HS, DS, 11)[0].astype(jnp.bfloat16)


def draw_key_small(key, part):
    return plant_pair(key, HS, DS, 11)[1].astype(jnp.bfloat16)


def draw_query_large(key, part):
    return plant_pair(key, HL, DL, 23)[0].astype(jnp.bfloat16)


def draw_key_large(key, part):
    return plant_pair(key, HL, DL, 23)[1].astype(jnp.bfloat16)


def draw_gates_small(key, part):
    return gate_totals(key, HS, 37)


def draw_gates_large(key, part):
    return gate_totals(key, HL, 41)


def shard_levels(own_key, extent, pieces, low, largest):
    factor_of = 1.0
    for position, shards_of in pieces:
        heights = jax.random.uniform(jax.random.fold_in(jax.random.fold_in(own_key, 6), position), (shards_of,), jnp.float32, low / len(pieces), largest / len(pieces))
        factor_of = factor_of * jnp.repeat(jnp.exp(heights), extent[position] // shards_of).reshape((-1,) + (1,) * (len(extent) - 1 - position))
    return factor_of


def gaussian(stream_key, extent, scale, reach, split=(), kind=jnp.bfloat16):
    array = scale * jax.random.normal(stream_key, extent, jnp.float32)
    if split:
        array = array * shard_levels(stream_key, extent, split, -0.22, 0.18)
    return jnp.clip(array, -reach, reach).astype(kind)


def setup_inputs(seed: int = 0) -> dict:
    key_list = jax.random.split(jax.random.key(seed), 19)
    return {
        "query_small": draw_query_small(jax.random.fold_in(key_list[18], 71), 0),
        "key_small": draw_key_small(jax.random.fold_in(key_list[18], 71), 0),
        "value_small": gaussian(key_list[2], (SEQUENCE_TOKENS, HS * DS), 1.0, 6.0, ((0, 16), (1, 8))),
        "gates_small": draw_gates_small(jax.random.fold_in(key_list[18], 71), 0),
        "query_large": draw_query_large(jax.random.fold_in(key_list[18], 71), 0),
        "key_large": draw_key_large(jax.random.fold_in(key_list[18], 71), 0),
        "value_large": gaussian(key_list[6], (SEQUENCE_TOKENS, HL * DL), 1.0, 6.0, ((0, 16), (1, 8))),
        "gates_large": draw_gates_large(jax.random.fold_in(key_list[18], 71), 0),
        "residual": gaussian(key_list[8], (SEQUENCE_TOKENS, D), 1.0, 6.0, ((0, 128),)),
        "mixer_small": gaussian(key_list[9], (HS * DS, D), ((HS * DS + HL * DL) // 64) ** -0.5, 1.0, ((0, 8),)),
        "mixer_large": gaussian(key_list[10], (HL * DL, D), ((HS * DS + HL * DL) // 64) ** -0.5, 1.0, ((0, 8),)),
        "mix_gain": jnp.clip(1.0 + 0.18 * jax.random.normal(key_list[11], (D,), jnp.float32), 0.1, 1.9),
        "value_weight": gaussian(key_list[12], (D, FF), D ** -0.5, 0.125, ((0, 16), (1, 8))),
        "gate_weight": gaussian(key_list[13], (D, FF), D ** -0.5, 0.125, ((0, 16), (1, 8))),
        "value_taps": gaussian(key_list[14], (3, FF), 0.577, 3.0, ((1, 8),), jnp.float32),
        "gate_taps": gaussian(key_list[15], (3, FF), 0.577, 3.0, ((1, 8),), jnp.float32),
        "down_weight": gaussian(key_list[16], (FF, D), FF ** -0.5, 0.078125, ((0, 8), (1, 16))),
        "final_gain": jnp.clip(1.0 + 0.18 * jax.random.normal(key_list[17], (D,), jnp.float32), 0.1, 1.9),
    }


residual_scale = 2.0 ** 0.5
epsilon = 1e-05

def norm_rows(values, gain):
    center = lax.optimization_barrier(jnp.mean(values, axis=-1, keepdims=True))
    spread = lax.optimization_barrier(jnp.mean(jnp.square(values - center), axis=-1, keepdims=True))
    return (values - center) * lax.rsqrt(spread + epsilon) * gain.astype(jnp.float32)

def attend(queries, key_rows, value_rows, gates, head_dim):
    total_rows = queries.shape[0]
    heads_here = gates.shape[1]
    block_rows = math.gcd(total_rows, 256)
    block_count = total_rows // block_rows
    key_heads = key_rows.astype(jnp.float32).reshape(total_rows, heads_here, head_dim)
    value_heads = value_rows.astype(jnp.float32).reshape(total_rows, heads_here, head_dim)
    query_blocks = queries.reshape(block_count, block_rows, heads_here, head_dim)
    gate_blocks = gates.reshape(block_count, block_rows, heads_here)
    key_positions = jnp.arange(total_rows)

    def one_block(inputs):
        query_part, gate_part, first_row = inputs
        scores = jnp.einsum('qhd,khd->hqk', query_part.astype(jnp.float32), key_heads) * head_dim ** (-0.5)
        scores = scores + gate_part.T[:, :, None] - gates.T[:, None, :]
        token_positions = first_row + jnp.arange(block_rows)
        allowed = token_positions[:, None] >= key_positions[None, :]
        scores = jnp.where(allowed[None], scores, -jnp.inf)
        highest = lax.optimization_barrier(jnp.max(scores, axis=-1, keepdims=True))
        weights = jnp.exp(scores - highest)
        weight_sum = lax.optimization_barrier(jnp.sum(weights, axis=-1))
        rounded = lax.optimization_barrier(weights.astype(jnp.bfloat16)).astype(jnp.float32)
        output = jnp.einsum('hqk,khd->qhd', rounded, value_heads) / weight_sum.T[:, :, None]
        return output.astype(jnp.bfloat16)
    firsts = jnp.arange(block_count) * block_rows
    output = lax.map(one_block, (query_blocks, gate_blocks, firsts))
    return output.reshape(total_rows, heads_here * head_dim)

def causal_filter(rows_in, taps):
    values = rows_in.astype(jnp.float32)
    padded = jnp.concatenate([jnp.zeros((2, values.shape[1]), jnp.float32), values], axis=0)
    return taps[0] * padded[:-2] + taps[1] * padded[1:-1] + taps[2] * padded[2:]

def reference(query_small, key_small, value_small, gates_small, query_large, key_large, value_large, gates_large, residual, mixer_small, mixer_large, mix_gain, value_weight, gate_weight, value_taps, gate_taps, down_weight, final_gain):
    small_out = attend(query_small, key_small, value_small, gates_small, DS)
    large_out = attend(query_large, key_large, value_large, gates_large, DL)
    mix = jnp.dot(small_out, mixer_small, preferred_element_type=jnp.float32) + jnp.dot(large_out, mixer_large, preferred_element_type=jnp.float32)
    mixed = norm_rows(residual_scale * residual.astype(jnp.float32) + mix, mix_gain).astype(jnp.bfloat16)
    up_value = jnp.dot(mixed, value_weight, preferred_element_type=jnp.float32).astype(jnp.bfloat16)
    up_gate = jnp.dot(mixed, gate_weight, preferred_element_type=jnp.float32).astype(jnp.bfloat16)
    filt_value = causal_filter(up_value, value_taps)
    filt_gate = causal_filter(up_gate, gate_taps)
    hidden = (jax.nn.silu(filt_gate) * filt_value).astype(jnp.bfloat16)
    ffn = jnp.dot(hidden, down_weight, preferred_element_type=jnp.float32)
    return norm_rows(residual_scale * mixed.astype(jnp.float32) + ffn, final_gain).astype(jnp.bfloat16)
```

```python
import math

import jax
import jax.numpy as jnp
from jax import lax
from jax.experimental import pallas as pl
from jax.experimental.pallas import tpu as pltpu
from jax.sharding import Mesh
from jax.sharding import PartitionSpec as P

DS = 64
DL = 128
TP = ("tp_0", "tp_1")
SP_TP = ("sp", "tp_0", "tp_1")
bf16 = jnp.bfloat16
f32 = jnp.float32


residual_scale = 2.0**0.5
epsilon = 1e-05


def gather_turned(arrays, axis, dims):
    turned = [jnp.moveaxis(a, dim, 0) for a, dim in zip(arrays, dims)]
    widths = [t[0].size for t in turned]
    both = jnp.concatenate([t.reshape(-1, w) for t, w in zip(turned, widths)], axis=1)
    out = lax.all_gather(both, axis, axis=0, tiled=True)
    pieces = jnp.split(out, [sum(widths[:k]) for k in range(1, len(widths))], axis=1)
    return tuple(
        (
            jnp.moveaxis(b.reshape(-1, *t.shape[1:]), 0, dim)
            for b, t, dim in zip(pieces, turned, dims)
        )
    )


def sent_together(arrays, axis, dim, along):
    both = jnp.concatenate(arrays, axis=along)
    out, at, finished = (lax.all_gather(both, axis, axis=dim, tiled=True), 0, [])
    for a in arrays:
        finished.append(lax.slice_in_dim(out, at, at + a.shape[along], axis=along))
        at += a.shape[along]
    return tuple(finished)


def passed_along(value, axis, steps):
    count = lax.axis_size(axis)
    first, last = (max(0, -steps), min(count, count - steps))
    return lax.ppermute(value, axis, [(source, source + steps) for source in range(first, last)])


def norm_rows(values, gain):
    center = jnp.mean(values, axis=-1, keepdims=True)
    spread = jnp.mean(jnp.square(values - center), axis=-1, keepdims=True)
    return (values - center) * lax.rsqrt(spread + epsilon) * gain


def attend(q, kv, gates, rank, heads, base):
    rows = q.shape[0]
    width = q.shape[1]
    d = width // heads
    chunk = 256
    chunks = rows // chunk
    ext = d + 16
    deep = width if heads == 2 else 2 * width
    root = d ** 0.5
    rate = math.log2(math.e) / root
    units = [(h, c) for h in range(heads) for c in range(chunks)]

    def body(rank_ref, q_ref, kv_ref, g_ref, o_ref, qa, ka, va, acc, peak, first):
        me = rank_ref[0]
        lane = lax.broadcasted_iota(jnp.int32, (rows, width), 1)
        for h in range(heads):
            if heads == 2:
                mine = (lane < d) if h == 0 else (lane >= d)
                at = d if h == 0 else 0
                one = ((lane >= at) & (lane < at + 3)).astype(f32)
                qa[h] = jnp.where(mine, q_ref[...].astype(f32), one).astype(bf16)
            else:
                qa[h, :, :width] = q_ref[...]
                qa[h, :, width:] = (lane < 3).astype(f32).astype(bf16)
            va[0, h, d:] = jnp.ones((16, rows), bf16)
            va[1, h, d:] = jnp.ones((16, rows), bf16)
        acc[...] = jnp.zeros(acc.shape, f32)
        peak[...] = jnp.full(peak.shape, -1e30, f32)
        start = g_ref[me][:, 0:1]

        def prepare(j, slot):
            at = pl.multiple_of(j * rows, rows)
            k = kv_ref[pl.ds(at, rows), :width]
            vt = kv_ref[pl.ds(at, rows), width:].T
            bias = jnp.maximum((start - g_ref[j]) * root, -1e30)
            hi = bias.astype(bf16).astype(f32)
            mid = (bias - hi).astype(bf16).astype(f32)
            low = bias - hi - mid
            zero = jnp.zeros((8, rows), f32)
            row = lax.broadcasted_iota(jnp.int32, (8, rows), 0)
            parts = []
            for h in range(heads):
                pick = lambda a: jnp.broadcast_to(a[base + h : base + h + 1], (8, rows))
                parts.append(jnp.where(row == 0, pick(hi), jnp.where(row == 1, pick(mid), jnp.where(row == 2, pick(low), zero))))
            if heads == 2:
                pad = jnp.zeros((d - 8, rows), f32)
                gt = jnp.concatenate([parts[1], pad, parts[0], pad], axis=0)
            else:
                gt = jnp.concatenate([parts[0], jnp.zeros((width - 8, rows), f32)], axis=0)
            gc = gt.astype(bf16).T
            for h in range(heads):
                if heads == 2:
                    mine = (lane < d) if h == 0 else (lane >= d)
                    ka[slot, h] = jnp.where(mine, k, gc)
                else:
                    ka[slot, h, :, :width] = k
                    ka[slot, h, :, width:] = gc
                va[slot, h, :d] = vt[h * d : (h + 1) * d]

        def scores(slot, u, t):
            h, c = u
            return lax.dot_general(
                ka[slot, h, t * chunk : (t + 1) * chunk],
                qa[h, c * chunk : (c + 1) * chunk],
                (((1,), (1,)), ((), ())),
                preferred_element_type=f32,
            )

        def masked(s, c, t):
            if t < c:
                return s
            kp = lax.broadcasted_iota(jnp.int32, (chunk, chunk), 0)
            qp = lax.broadcasted_iota(jnp.int32, (chunk, chunk), 1)
            return jnp.where(kp <= qp, s, -1e30)

        def step(slot, diagonal, ahead=None):
            count = lambda u: u[1] + 1 if diagonal else chunks
            held = [first[t * chunk : (t + 1) * chunk] for t in range(count(units[0]))]
            if ahead is not None:
                ahead()
            for i, u in enumerate(units):
                h, c = u
                cols = slice(c * chunk, (c + 1) * chunk)
                if diagonal:
                    held = [masked(s, c, t) for t, s in enumerate(held)]
                top = held[0]
                for s in held[1:]:
                    top = jnp.maximum(top, s)
                old = peak[h : h + 1, cols]
                new = jnp.maximum(old, jnp.max(top, axis=0, keepdims=True))
                scaled = new * rate
                factor = jnp.exp2(old * rate - scaled)
                peak[h : h + 1, cols] = new
                following = units[i + 1] if i + 1 < len(units) else None
                coming = []
                total_add = None
                if following:
                    ahead_count = count(following)
                else:
                    ahead_count = 0 if diagonal else chunks
                for t in range(max(len(held), ahead_count)):
                    if t < ahead_count:
                        if following:
                            coming.append(scores(slot, following, t))
                        else:
                            first[t * chunk : (t + 1) * chunk] = scores(1 - slot, units[0], t)
                    if t < len(held):
                        w = jnp.exp2(held[t] * rate - scaled).astype(bf16)
                        add = jnp.dot(va[slot, h, :, t * chunk : (t + 1) * chunk], w, preferred_element_type=f32)
                        total_add = add if total_add is None else total_add + add
                acc[h, :, cols] = acc[h, :, cols] * factor + total_add
                held = coming

        prepare(0, 0)
        for t in range(chunks):
            first[t * chunk : (t + 1) * chunk] = scores(0, units[0], t)

        @pl.loop(0, me)
        def _(j):
            slot = lax.rem(j, 2)
            step(slot, False, lambda: prepare(j + 1, 1 - slot))

        step(lax.rem(me, 2), True)
        outs = [acc[h, :d] / acc[h, d : d + 1] for h in range(heads)]
        o = outs[0] if heads == 1 else jnp.concatenate(outs, axis=0)
        o_ref[...] = o.T.astype(bf16)

    vm = pl.BlockSpec(memory_space=pltpu.VMEM)
    return pl.pallas_call(
        body,
        in_specs=[pl.BlockSpec(memory_space=pltpu.SMEM), vm, vm, vm],
        out_specs=vm,
        scratch_shapes=[
            pltpu.VMEM((heads, rows, deep), bf16),
            pltpu.VMEM((2, heads, rows, deep), bf16),
            pltpu.VMEM((2, heads, ext, rows), bf16),
            pltpu.VMEM((heads, ext, rows), f32),
            pltpu.VMEM((8, rows), f32),
            pltpu.VMEM((rows, chunk), f32),
        ],
        out_shape=jax.ShapeDtypeStruct((rows, width), bf16),
        compiler_params=pltpu.CompilerParams(vmem_limit_bytes=50 * 2**20),
    )(rank, q, kv, gates)


def per_device(
    query_small,
    key_small,
    value_small,
    gates_small,
    query_large,
    key_large,
    value_large,
    gates_large,
    residual,
    mixer_small,
    mixer_large,
    mix_gain,
    value_weight,
    gate_weight,
    value_taps,
    gate_taps,
    down_weight,
    final_gain,
):
    shard_rows = query_small.shape[0]
    rank = lax.axis_index("sp").astype(jnp.int32).reshape(1)
    heads_small = gates_small.shape[1]
    heads_large = gates_large.shape[1]
    own_gates = jnp.concatenate(
        [
            gates_small.T,
            gates_large.T,
            jnp.zeros((8 - heads_small - heads_large, shard_rows), f32),
        ],
        axis=0,
    )
    small_pairs = lax.all_gather(
        jnp.concatenate([key_small, value_small], axis=1), "sp", axis=0, tiled=True
    )
    every_gate = lax.all_gather(own_gates, "sp", axis=0)
    large_pairs = lax.all_gather(
        jnp.concatenate([key_large, value_large], axis=1), "sp", axis=0, tiled=True
    )
    whole_value, whole_gate, whole_down = gather_turned(
        (value_weight, gate_weight, down_weight), "sp", (0, 0, 1)
    )
    small_out = attend(query_small, small_pairs, every_gate, rank, heads_small, 0)
    large_out = attend(query_large, large_pairs, every_gate, rank, heads_large, heads_small)
    tensor_parts = lax.axis_size(TP)
    own_rows = shard_rows // tensor_parts
    joined = jnp.concatenate([small_out, large_out], axis=1)
    pieces = joined.reshape(tensor_parts, own_rows, joined.shape[1])
    arrived = lax.all_to_all(pieces, TP, split_axis=0, concat_axis=0, tiled=True)
    layout = jnp.moveaxis(arrived, 0, 1)
    small_width = small_out.shape[1]
    all_small = layout[:, :, :small_width].reshape(own_rows, tensor_parts * small_width)
    all_large = layout[:, :, small_width:].reshape(own_rows, tensor_parts * large_out.shape[1])
    add_pieces = sent_together((mixer_small, mixer_large), TP, 0, 1)
    mix = jnp.dot(all_small, add_pieces[0], preferred_element_type=jnp.float32) + jnp.dot(
        all_large, add_pieces[1], preferred_element_type=jnp.float32
    )
    mixed = norm_rows(residual_scale * residual.astype(jnp.float32) + mix, mix_gain).astype(
        jnp.bfloat16
    )
    block_input = lax.all_gather(mixed, TP, axis=0, tiled=True)
    up_value = jnp.dot(block_input, whole_value, preferred_element_type=jnp.float32)
    up_gate = jnp.dot(block_input, whole_gate, preferred_element_type=jnp.float32)
    up_value = up_value.astype(jnp.bfloat16)
    up_gate = up_gate.astype(jnp.bfloat16)
    hidden_width = up_value.shape[1]
    trailing = jnp.concatenate([up_value[-2:], up_gate[-2:]], axis=1)
    earlier = passed_along(trailing, "sp", 1)
    padded_value = jnp.concatenate([earlier[:, :hidden_width], up_value], axis=0).astype(
        jnp.float32
    )
    padded_gate = jnp.concatenate([earlier[:, hidden_width:], up_gate], axis=0).astype(jnp.float32)
    filt_value = (
        value_taps[0] * padded_value[:-2]
        + value_taps[1] * padded_value[1:-1]
        + value_taps[2] * padded_value[2:]
    )
    filt_gate = (
        gate_taps[0] * padded_gate[:-2]
        + gate_taps[1] * padded_gate[1:-1]
        + gate_taps[2] * padded_gate[2:]
    )
    hidden = (jax.nn.silu(filt_gate) * filt_value).astype(jnp.bfloat16)
    ffn_terms = jnp.dot(hidden, whole_down, preferred_element_type=jnp.float32)
    ffn = lax.psum_scatter(
        ffn_terms.astype(jnp.bfloat16), TP, scatter_dimension=0, tiled=True
    ).astype(jnp.float32)
    return norm_rows(residual_scale * mixed.astype(jnp.float32) + ffn, final_gain).astype(
        jnp.bfloat16
    )


def solution(mesh):
    split = Mesh(mesh.devices.reshape(mesh.shape["sp"], 4, 2), ("sp", "tp_0", "tp_1"))
    placed = (
        P("sp", TP),
        P("sp", TP),
        P("sp", TP),
        P("sp", TP),
        P("sp", TP),
        P("sp", TP),
        P("sp", TP),
        P("sp", TP),
        P(SP_TP, None),
        P(TP, None),
        P(TP, None),
        P(),
        P("sp", TP),
        P("sp", TP),
        P(None, TP),
        P(None, TP),
        P(TP, "sp"),
        P(),
    )
    return jax.shard_map(
        per_device, mesh=split, in_specs=placed, out_specs=P(SP_TP, None), check_vma=False
    )
```

```python
import math

import jax
import jax.numpy as jnp
import numpy as np
from jax import lax
from jax.experimental import pallas as pl
from jax.experimental.pallas import tpu as pltpu
from jax.sharding import Mesh
from jax.sharding import PartitionSpec as P

SP = ("sp_z", "sp_x")
TP = ("tp_y", "tp_c")
ALL = SP + TP
bf16 = jnp.bfloat16
f32 = jnp.float32
residual_scale = 2.0**0.5
epsilon = 1e-05


def gather_turned(arrays, axis, dims):
    turned = [jnp.moveaxis(a, dim, 0) for a, dim in zip(arrays, dims)]
    widths = [t[0].size for t in turned]
    both = jnp.concatenate([t.reshape(-1, w) for t, w in zip(turned, widths)], axis=1)
    out = lax.all_gather(both, axis, axis=0, tiled=True)
    pieces = jnp.split(out, [sum(widths[:k]) for k in range(1, len(widths))], axis=1)
    return tuple(
        (
            jnp.moveaxis(b.reshape(-1, *t.shape[1:]), 0, dim)
            for b, t, dim in zip(pieces, turned, dims)
        )
    )


def shifted(value, axis, steps):
    count = lax.axis_size(axis)
    return lax.ppermute(value, axis, [(i, (i + steps) % count) for i in range(count)])


def passed_along(value, axis, steps):
    count = lax.axis_size(axis)
    first, last = (max(0, -steps), min(count, count - steps))
    return lax.ppermute(value, axis, [(source, source + steps) for source in range(first, last)])


def norm_rows(values, gain):
    center = jnp.mean(values, axis=-1, keepdims=True)
    spread = jnp.mean(jnp.square(values - center), axis=-1, keepdims=True)
    return (values - center) * lax.rsqrt(spread + epsilon) * gain


LOW = -1e30
CHUNK = 256
EXTRA = 32
STAT_ROWS = 16


def in_pieces(value):
    high = value.astype(bf16).astype(f32)
    middle = (value - high).astype(bf16).astype(f32)
    return high, middle, value - high - middle


def pack(key_small, value_small, key_large, value_large, query_small, query_large, gates):
    rows, width = key_small.shape
    half = rows // 2
    low = width // 2
    tiles = rows // width

    def body(ks, vs, kl, vl, qs, ql, g, kv, q):
        lane = lax.broadcasted_iota(jnp.int32, (rows, width), 1)
        turn = lambda ref: pltpu.roll(ref[...].astype(f32), low, 1)
        for slot in range(2):
            part = slice(slot * half, (slot + 1) * half)
            kv[slot, :half] = kl[part]
            kv[slot, half:rows] = vl[part]
            q[slot] = ql[...]
        kv[2, :rows] = jnp.where(lane < low, ks[...].astype(f32), turn(vs)).astype(bf16)
        kv[3, :rows] = jnp.where(lane < low, turn(ks), vs[...].astype(f32)).astype(bf16)
        q[2] = qs[...]
        q[3] = turn(qs).astype(bf16)
        for slot, head in ((0, 2), (1, 2), (2, 0), (3, 1)):
            blocks = []
            for piece in in_pieces(g[head : head + 1, :]):
                blocks += [piece[:, i * width : (i + 1) * width] for i in range(tiles)]
                blocks.append(jnp.zeros((8 - tiles, width), f32))
            blocks.append(jnp.zeros((EXTRA - 24, width), f32))
            kv[slot, rows:] = jnp.concatenate(blocks, axis=0).astype(bf16)

    vm = pl.BlockSpec(memory_space=pltpu.VMEM)
    return pl.pallas_call(
        body,
        in_specs=[vm] * 7,
        out_specs=[vm, vm],
        out_shape=[
            jax.ShapeDtypeStruct((4, rows + EXTRA, width), bf16),
            jax.ShapeDtypeStruct((4, rows, width), bf16),
        ],
    )(key_small, value_small, key_large, value_large, query_small, query_large, gates)


def work_tables(calls, depth, turns):
    tables = []
    for here in range(turns):
        row = []
        for shifts in calls:
            steps = []
            for z in range(depth):
                for n, shift in enumerate(shifts):
                    there = (here + shift) % turns
                    for w in range(depth):
                        key, query = w * turns + there, z * turns + here
                        if key < query:
                            steps.append((z, n * depth + w, 0))
                for n, shift in enumerate(shifts):
                    if shift == 0:
                        steps.append((z, n * depth + z, 1))
            row.append(steps)
        tables.append(row)
    longest = [max(len(tables[h][k]) for h in range(turns)) + 1 for k in range(len(calls))]
    out = []
    for k in range(len(calls)):
        table = np.zeros((turns, longest[k] * 3 + 1), np.int32)
        for h in range(turns):
            flat = np.array(tables[h][k] + [(0, 0, 0)] * (longest[k] - len(tables[h][k])), np.int32)
            table[h, :-1] = flat.reshape(-1)
            table[h, -1] = len(tables[h][k])
        out.append(table)
    return out


def attend(where, table, queries, chunks, state, final, tensor_parts):
    depth, rows, width = queries.shape
    half = rows // 2
    low = width // 2
    tiles = rows // width
    blocks = sum(c.shape[0] for c in chunks)
    columns = rows // CHUNK
    tall = width + 16
    last = table.shape[0] - 1
    own = rows // tensor_parts
    fresh = state is None

    def body(*refs):
        where_ref, table_ref, q_ref = refs[:3]
        chunk_refs = refs[3 : 3 + len(chunks)]
        at = 3 + len(chunks) + (0 if fresh else 2)
        state_in = () if fresh else refs[at - 2 : at]
        if final:
            out_ref = refs[at]
            acc, peak = refs[at + 1 : at + 3]
            scratch = refs[at + 3 :]
        else:
            acc, peak = refs[at : at + 2]
            scratch = refs[at + 2 :]
        qa, ka_small, va_small, ka_large, va_large, first = scratch
        slot = where_ref[0]
        count = table_ref[last]
        if fresh:
            acc[...] = jnp.zeros(acc.shape, f32)
            peak[...] = jnp.full(peak.shape, LOW, f32)
        elif final:
            acc[...] = state_in[0][...]
            peak[...] = state_in[1][...]

        def attention(small):
            d = low if small else width
            ext = d + 16
            span = rows if small else half
            tile = CHUNK if small else half
            parts = span // tile
            root = d**0.5
            rate = math.log2(math.e) / root
            ka, va = (ka_small, va_small) if small else (ka_large, va_large)
            deep = width if small else 2 * width
            lane = lax.broadcasted_iota(jnp.int32, (rows, width), 1)

            @pl.loop(0, depth)
            def _(z):
                q = q_ref[z]
                if small:
                    one = ((lane >= d) & (lane < d + 3)).astype(f32)
                    qa[z, :, :width] = jnp.where(lane < d, q.astype(f32), one).astype(bf16)
                else:
                    qa[z, :, :width] = q
                    qa[z, :, width:] = (lane < 3).astype(f32).astype(bf16)

            def prepare(ref, n, block):
                pieces = ref[n, rows : rows + 24].astype(f32)
                gate = pieces[0:8] + pieces[8:16] + pieces[16:24]
                bias = jnp.concatenate([gate[i : i + 1] for i in range(tiles)], axis=1) * -root
                bias = jnp.broadcast_to(bias, (8, rows))
                if not small:
                    bias = jnp.where(slot == 0, bias[:, :half], bias[:, half:])
                high, middle, rest = in_pieces(bias)
                row = lax.broadcasted_iota(jnp.int32, (8, span), 0)
                zero = jnp.zeros((8, span), f32)
                picked = jnp.where(row == 0, high, jnp.where(row == 1, middle, jnp.where(row == 2, rest, zero)))
                before = d if small else 0
                stack = [picked, jnp.zeros((width - before - 8, span), f32)]
                if before:
                    stack = [jnp.zeros((before, span), f32)] + stack
                gate_columns = jnp.concatenate(stack, axis=0).astype(bf16).T
                if small:
                    kv = ref[n, :rows]
                    ka[block] = jnp.where(lane < d, kv, gate_columns)
                    va[block, :d] = kv.T[d:]
                else:
                    ka[block, :, :width] = ref[n, :half]
                    ka[block, :, width:] = gate_columns
                    va[block, :d] = ref[n, half:rows].T
                va[block, d:] = jnp.ones((16, span), bf16)

            offset = 0
            for ref in chunk_refs:
                base = offset

                @pl.loop(0, ref.shape[0])
                def _(n):
                    prepare(ref, n, base + n)

                offset += ref.shape[0]

            def scores(z, block, c, t):
                return lax.dot_general(
                    ka[block, t * tile : (t + 1) * tile],
                    qa[z, c * CHUNK : (c + 1) * CHUNK, :deep],
                    (((1,), (1,)), ((), ())),
                    preferred_element_type=f32,
                )

            def masked(s, c, t):
                if small and t < c:
                    return s
                key = lax.broadcasted_iota(jnp.int32, (tile, CHUNK), 0) + t * tile
                if not small:
                    key = key + slot * half
                query = lax.broadcasted_iota(jnp.int32, (tile, CHUNK), 1) + c * CHUNK
                return jnp.where(key <= query, s, LOW)

            def step(n, diagonal):
                z, block = table_ref[3 * n], table_ref[3 * n + 1]
                next_z, next_block = table_ref[3 * n + 3], table_ref[3 * n + 4]
                held_count = lambda c: c + 1 if diagonal and small else parts
                held = [first[t * tile : (t + 1) * tile] for t in range(held_count(0))]
                for c in range(columns):
                    cols = slice(c * CHUNK, (c + 1) * CHUNK)
                    if diagonal:
                        held = [masked(s, c, t) for t, s in enumerate(held)]
                    top = held[0]
                    for s in held[1:]:
                        top = jnp.maximum(top, s)
                    old = peak[z, 0:1, cols]
                    new = jnp.maximum(old, jnp.max(top, axis=0, keepdims=True))
                    scaled = new * rate
                    factor = jnp.exp2(old * rate - scaled)
                    peak[z, 0:1, cols] = new
                    coming = []
                    added = None
                    following = c + 1 < columns
                    ahead = held_count(c + 1) if following else parts
                    for t in range(max(len(held), ahead)):
                        if t < ahead:
                            if following:
                                coming.append(scores(z, block, c + 1, t))
                            else:
                                first[t * tile : (t + 1) * tile] = scores(next_z, next_block, 0, t)
                        if t < len(held):
                            w = jnp.exp2(held[t] * rate - scaled).astype(bf16)
                            add = jnp.dot(
                                va[block, :, t * tile : (t + 1) * tile], w, preferred_element_type=f32
                            )
                            added = add if added is None else added + add
                    acc[z, :ext, cols] = acc[z, :ext, cols] * factor + added
                    held = coming

            for t in range(parts):
                first[t * tile : (t + 1) * tile] = scores(table_ref[0], table_ref[1], 0, t)

            @pl.loop(0, count)
            def _(n):
                diagonal = table_ref[3 * n + 2]

                @pl.when(diagonal == 0)
                def _():
                    step(n, False)

                @pl.when(diagonal == 1)
                def _():
                    step(n, True)

            if final:

                @pl.loop(0, depth)
                def _(z):
                    total = acc[z, d : d + 1]
                    out = acc[z, :d] / total
                    if small:
                        out = jnp.concatenate([out, jnp.zeros((width - d, rows), f32)], axis=0)
                    out = out.T.astype(bf16)
                    level = peak[z, 0:1] * rate + jnp.log2(total)
                    stat = jnp.concatenate([*in_pieces(level), jnp.zeros((STAT_ROWS - 3, rows), f32)], axis=0)
                    for r in range(tensor_parts):
                        out_ref[z * tensor_parts + r, :own] = out[r * own : (r + 1) * own]
                        if not small:
                            mine = stat[:, r * own : (r + 1) * own]
                            mine = jnp.concatenate([mine, jnp.zeros((STAT_ROWS, width - own), f32)], axis=1)
                            out_ref[z * tensor_parts + r, own:] = mine.astype(bf16)
                        else:
                            out_ref[z * tensor_parts + r, own:] = jnp.zeros((STAT_ROWS, width), bf16)

        @pl.when(slot < 2)
        def _():
            attention(False)

        @pl.when(slot >= 2)
        def _():
            attention(True)

    vm = pl.BlockSpec(memory_space=pltpu.VMEM)
    sm = pl.BlockSpec(memory_space=pltpu.SMEM)
    state_shapes = [((depth, tall, rows), f32), ((depth, 8, rows), f32)]
    scratch = [pltpu.VMEM(s, t) for s, t in state_shapes] if final else []
    scratch += [
        pltpu.VMEM((depth, rows, 2 * width), bf16),
        pltpu.VMEM((blocks, rows, width), bf16),
        pltpu.VMEM((blocks, low + 16, rows), bf16),
        pltpu.VMEM((blocks, half, 2 * width), bf16),
        pltpu.VMEM((blocks, tall, half), bf16),
        pltpu.VMEM((rows, CHUNK), f32),
    ]
    if final:
        out_shape = jax.ShapeDtypeStruct((depth * tensor_parts, own + STAT_ROWS, width), bf16)
        out_specs = vm
        aliases = {}
    else:
        out_shape = [jax.ShapeDtypeStruct(s, t) for s, t in state_shapes]
        out_specs = [vm, vm]
        at = 3 + len(chunks)
        aliases = {} if fresh else {at: 0, at + 1: 1}
    args = [where, table, queries, *chunks] + ([] if fresh else list(state))
    return pl.pallas_call(
        body,
        in_specs=[sm, sm] + [vm] * (len(args) - 2),
        out_specs=out_specs,
        scratch_shapes=scratch,
        out_shape=out_shape,
        input_output_aliases=aliases,
        compiler_params=pltpu.CompilerParams(vmem_limit_bytes=58 * 2**20),
    )(*args)


def mix_rows(place, arrived, mixers, residual, gain):
    own, wide = residual.shape
    width = arrived.shape[2]
    cores = 2
    turns = arrived.shape[0] // 4 // cores
    parts = turns * cores

    def body(place_ref, arrived_ref, *refs):
        mixer_refs = refs[: len(mixers)]
        residual_ref, gain_ref, out_ref, acc = refs[len(mixers) :]
        lane = lax.broadcasted_iota(jnp.int32, (own, width), 1)

        def level(index):
            pieces = arrived_ref[index, own:].astype(f32)
            line = pieces[0:1] + pieces[1:2] + pieces[2:3]
            return jnp.broadcast_to(line, (8, width)).T[:own, 0:1]

        def rows_of(part):
            second = pltpu.roll(arrived_ref[3 * parts + part, :own].astype(f32), width // 2, 1)
            small = jnp.where(lane < width // 2, arrived_ref[2 * parts + part, :own].astype(f32), second)
            share = 1.0 / (1.0 + jnp.exp2(level(part) - level(parts + part)))
            large = arrived_ref[part, :own].astype(f32) * (1.0 - share) + arrived_ref[
                parts + part, :own
            ].astype(f32) * share
            return small.astype(bf16), large.astype(bf16)

        acc[...] = residual_ref[...].astype(f32) * residual_scale
        for ref, (_, shift, other, first) in zip(mixer_refs, mixers):
            y = lax.rem(place_ref[0] + shift + turns, turns)
            core = place_ref[1] if other == 0 else 1 - place_ref[1]
            both = rows_of(y * cores + core)
            if ref.shape[0] == 2 * width:
                left = jnp.concatenate(both, axis=1)
            else:
                left = both[first]
            acc[...] += jnp.dot(left, ref[...], preferred_element_type=f32)
        values = acc[...]
        center = jnp.mean(values, axis=-1, keepdims=True)
        values = values - center
        spread = jnp.mean(jnp.square(values), axis=-1, keepdims=True)
        out_ref[...] = (values * lax.rsqrt(spread + epsilon) * gain_ref[...]).astype(bf16)

    vm = pl.BlockSpec(memory_space=pltpu.VMEM)
    return pl.pallas_call(
        body,
        in_specs=[pl.BlockSpec(memory_space=pltpu.SMEM)] + [vm] * (len(mixers) + 3),
        out_specs=vm,
        scratch_shapes=[pltpu.VMEM((own, wide), f32)],
        out_shape=jax.ShapeDtypeStruct((own, wide), bf16),
        compiler_params=pltpu.CompilerParams(vmem_limit_bytes=40 * 2**20),
    )(place, arrived, *[m[0] for m in mixers], residual, gain.reshape(1, wide))


def mixers_of_all(mixer_small, mixer_large):
    half = mixer_small.shape[0]
    mine = jnp.concatenate([mixer_small, mixer_large], axis=0)
    before = shifted(mine, "tp_y", 1)
    after = shifted(mine, "tp_y", -1)
    far_small = shifted(before[:half], "tp_y", 1)
    far_large = shifted(after[half:], "tp_y", -1)
    pieces = [(mine, 0, 0), (before, -1, 0), (after, 1, 0), (far_small, 2, 0), (far_large, 2, 1)]
    here = [(a, shift, 0, first) for a, shift, first in pieces]
    there = [(shifted(a, "tp_c", 1), shift, 1, first) for a, shift, first in pieces]
    return here + there


def per_device(
    query_small,
    key_small,
    value_small,
    gates_small,
    query_large,
    key_large,
    value_large,
    gates_large,
    residual,
    mixer_small,
    mixer_large,
    mix_gain,
    value_weight,
    gate_weight,
    value_taps,
    gate_taps,
    down_weight,
    final_gain,
):
    shard_rows = query_small.shape[0]
    slot = lax.axis_index("sp_z").astype(jnp.int32)
    column = lax.axis_index("sp_x")
    depth, turns = lax.axis_size("sp_z"), lax.axis_size("sp_x")
    heads_small = gates_small.shape[1]
    heads_large = gates_large.shape[1]
    blank = jnp.zeros((8 - heads_small - heads_large, shard_rows), f32)
    own_gates = jnp.concatenate([gates_small.T, gates_large.T, blank], axis=0)
    packed, asked = pack(
        key_small, value_small, key_large, value_large, query_small, query_large, own_gates
    )
    pairs = lax.all_to_all(packed, "sp_z", split_axis=0, concat_axis=0, tiled=True)
    queries = lax.all_to_all(asked, "sp_z", split_axis=0, concat_axis=0, tiled=True)
    before = shifted(pairs, "sp_x", 1)
    after = shifted(pairs, "sp_x", -1)
    far_first = shifted(before[: depth // 2], "sp_x", 1)
    far_second = shifted(after[depth // 2 :], "sp_x", -1)
    mixers = mixers_of_all(mixer_small, mixer_large)
    whole_value, whole_gate, whole_down = gather_turned(
        (value_weight, gate_weight, down_weight), SP, (0, 0, 1)
    )
    (table,) = work_tables([(0, -1, 1, 2)], depth, turns)
    sent = attend(
        slot.reshape(1),
        lax.dynamic_index_in_dim(jnp.asarray(table), column, 0, keepdims=False),
        queries,
        [pairs, before, after, far_first, far_second],
        None,
        True,
        lax.axis_size(TP),
    )
    arrived = lax.all_to_all(sent, ("sp_z",) + TP, split_axis=0, concat_axis=0, tiled=True)
    place = jnp.stack([lax.axis_index("tp_y"), lax.axis_index("tp_c")]).astype(jnp.int32)
    mixed = mix_rows(place, arrived, mixers, residual, mix_gain)
    block_input = lax.all_gather(mixed, TP, axis=0, tiled=True)
    up_value = jnp.dot(block_input, whole_value, preferred_element_type=jnp.float32)
    up_gate = jnp.dot(block_input, whole_gate, preferred_element_type=jnp.float32)
    up_value = up_value.astype(jnp.bfloat16)
    up_gate = up_gate.astype(jnp.bfloat16)
    hidden_width = up_value.shape[1]
    trailing = jnp.concatenate([up_value[-2:], up_gate[-2:]], axis=1)
    earlier = passed_along(trailing, SP, 1)
    padded_value = jnp.concatenate([earlier[:, :hidden_width], up_value], axis=0).astype(
        jnp.float32
    )
    padded_gate = jnp.concatenate([earlier[:, hidden_width:], up_gate], axis=0).astype(jnp.float32)
    filt_value = (
        value_taps[0] * padded_value[:-2]
        + value_taps[1] * padded_value[1:-1]
        + value_taps[2] * padded_value[2:]
    )
    filt_gate = (
        gate_taps[0] * padded_gate[:-2]
        + gate_taps[1] * padded_gate[1:-1]
        + gate_taps[2] * padded_gate[2:]
    )
    hidden = (jax.nn.silu(filt_gate) * filt_value).astype(jnp.bfloat16)
    ffn_terms = jnp.dot(hidden, whole_down, preferred_element_type=jnp.float32)
    ffn = lax.psum_scatter(
        ffn_terms.astype(jnp.bfloat16), TP, scatter_dimension=0, tiled=True
    ).astype(jnp.float32)
    return norm_rows(residual_scale * mixed.astype(jnp.float32) + ffn, final_gain).astype(
        jnp.bfloat16
    )


def solution(mesh):
    split = Mesh(mesh.devices.reshape(4, 4, 4, 2), ALL)
    placed = (P(SP, TP),) * 8 + (
        P(ALL, None),
        P(TP, None),
        P(TP, None),
        P(),
        P(SP, TP),
        P(SP, TP),
        P(None, TP),
        P(None, TP),
        P(TP, SP),
        P(),
    )
    return jax.shard_map(
        per_device, mesh=split, in_specs=placed, out_specs=P(ALL, None), check_vma=False
    )
```

```python
import math

import jax
import jax.numpy as jnp
import numpy as np
from jax import lax
from jax.experimental import pallas as pl
from jax.experimental.pallas import tpu as pltpu
from jax.sharding import Mesh
from jax.sharding import PartitionSpec as P

SP = ("sp_z", "sp_x")
TP = ("tp_y", "tp_c")
ALL = SP + TP
bf16 = jnp.bfloat16
f32 = jnp.float32
residual_scale = 2.0**0.5
epsilon = 1e-05


def gather_turned(arrays, axis, dims):
    turned = [jnp.moveaxis(a, dim, 0) for a, dim in zip(arrays, dims)]
    widths = [t[0].size for t in turned]
    both = jnp.concatenate([t.reshape(-1, w) for t, w in zip(turned, widths)], axis=1)
    out = lax.all_gather(both, axis, axis=0, tiled=True)
    pieces = jnp.split(out, [sum(widths[:k]) for k in range(1, len(widths))], axis=1)
    return tuple(
        (
            jnp.moveaxis(b.reshape(-1, *t.shape[1:]), 0, dim)
            for b, t, dim in zip(pieces, turned, dims)
        )
    )


def shifted(value, axis, steps):
    count = lax.axis_size(axis)
    return lax.ppermute(value, axis, [(i, (i + steps) % count) for i in range(count)])


def passed_along(value, axis, steps):
    count = lax.axis_size(axis)
    first, last = (max(0, -steps), min(count, count - steps))
    return lax.ppermute(value, axis, [(source, source + steps) for source in range(first, last)])


def norm_rows(values, gain):
    center = jnp.mean(values, axis=-1, keepdims=True)
    spread = jnp.mean(jnp.square(values - center), axis=-1, keepdims=True)
    return (values - center) * lax.rsqrt(spread + epsilon) * gain


LOW = -1e30
CHUNK = 256
EXTRA = 32
STAT_ROWS = 16


def in_pieces(value):
    high = value.astype(bf16).astype(f32)
    middle = (value - high).astype(bf16).astype(f32)
    return high, middle, value - high - middle


def pack(key_small, value_small, key_large, value_large, query_small, query_large, gates):
    rows, width = key_small.shape
    half = rows // 2
    low = width // 2
    tiles = rows // width

    def body(ks, vs, kl, vl, qs, ql, g, kv, q):
        lane = lax.broadcasted_iota(jnp.int32, (rows, width), 1)
        turn = lambda ref: pltpu.roll(ref[...].astype(f32), low, 1)
        for slot in range(2):
            part = slice(slot * half, (slot + 1) * half)
            kv[slot, :half] = kl[part]
            kv[slot, half:rows] = vl[part]
            q[slot] = ql[...]
        kv[2, :rows] = jnp.where(lane < low, ks[...].astype(f32), turn(vs)).astype(bf16)
        kv[3, :rows] = jnp.where(lane < low, turn(ks), vs[...].astype(f32)).astype(bf16)
        q[2] = qs[...]
        q[3] = turn(qs).astype(bf16)
        for slot, head in ((0, 2), (1, 2), (2, 0), (3, 1)):
            blocks = []
            for piece in in_pieces(g[head : head + 1, :]):
                blocks += [piece[:, i * width : (i + 1) * width] for i in range(tiles)]
                blocks.append(jnp.zeros((8 - tiles, width), f32))
            blocks.append(jnp.zeros((EXTRA - 24, width), f32))
            kv[slot, rows:] = jnp.concatenate(blocks, axis=0).astype(bf16)

    vm = pl.BlockSpec(memory_space=pltpu.VMEM)
    return pl.pallas_call(
        body,
        in_specs=[vm] * 7,
        out_specs=[vm, vm],
        out_shape=[
            jax.ShapeDtypeStruct((4, rows + EXTRA, width), bf16),
            jax.ShapeDtypeStruct((4, rows, width), bf16),
        ],
    )(key_small, value_small, key_large, value_large, query_small, query_large, gates)


def work_tables(calls, depth, turns):
    tables = []
    for here in range(turns):
        row = []
        for shifts in calls:
            steps = []
            for z in range(depth):
                for n, shift in enumerate(shifts):
                    there = (here + shift) % turns
                    for w in range(depth):
                        key, query = w * turns + there, z * turns + here
                        if key < query:
                            steps.append((z, n * depth + w, 0))
                for n, shift in enumerate(shifts):
                    if shift == 0:
                        steps.append((z, n * depth + z, 1))
            row.append(steps)
        tables.append(row)
    longest = [max(len(tables[h][k]) for h in range(turns)) + 1 for k in range(len(calls))]
    out = []
    for k in range(len(calls)):
        table = np.zeros((turns, longest[k] * 3 + 1), np.int32)
        for h in range(turns):
            flat = np.array(tables[h][k] + [(0, 0, 0)] * (longest[k] - len(tables[h][k])), np.int32)
            table[h, :-1] = flat.reshape(-1)
            table[h, -1] = len(tables[h][k])
        out.append(table)
    return out


def attend(where, table, queries, chunks, state, final, tensor_parts):
    depth, rows, width = queries.shape
    half = rows // 2
    low = width // 2
    tiles = rows // width
    blocks = sum(c.shape[0] for c in chunks)
    columns = rows // CHUNK
    tall = width + 16
    last = table.shape[0] - 1
    own = rows // tensor_parts
    fresh = state is None

    def body(*refs):
        where_ref, table_ref, q_ref = refs[:3]
        chunk_refs = refs[3 : 3 + len(chunks)]
        at = 3 + len(chunks) + (0 if fresh else 2)
        state_in = () if fresh else refs[at - 2 : at]
        if final:
            out_ref = refs[at]
            acc, peak = refs[at + 1 : at + 3]
            scratch = refs[at + 3 :]
        else:
            acc, peak = refs[at : at + 2]
            scratch = refs[at + 2 :]
        qa, ka_small, va_small, ka_large, va_large, first = scratch
        slot = where_ref[0]
        count = table_ref[last]
        if fresh:
            acc[...] = jnp.zeros(acc.shape, f32)
            peak[...] = jnp.full(peak.shape, LOW, f32)
        elif final:
            acc[...] = state_in[0][...]
            peak[...] = state_in[1][...]

        def attention(small):
            d = low if small else width
            ext = d + 16
            span = rows if small else half
            tile = CHUNK if small else half
            parts = span // tile
            root = d**0.5
            rate = math.log2(math.e) / root
            ka, va = (ka_small, va_small) if small else (ka_large, va_large)
            deep = width if small else 2 * width
            lane = lax.broadcasted_iota(jnp.int32, (rows, width), 1)

            @pl.loop(0, depth)
            def _(z):
                q = q_ref[z]
                if small:
                    one = ((lane >= d) & (lane < d + 3)).astype(f32)
                    qa[z, :, :width] = jnp.where(lane < d, q.astype(f32), one).astype(bf16)
                else:
                    qa[z, :, :width] = q
                    qa[z, :, width:] = (lane < 3).astype(f32).astype(bf16)

            def prepare(ref, n, block):
                pieces = ref[n, rows : rows + 24].astype(f32)
                gate = pieces[0:8] + pieces[8:16] + pieces[16:24]
                bias = jnp.concatenate([gate[i : i + 1] for i in range(tiles)], axis=1) * -root
                bias = jnp.broadcast_to(bias, (8, rows))
                if not small:
                    bias = jnp.where(slot == 0, bias[:, :half], bias[:, half:])
                high, middle, rest = in_pieces(bias)
                row = lax.broadcasted_iota(jnp.int32, (8, span), 0)
                zero = jnp.zeros((8, span), f32)
                picked = jnp.where(row == 0, high, jnp.where(row == 1, middle, jnp.where(row == 2, rest, zero)))
                before = d if small else 0
                stack = [picked, jnp.zeros((width - before - 8, span), f32)]
                if before:
                    stack = [jnp.zeros((before, span), f32)] + stack
                gate_columns = jnp.concatenate(stack, axis=0).astype(bf16).T
                if small:
                    kv = ref[n, :rows]
                    ka[block] = jnp.where(lane < d, kv, gate_columns)
                    va[block, :d] = kv.T[d:]
                else:
                    ka[block, :, :width] = ref[n, :half]
                    ka[block, :, width:] = gate_columns
                    va[block, :d] = ref[n, half:rows].T
                va[block, d:] = jnp.ones((16, span), bf16)

            offset = 0
            for ref in chunk_refs:
                base = offset

                @pl.loop(0, ref.shape[0])
                def _(n):
                    prepare(ref, n, base + n)

                offset += ref.shape[0]

            def scores(z, block, c, t):
                return lax.dot_general(
                    ka[block, t * tile : (t + 1) * tile],
                    qa[z, c * CHUNK : (c + 1) * CHUNK, :deep],
                    (((1,), (1,)), ((), ())),
                    preferred_element_type=f32,
                )

            def masked(s, c, t):
                if small and t < c:
                    return s
                key = lax.broadcasted_iota(jnp.int32, (tile, CHUNK), 0) + t * tile
                if not small:
                    key = key + slot * half
                query = lax.broadcasted_iota(jnp.int32, (tile, CHUNK), 1) + c * CHUNK
                return jnp.where(key <= query, s, LOW)

            def step(n, diagonal):
                z, block = table_ref[3 * n], table_ref[3 * n + 1]
                next_z, next_block = table_ref[3 * n + 3], table_ref[3 * n + 4]
                held_count = lambda c: c + 1 if diagonal and small else parts
                held = [first[t * tile : (t + 1) * tile] for t in range(held_count(0))]
                for c in range(columns):
                    cols = slice(c * CHUNK, (c + 1) * CHUNK)
                    if diagonal:
                        held = [masked(s, c, t) for t, s in enumerate(held)]
                    top = held[0]
                    for s in held[1:]:
                        top = jnp.maximum(top, s)
                    old = peak[z, 0:1, cols]
                    new = jnp.maximum(old, jnp.max(top, axis=0, keepdims=True))
                    scaled = new * rate
                    factor = jnp.exp2(old * rate - scaled)
                    peak[z, 0:1, cols] = new
                    coming = []
                    added = None
                    following = c + 1 < columns
                    ahead = held_count(c + 1) if following else parts
                    for t in range(max(len(held), ahead)):
                        if t < ahead:
                            if following:
                                coming.append(scores(z, block, c + 1, t))
                            else:
                                first[t * tile : (t + 1) * tile] = scores(next_z, next_block, 0, t)
                        if t < len(held):
                            w = jnp.exp2(held[t] * rate - scaled).astype(bf16)
                            add = jnp.dot(
                                va[block, :, t * tile : (t + 1) * tile], w, preferred_element_type=f32
                            )
                            added = add if added is None else added + add
                    acc[z, :ext, cols] = acc[z, :ext, cols] * factor + added
                    held = coming

            for t in range(parts):
                first[t * tile : (t + 1) * tile] = scores(table_ref[0], table_ref[1], 0, t)

            @pl.loop(0, count)
            def _(n):
                diagonal = table_ref[3 * n + 2]

                @pl.when(diagonal == 0)
                def _():
                    step(n, False)

                @pl.when(diagonal == 1)
                def _():
                    step(n, True)

            if final:

                @pl.loop(0, depth)
                def _(z):
                    total = acc[z, d : d + 1]
                    out = acc[z, :d] / total
                    if small:
                        out = jnp.concatenate([out, jnp.zeros((width - d, rows), f32)], axis=0)
                    out = out.T.astype(bf16)
                    level = peak[z, 0:1] * rate + jnp.log2(total)
                    stat = jnp.concatenate([*in_pieces(level), jnp.zeros((STAT_ROWS - 3, rows), f32)], axis=0)
                    for r in range(tensor_parts):
                        out_ref[z * tensor_parts + r, :own] = out[r * own : (r + 1) * own]
                        if not small:
                            mine = stat[:, r * own : (r + 1) * own]
                            mine = jnp.concatenate([mine, jnp.zeros((STAT_ROWS, width - own), f32)], axis=1)
                            out_ref[z * tensor_parts + r, own:] = mine.astype(bf16)
                        else:
                            out_ref[z * tensor_parts + r, own:] = jnp.zeros((STAT_ROWS, width), bf16)

        @pl.when(slot < 2)
        def _():
            attention(False)

        @pl.when(slot >= 2)
        def _():
            attention(True)

    vm = pl.BlockSpec(memory_space=pltpu.VMEM)
    sm = pl.BlockSpec(memory_space=pltpu.SMEM)
    state_shapes = [((depth, tall, rows), f32), ((depth, 8, rows), f32)]
    scratch = [pltpu.VMEM(s, t) for s, t in state_shapes] if final else []
    scratch += [
        pltpu.VMEM((depth, rows, 2 * width), bf16),
        pltpu.VMEM((blocks, rows, width), bf16),
        pltpu.VMEM((blocks, low + 16, rows), bf16),
        pltpu.VMEM((blocks, half, 2 * width), bf16),
        pltpu.VMEM((blocks, tall, half), bf16),
        pltpu.VMEM((rows, CHUNK), f32),
    ]
    if final:
        out_shape = jax.ShapeDtypeStruct((depth * tensor_parts, own + STAT_ROWS, width), bf16)
        out_specs = vm
        aliases = {}
    else:
        out_shape = [jax.ShapeDtypeStruct(s, t) for s, t in state_shapes]
        out_specs = [vm, vm]
        at = 3 + len(chunks)
        aliases = {} if fresh else {at: 0, at + 1: 1}
    args = [where, table, queries, *chunks] + ([] if fresh else list(state))
    return pl.pallas_call(
        body,
        in_specs=[sm, sm] + [vm] * (len(args) - 2),
        out_specs=out_specs,
        scratch_shapes=scratch,
        out_shape=out_shape,
        input_output_aliases=aliases,
        compiler_params=pltpu.CompilerParams(vmem_limit_bytes=58 * 2**20),
    )(*args)


def mix_rows(place, arrived, mixers, residual, gain):
    own, wide = residual.shape
    width = arrived.shape[2]
    cores = 2
    turns = arrived.shape[0] // 4 // cores
    parts = turns * cores

    def body(place_ref, arrived_ref, *refs):
        mixer_refs = refs[: len(mixers)]
        residual_ref, gain_ref, out_ref, acc = refs[len(mixers) :]
        lane = lax.broadcasted_iota(jnp.int32, (own, width), 1)

        def level(index):
            pieces = arrived_ref[index, own:].astype(f32)
            line = pieces[0:1] + pieces[1:2] + pieces[2:3]
            return jnp.broadcast_to(line, (8, width)).T[:own, 0:1]

        def rows_of(part):
            second = pltpu.roll(arrived_ref[3 * parts + part, :own].astype(f32), width // 2, 1)
            small = jnp.where(lane < width // 2, arrived_ref[2 * parts + part, :own].astype(f32), second)
            share = 1.0 / (1.0 + jnp.exp2(level(part) - level(parts + part)))
            large = arrived_ref[part, :own].astype(f32) * (1.0 - share) + arrived_ref[
                parts + part, :own
            ].astype(f32) * share
            return small.astype(bf16), large.astype(bf16)

        acc[...] = residual_ref[...].astype(f32) * residual_scale
        for ref, (_, shift, other, first) in zip(mixer_refs, mixers):
            y = lax.rem(place_ref[0] + shift + turns, turns)
            core = place_ref[1] if other == 0 else 1 - place_ref[1]
            both = rows_of(y * cores + core)
            if ref.shape[0] == 2 * width:
                left = jnp.concatenate(both, axis=1)
            else:
                left = both[first]
            acc[...] += jnp.dot(left, ref[...], preferred_element_type=f32)
        values = acc[...]
        center = jnp.mean(values, axis=-1, keepdims=True)
        values = values - center
        spread = jnp.mean(jnp.square(values), axis=-1, keepdims=True)
        out_ref[...] = (values * lax.rsqrt(spread + epsilon) * gain_ref[...]).astype(bf16)

    vm = pl.BlockSpec(memory_space=pltpu.VMEM)
    return pl.pallas_call(
        body,
        in_specs=[pl.BlockSpec(memory_space=pltpu.SMEM)] + [vm] * (len(mixers) + 3),
        out_specs=vm,
        scratch_shapes=[pltpu.VMEM((own, wide), f32)],
        out_shape=jax.ShapeDtypeStruct((own, wide), bf16),
        compiler_params=pltpu.CompilerParams(vmem_limit_bytes=40 * 2**20),
    )(place, arrived, *[m[0] for m in mixers], residual, gain.reshape(1, wide))


def mixers_of_all(mixer_small, mixer_large):
    half = mixer_small.shape[0]
    mine = jnp.concatenate([mixer_small, mixer_large], axis=0)
    before = shifted(mine, "tp_y", 1)
    after = shifted(mine, "tp_y", -1)
    far_small = shifted(before[:half], "tp_y", 1)
    far_large = shifted(after[half:], "tp_y", -1)
    pieces = [(mine, 0, 0), (before, -1, 0), (after, 1, 0), (far_small, 2, 0), (far_large, 2, 1)]
    here = [(a, shift, 0, first) for a, shift, first in pieces]
    there = [(shifted(a, "tp_c", 1), shift, 1, first) for a, shift, first in pieces]
    return here + there


def per_device(
    query_small,
    key_small,
    value_small,
    gates_small,
    query_large,
    key_large,
    value_large,
    gates_large,
    residual,
    mixer_small,
    mixer_large,
    mix_gain,
    value_weight,
    gate_weight,
    value_taps,
    gate_taps,
    down_weight,
    final_gain,
):
    shard_rows = query_small.shape[0]
    slot = lax.axis_index("sp_z").astype(jnp.int32)
    column = lax.axis_index("sp_x")
    depth, turns = lax.axis_size("sp_z"), lax.axis_size("sp_x")
    heads_small = gates_small.shape[1]
    heads_large = gates_large.shape[1]
    blank = jnp.zeros((8 - heads_small - heads_large, shard_rows), f32)
    own_gates = jnp.concatenate([gates_small.T, gates_large.T, blank], axis=0)
    packed, asked = pack(
        key_small, value_small, key_large, value_large, query_small, query_large, own_gates
    )
    pairs = lax.all_to_all(packed, "sp_z", split_axis=0, concat_axis=0, tiled=True)
    queries = lax.all_to_all(asked, "sp_z", split_axis=0, concat_axis=0, tiled=True)
    before = shifted(pairs, "sp_x", 1)
    after = shifted(pairs, "sp_x", -1)
    far_first = shifted(before[: depth // 2], "sp_x", 1)
    far_second = shifted(after[depth // 2 :], "sp_x", -1)
    mixers = mixers_of_all(mixer_small, mixer_large)
    whole_value, whole_gate, whole_down = gather_turned(
        (value_weight, gate_weight, down_weight), SP, (0, 0, 1)
    )
    (table,) = work_tables([(0, -1, 1, 2)], depth, turns)
    sent = attend(
        slot.reshape(1),
        lax.dynamic_index_in_dim(jnp.asarray(table), column, 0, keepdims=False),
        queries,
        [pairs, before, after, far_first, far_second],
        None,
        True,
        lax.axis_size(TP),
    )
    arrived = lax.all_to_all(sent, ("sp_z",) + TP, split_axis=0, concat_axis=0, tiled=True)
    place = jnp.stack([lax.axis_index("tp_y"), lax.axis_index("tp_c")]).astype(jnp.int32)
    arrived, whole_value, whole_gate, whole_down = lax.optimization_barrier(
        (arrived, whole_value, whole_gate, whole_down)
    )
    mixed = mix_rows(place, arrived, mixers, residual, mix_gain)
    block_input = lax.all_gather(mixed, TP, axis=0, tiled=True)
    up_value = jnp.dot(block_input, whole_value, preferred_element_type=jnp.float32)
    up_gate = jnp.dot(block_input, whole_gate, preferred_element_type=jnp.float32)
    up_value = up_value.astype(jnp.bfloat16)
    up_gate = up_gate.astype(jnp.bfloat16)
    hidden_width = up_value.shape[1]
    trailing = jnp.concatenate([up_value[-2:], up_gate[-2:]], axis=1)
    earlier = passed_along(trailing, SP, 1)
    padded_value = jnp.concatenate([earlier[:, :hidden_width], up_value], axis=0).astype(
        jnp.float32
    )
    padded_gate = jnp.concatenate([earlier[:, hidden_width:], up_gate], axis=0).astype(jnp.float32)
    filt_value = (
        value_taps[0] * padded_value[:-2]
        + value_taps[1] * padded_value[1:-1]
        + value_taps[2] * padded_value[2:]
    )
    filt_gate = (
        gate_taps[0] * padded_gate[:-2]
        + gate_taps[1] * padded_gate[1:-1]
        + gate_taps[2] * padded_gate[2:]
    )
    hidden = (jax.nn.silu(filt_gate) * filt_value).astype(jnp.bfloat16)
    turns_y, cores = lax.axis_size("tp_y"), lax.axis_size("tp_c")
    core = lax.axis_index("tp_c")
    by_core = hidden.reshape(turns_y, cores, -1, hidden_width)

    def down(which):
        rows = lax.dynamic_index_in_dim(by_core, which, 1, keepdims=False)
        return jnp.dot(rows.reshape(-1, hidden_width), whole_down, preferred_element_type=f32)

    theirs = shifted(down(1 - core).astype(bf16), "tp_c", 1)
    both = (down(core) + theirs.astype(f32)).astype(bf16)
    shares = lax.all_to_all(
        both.reshape(turns_y, -1, both.shape[1]), "tp_y", split_axis=0, concat_axis=0, tiled=True
    )
    ffn = jnp.sum(shares.astype(f32), axis=0)
    return norm_rows(residual_scale * mixed.astype(jnp.float32) + ffn, final_gain).astype(
        jnp.bfloat16
    )


def solution(mesh):
    split = Mesh(mesh.devices.reshape(4, 4, 4, 2), ALL)
    placed = (P(SP, TP),) * 8 + (
        P(ALL, None),
        P(TP, None),
        P(TP, None),
        P(),
        P(SP, TP),
        P(SP, TP),
        P(None, TP),
        P(None, TP),
        P(TP, SP),
        P(),
    )
    return jax.shard_map(
        per_device, mesh=split, in_specs=placed, out_specs=P(ALL, None), check_vma=False
    )
```

```python
import math

import jax
import jax.numpy as jnp
import numpy as np
from jax import lax
from jax.experimental import pallas as pl
from jax.experimental.pallas import tpu as pltpu
from jax.sharding import Mesh
from jax.sharding import PartitionSpec as P

SP = ("sp_z", "sp_x")
TP = ("tp_y", "tp_c")
ALL = SP + TP
bf16 = jnp.bfloat16
f32 = jnp.float32
residual_scale = 2.0**0.5
epsilon = 1e-05


def gather_turned(arrays, axis, dims):
    turned = [jnp.moveaxis(a, dim, 0) for a, dim in zip(arrays, dims)]
    widths = [t[0].size for t in turned]
    both = jnp.concatenate([t.reshape(-1, w) for t, w in zip(turned, widths)], axis=1)
    out = lax.all_gather(both, axis, axis=0, tiled=True)
    pieces = jnp.split(out, [sum(widths[:k]) for k in range(1, len(widths))], axis=1)
    return tuple(
        (
            jnp.moveaxis(b.reshape(-1, *t.shape[1:]), 0, dim)
            for b, t, dim in zip(pieces, turned, dims)
        )
    )


def shifted(value, axis, steps):
    count = lax.axis_size(axis)
    return lax.ppermute(value, axis, [(i, (i + steps) % count) for i in range(count)])


def passed_along(value, axis, steps):
    count = lax.axis_size(axis)
    first, last = (max(0, -steps), min(count, count - steps))
    return lax.ppermute(value, axis, [(source, source + steps) for source in range(first, last)])


def norm_rows(values, gain):
    center = jnp.mean(values, axis=-1, keepdims=True)
    spread = jnp.mean(jnp.square(values - center), axis=-1, keepdims=True)
    return (values - center) * lax.rsqrt(spread + epsilon) * gain


LOW = -1e30
CHUNK = 256
EXTRA = 32
STAT_ROWS = 16
RATE = 250e6


def in_pieces(value):
    high = value.astype(bf16).astype(f32)
    middle = (value - high).astype(bf16).astype(f32)
    return high, middle, value - high - middle


def cost_of(us):
    return pl.CostEstimate(flops=int(us * RATE), transcendentals=0, bytes_accessed=0)


def pack(key_small, value_small, key_large, value_large, query_small, query_large, gates):
    rows, width = key_small.shape
    half = rows // 2
    low = width // 2
    tiles = rows // width

    def body(ks, vs, kl, vl, qs, ql, g, kv, q):
        lane = lax.broadcasted_iota(jnp.int32, (rows, width), 1)
        turn = lambda ref: pltpu.roll(ref[...].astype(f32), low, 1)
        for slot in range(2):
            part = slice(slot * half, (slot + 1) * half)
            kv[slot, :half] = kl[part]
            kv[slot, half:rows] = vl[part]
            q[slot] = ql[...]
        kv[2, :rows] = jnp.where(lane < low, ks[...].astype(f32), turn(vs)).astype(bf16)
        kv[3, :rows] = jnp.where(lane < low, turn(ks), vs[...].astype(f32)).astype(bf16)
        q[2] = qs[...]
        q[3] = turn(qs).astype(bf16)
        for slot, head in ((0, 2), (1, 2), (2, 0), (3, 1)):
            blocks = []
            for piece in in_pieces(g[head : head + 1, :]):
                blocks += [piece[:, i * width : (i + 1) * width] for i in range(tiles)]
                blocks.append(jnp.zeros((8 - tiles, width), f32))
            blocks.append(jnp.zeros((EXTRA - 24, width), f32))
            kv[slot, rows:] = jnp.concatenate(blocks, axis=0).astype(bf16)

    vm = pl.BlockSpec(memory_space=pltpu.VMEM)
    return pl.pallas_call(
        body,
        in_specs=[vm] * 7,
        out_specs=[vm, vm],
        out_shape=[
            jax.ShapeDtypeStruct((4, rows + EXTRA, width), bf16),
            jax.ShapeDtypeStruct((4, rows, width), bf16),
        ],
    )(key_small, value_small, key_large, value_large, query_small, query_large, gates)


def work_tables(calls, depth, turns):
    tables = []
    for here in range(turns):
        row = []
        for shifts in calls:
            steps = []
            for z in range(depth):
                for n, shift in enumerate(shifts):
                    there = (here + shift) % turns
                    for w in range(depth):
                        key, query = w * turns + there, z * turns + here
                        if key < query:
                            steps.append((z, n * depth + w, 0))
                for n, shift in enumerate(shifts):
                    if shift == 0:
                        steps.append((z, n * depth + z, 1))
            row.append(steps)
        tables.append(row)
    longest = [max(len(tables[h][k]) for h in range(turns)) + 1 for k in range(len(calls))]
    out = []
    for k in range(len(calls)):
        table = np.zeros((turns, longest[k] * 3 + 1), np.int32)
        for h in range(turns):
            flat = np.array(tables[h][k] + [(0, 0, 0)] * (longest[k] - len(tables[h][k])), np.int32)
            table[h, :-1] = flat.reshape(-1)
            table[h, -1] = len(tables[h][k])
        out.append(table)
    return out


def attend(where, table, queries, chunks, state, final, tensor_parts, has_diagonal, cost):
    depth, rows, width = queries.shape
    half = rows // 2
    low = width // 2
    tiles = rows // width
    blocks = sum(c.shape[0] for c in chunks)
    columns = rows // CHUNK
    tall = width + 16
    last = table.shape[0] - 1
    own = rows // tensor_parts
    fresh = state is None

    def body(*refs):
        where_ref, table_ref, q_ref = refs[:3]
        chunk_refs = refs[3 : 3 + len(chunks)]
        at = 3 + len(chunks) + (0 if fresh else 2)
        state_in = () if fresh else refs[at - 2 : at]
        if final:
            out_ref = refs[at]
            acc, peak = refs[at + 1 : at + 3]
            scratch = refs[at + 3 :]
        else:
            acc, peak = refs[at : at + 2]
            scratch = refs[at + 2 :]
        qa, ka_small, va_small, ka_large, va_large, first = scratch
        slot = where_ref[0]
        count = table_ref[last]
        if fresh:
            acc[...] = jnp.zeros(acc.shape, f32)
            peak[...] = jnp.full(peak.shape, LOW, f32)
        else:
            acc[...] = state_in[0][...]
            peak[...] = state_in[1][...]

        def attention(small):
            d = low if small else width
            ext = d + 16
            span = rows if small else half
            tile = CHUNK if small else half
            parts = span // tile
            root = d**0.5
            rate = math.log2(math.e) / root
            ka, va = (ka_small, va_small) if small else (ka_large, va_large)
            deep = width if small else 2 * width
            lane = lax.broadcasted_iota(jnp.int32, (rows, width), 1)

            @pl.loop(0, depth)
            def _(z):
                q = q_ref[z]
                if small:
                    one = ((lane >= d) & (lane < d + 3)).astype(f32)
                    qa[z, :, :width] = jnp.where(lane < d, q.astype(f32), one).astype(bf16)
                else:
                    qa[z, :, :width] = q
                    qa[z, :, width:] = (lane < 3).astype(f32).astype(bf16)

            def prepare(ref, n, block):
                pieces = ref[n, rows : rows + 24].astype(f32)
                gate = pieces[0:8] + pieces[8:16] + pieces[16:24]
                bias = jnp.concatenate([gate[i : i + 1] for i in range(tiles)], axis=1) * -root
                bias = jnp.broadcast_to(bias, (8, rows))
                if not small:
                    bias = jnp.where(slot == 0, bias[:, :half], bias[:, half:])
                high, middle, rest = in_pieces(bias)
                row = lax.broadcasted_iota(jnp.int32, (8, span), 0)
                zero = jnp.zeros((8, span), f32)
                picked = jnp.where(row == 0, high, jnp.where(row == 1, middle, jnp.where(row == 2, rest, zero)))
                before = d if small else 0
                stack = [picked, jnp.zeros((width - before - 8, span), f32)]
                if before:
                    stack = [jnp.zeros((before, span), f32)] + stack
                gate_columns = jnp.concatenate(stack, axis=0).astype(bf16).T
                if small:
                    kv = ref[n, :rows]
                    ka[block] = jnp.where(lane < d, kv, gate_columns)
                    va[block, :d] = kv.T[d:]
                else:
                    ka[block, :, :width] = ref[n, :half]
                    ka[block, :, width:] = gate_columns
                    va[block, :d] = ref[n, half:rows].T
                va[block, d:] = jnp.ones((16, span), bf16)

            offset = 0
            for ref in chunk_refs:
                base = offset

                @pl.loop(0, ref.shape[0])
                def _(n):
                    prepare(ref, n, base + n)

                offset += ref.shape[0]

            def scores(z, block, c, t):
                return lax.dot_general(
                    ka[block, t * tile : (t + 1) * tile],
                    qa[z, c * CHUNK : (c + 1) * CHUNK, :deep],
                    (((1,), (1,)), ((), ())),
                    preferred_element_type=f32,
                )

            def masked(s, c, t):
                if small and t < c:
                    return s
                key = lax.broadcasted_iota(jnp.int32, (tile, CHUNK), 0) + t * tile
                if not small:
                    key = key + slot * half
                query = lax.broadcasted_iota(jnp.int32, (tile, CHUNK), 1) + c * CHUNK
                return jnp.where(key <= query, s, LOW)

            def step(n, diagonal):
                z, block = table_ref[3 * n], table_ref[3 * n + 1]
                next_z, next_block = table_ref[3 * n + 3], table_ref[3 * n + 4]
                held_count = lambda c: c + 1 if diagonal and small else parts
                held = [first[t * tile : (t + 1) * tile] for t in range(held_count(0))]
                for c in range(columns):
                    cols = slice(c * CHUNK, (c + 1) * CHUNK)
                    if diagonal:
                        held = [masked(s, c, t) for t, s in enumerate(held)]
                    top = held[0]
                    for s in held[1:]:
                        top = jnp.maximum(top, s)
                    old = peak[z, 0:1, cols]
                    new = jnp.maximum(old, jnp.max(top, axis=0, keepdims=True))
                    scaled = new * rate
                    factor = jnp.exp2(old * rate - scaled)
                    peak[z, 0:1, cols] = new
                    coming = []
                    added = None
                    following = c + 1 < columns
                    ahead = held_count(c + 1) if following else parts
                    for t in range(max(len(held), ahead)):
                        if t < ahead:
                            if following:
                                coming.append(scores(z, block, c + 1, t))
                            else:
                                first[t * tile : (t + 1) * tile] = scores(next_z, next_block, 0, t)
                        if t < len(held):
                            w = jnp.exp2(held[t] * rate - scaled).astype(bf16)
                            add = jnp.dot(
                                va[block, :, t * tile : (t + 1) * tile], w, preferred_element_type=f32
                            )
                            added = add if added is None else added + add
                    acc[z, :ext, cols] = acc[z, :ext, cols] * factor + added
                    held = coming

            for t in range(parts):
                first[t * tile : (t + 1) * tile] = scores(table_ref[0], table_ref[1], 0, t)

            @pl.loop(0, count)
            def _(n):
                if not has_diagonal:
                    step(n, False)
                    return
                diagonal = table_ref[3 * n + 2]

                @pl.when(diagonal == 0)
                def _():
                    step(n, False)

                @pl.when(diagonal == 1)
                def _():
                    step(n, True)

            if final:

                @pl.loop(0, depth)
                def _(z):
                    total = acc[z, d : d + 1]
                    out = acc[z, :d] / total
                    if small:
                        out = jnp.concatenate([out, jnp.zeros((width - d, rows), f32)], axis=0)
                    out = out.T.astype(bf16)
                    level = peak[z, 0:1] * rate + jnp.log2(total)
                    stat = jnp.concatenate([*in_pieces(level), jnp.zeros((STAT_ROWS - 3, rows), f32)], axis=0)
                    for r in range(tensor_parts):
                        out_ref[z * tensor_parts + r, :own] = out[r * own : (r + 1) * own]
                        if not small:
                            mine = stat[:, r * own : (r + 1) * own]
                            mine = jnp.concatenate([mine, jnp.zeros((STAT_ROWS, width - own), f32)], axis=1)
                            out_ref[z * tensor_parts + r, own:] = mine.astype(bf16)
                        else:
                            out_ref[z * tensor_parts + r, own:] = jnp.zeros((STAT_ROWS, width), bf16)

        @pl.when(slot < 2)
        def _():
            attention(False)

        @pl.when(slot >= 2)
        def _():
            attention(True)

    vm = pl.BlockSpec(memory_space=pltpu.VMEM)
    sm = pl.BlockSpec(memory_space=pltpu.SMEM)
    state_shapes = [((depth, tall, rows), f32), ((depth, 8, rows), f32)]
    scratch = [pltpu.VMEM(s, t) for s, t in state_shapes] if final else []
    scratch += [
        pltpu.VMEM((depth, rows, 2 * width), bf16),
        pltpu.VMEM((blocks, rows, width), bf16),
        pltpu.VMEM((blocks, low + 16, rows), bf16),
        pltpu.VMEM((blocks, half, 2 * width), bf16),
        pltpu.VMEM((blocks, tall, half), bf16),
        pltpu.VMEM((rows, CHUNK), f32),
    ]
    if final:
        out_shape = jax.ShapeDtypeStruct((depth * tensor_parts, own + STAT_ROWS, width), bf16)
        out_specs = vm
    else:
        out_shape = [jax.ShapeDtypeStruct(s, t) for s, t in state_shapes]
        out_specs = [vm, vm]
    args = [where, table, queries, *chunks] + ([] if fresh else list(state))
    return pl.pallas_call(
        body,
        in_specs=[sm, sm] + [vm] * (len(args) - 2),
        out_specs=out_specs,
        scratch_shapes=scratch,
        out_shape=out_shape,
        compiler_params=pltpu.CompilerParams(vmem_limit_bytes=58 * 2**20),
        cost_estimate=cost_of(cost),
    )(*args)


def mix_rows(place, arrived, mixers, residual, gain):
    own, wide = residual.shape
    width = arrived.shape[2]
    cores = 2
    turns = arrived.shape[0] // 4 // cores
    parts = turns * cores

    def body(place_ref, arrived_ref, *refs):
        mixer_refs = refs[: len(mixers)]
        residual_ref, gain_ref, out_ref, acc = refs[len(mixers) :]
        lane = lax.broadcasted_iota(jnp.int32, (own, width), 1)

        def level(index):
            pieces = arrived_ref[index, own:].astype(f32)
            line = pieces[0:1] + pieces[1:2] + pieces[2:3]
            return jnp.broadcast_to(line, (8, width)).T[:own, 0:1]

        def rows_of(part):
            second = pltpu.roll(arrived_ref[3 * parts + part, :own].astype(f32), width // 2, 1)
            small = jnp.where(lane < width // 2, arrived_ref[2 * parts + part, :own].astype(f32), second)
            share = 1.0 / (1.0 + jnp.exp2(level(part) - level(parts + part)))
            large = arrived_ref[part, :own].astype(f32) * (1.0 - share) + arrived_ref[
                parts + part, :own
            ].astype(f32) * share
            return small.astype(bf16), large.astype(bf16)

        acc[...] = residual_ref[...].astype(f32) * residual_scale
        for ref, (_, shift, other, first) in zip(mixer_refs, mixers):
            y = lax.rem(place_ref[0] + shift + turns, turns)
            core = place_ref[1] if other == 0 else 1 - place_ref[1]
            both = rows_of(y * cores + core)
            if ref.shape[0] == 2 * width:
                left = jnp.concatenate(both, axis=1)
            else:
                left = both[first]
            acc[...] += jnp.dot(left, ref[...], preferred_element_type=f32)
        values = acc[...]
        center = jnp.mean(values, axis=-1, keepdims=True)
        values = values - center
        spread = jnp.mean(jnp.square(values), axis=-1, keepdims=True)
        out_ref[...] = (values * lax.rsqrt(spread + epsilon) * gain_ref[...]).astype(bf16)

    vm = pl.BlockSpec(memory_space=pltpu.VMEM)
    return pl.pallas_call(
        body,
        in_specs=[pl.BlockSpec(memory_space=pltpu.SMEM)] + [vm] * (len(mixers) + 3),
        out_specs=vm,
        scratch_shapes=[pltpu.VMEM((own, wide), f32)],
        out_shape=jax.ShapeDtypeStruct((own, wide), bf16),
        compiler_params=pltpu.CompilerParams(vmem_limit_bytes=40 * 2**20),
    )(place, arrived, *[m[0] for m in mixers], residual, gain.reshape(1, wide))


def mixers_of_all(mixer_small, mixer_large):
    half = mixer_small.shape[0]
    mine = jnp.concatenate([mixer_small, mixer_large], axis=0)
    before = shifted(mine, "tp_y", 1)
    after = shifted(mine, "tp_y", -1)
    far_small = shifted(before[:half], "tp_y", 1)
    far_large = shifted(after[half:], "tp_y", -1)
    pieces = [(mine, 0, 0), (before, -1, 0), (after, 1, 0), (far_small, 2, 0), (far_large, 2, 1)]
    here = [(a, shift, 0, first) for a, shift, first in pieces]
    there = [(shifted(a, "tp_c", 1), shift, 1, first) for a, shift, first in pieces]
    return here + there


def per_device(
    query_small,
    key_small,
    value_small,
    gates_small,
    query_large,
    key_large,
    value_large,
    gates_large,
    residual,
    mixer_small,
    mixer_large,
    mix_gain,
    value_weight,
    gate_weight,
    value_taps,
    gate_taps,
    down_weight,
    final_gain,
):
    shard_rows = query_small.shape[0]
    slot = lax.axis_index("sp_z").astype(jnp.int32)
    column = lax.axis_index("sp_x")
    depth, turns = lax.axis_size("sp_z"), lax.axis_size("sp_x")
    heads_small = gates_small.shape[1]
    heads_large = gates_large.shape[1]
    blank = jnp.zeros((8 - heads_small - heads_large, shard_rows), f32)
    own_gates = jnp.concatenate([gates_small.T, gates_large.T, blank], axis=0)
    packed, asked = pack(
        key_small, value_small, key_large, value_large, query_small, query_large, own_gates
    )
    pairs = lax.all_to_all(packed, "sp_z", split_axis=0, concat_axis=0, tiled=True)
    queries = lax.all_to_all(asked, "sp_z", split_axis=0, concat_axis=0, tiled=True)
    before = shifted(pairs, "sp_x", 1)
    after = shifted(pairs, "sp_x", -1)
    far_first = shifted(before[: depth // 2], "sp_x", 1)
    far_second = shifted(after[depth // 2 :], "sp_x", -1)
    mixers = mixers_of_all(mixer_small, mixer_large)
    whole_value, whole_gate, whole_down = gather_turned(
        (value_weight, gate_weight, down_weight), SP, (0, 0, 1)
    )
    calls = ((0,), (-1, 1), (2,))
    state = None
    for k, (table, chunks) in enumerate(
        zip(work_tables(calls, depth, turns), ([pairs], [before, after], [far_first, far_second]))
    ):
        state = attend(
            slot.reshape(1),
            lax.dynamic_index_in_dim(jnp.asarray(table), column, 0, keepdims=False),
            queries,
            chunks,
            state,
            k + 1 == len(calls),
            lax.axis_size(TP),
            0 in calls[k],
            12.0 * len(calls[k]),
        )
    arrived = lax.all_to_all(state, ("sp_z",) + TP, split_axis=0, concat_axis=0, tiled=True)
    place = jnp.stack([lax.axis_index("tp_y"), lax.axis_index("tp_c")]).astype(jnp.int32)
    arrived, whole_value, whole_gate, whole_down = lax.optimization_barrier(
        (arrived, whole_value, whole_gate, whole_down)
    )
    mixed = mix_rows(place, arrived, mixers, residual, mix_gain)
    block_input = lax.all_gather(mixed, TP, axis=0, tiled=True)
    up_value = jnp.dot(block_input, whole_value, preferred_element_type=jnp.float32)
    up_gate = jnp.dot(block_input, whole_gate, preferred_element_type=jnp.float32)
    up_value = up_value.astype(jnp.bfloat16)
    up_gate = up_gate.astype(jnp.bfloat16)
    hidden_width = up_value.shape[1]
    trailing = jnp.concatenate([up_value[-2:], up_gate[-2:]], axis=1)
    earlier = passed_along(trailing, SP, 1)
    padded_value = jnp.concatenate([earlier[:, :hidden_width], up_value], axis=0).astype(
        jnp.float32
    )
    padded_gate = jnp.concatenate([earlier[:, hidden_width:], up_gate], axis=0).astype(jnp.float32)
    filt_value = (
        value_taps[0] * padded_value[:-2]
        + value_taps[1] * padded_value[1:-1]
        + value_taps[2] * padded_value[2:]
    )
    filt_gate = (
        gate_taps[0] * padded_gate[:-2]
        + gate_taps[1] * padded_gate[1:-1]
        + gate_taps[2] * padded_gate[2:]
    )
    hidden = (jax.nn.silu(filt_gate) * filt_value).astype(jnp.bfloat16)
    turns_y, cores = lax.axis_size("tp_y"), lax.axis_size("tp_c")
    core = lax.axis_index("tp_c")
    by_core = hidden.reshape(turns_y, cores, -1, hidden_width)

    def down(which):
        rows = lax.dynamic_index_in_dim(by_core, which, 1, keepdims=False)
        return jnp.dot(rows.reshape(-1, hidden_width), whole_down, preferred_element_type=f32)

    theirs = shifted(down(1 - core).astype(bf16), "tp_c", 1)
    both = (down(core) + theirs.astype(f32)).astype(bf16)
    shares = lax.all_to_all(
        both.reshape(turns_y, -1, both.shape[1]), "tp_y", split_axis=0, concat_axis=0, tiled=True
    )
    ffn = jnp.sum(shares.astype(f32), axis=0)
    return norm_rows(residual_scale * mixed.astype(jnp.float32) + ffn, final_gain).astype(
        jnp.bfloat16
    )


def solution(mesh):
    split = Mesh(mesh.devices.reshape(4, 4, 4, 2), ALL)
    placed = (P(SP, TP),) * 8 + (
        P(ALL, None),
        P(TP, None),
        P(TP, None),
        P(),
        P(SP, TP),
        P(SP, TP),
        P(None, TP),
        P(None, TP),
        P(TP, SP),
        P(),
    )
    return jax.shard_map(
        per_device, mesh=split, in_specs=placed, out_specs=P(ALL, None), check_vma=False
    )
```

```python
import math

import jax
import jax.numpy as jnp
import numpy as np
from jax import lax
from jax.experimental import pallas as pl
from jax.experimental.pallas import tpu as pltpu
from jax.sharding import Mesh
from jax.sharding import PartitionSpec as P

SP = ("sp_z", "sp_x")
TP = ("tp_y", "tp_c")
ALL = SP + TP
bf16 = jnp.bfloat16
f32 = jnp.float32
residual_scale = 2.0**0.5
epsilon = 1e-05


def gather_turned(arrays, axis, dims):
    turned = [jnp.moveaxis(a, dim, 0) for a, dim in zip(arrays, dims)]
    widths = [t[0].size for t in turned]
    both = jnp.concatenate([t.reshape(-1, w) for t, w in zip(turned, widths)], axis=1)
    out = lax.all_gather(both, axis, axis=0, tiled=True)
    pieces = jnp.split(out, [sum(widths[:k]) for k in range(1, len(widths))], axis=1)
    return tuple(
        (
            jnp.moveaxis(b.reshape(-1, *t.shape[1:]), 0, dim)
            for b, t, dim in zip(pieces, turned, dims)
        )
    )


def shifted(value, axis, steps):
    count = lax.axis_size(axis)
    return lax.ppermute(value, axis, [(i, (i + steps) % count) for i in range(count)])


def passed_along(value, axis, steps):
    count = lax.axis_size(axis)
    first, last = (max(0, -steps), min(count, count - steps))
    return lax.ppermute(value, axis, [(source, source + steps) for source in range(first, last)])


LOW = -1e30
CHUNK = 256
EXTRA = 32
STAT_ROWS = 16
RATE = 250e6


def in_pieces(value):
    high = value.astype(bf16).astype(f32)
    middle = (value - high).astype(bf16).astype(f32)
    return high, middle, value - high - middle


def cost_of(us):
    return pl.CostEstimate(flops=int(us * RATE), transcendentals=0, bytes_accessed=0)


def pack(slot, key_small, value_small, key_large, value_large, query_small, query_large, gates):
    rows, width = key_small.shape
    half = rows // 2
    low = width // 2
    tiles = rows // width

    def body(slot_ref, ks, vs, kl, vl, qs, ql, g, kv, *q):
        lane = lax.broadcasted_iota(jnp.int32, (rows, width), 1)
        turn = lambda ref: pltpu.roll(ref[...].astype(f32), low, 1)
        for slot in range(2):
            part = slice(slot * half, (slot + 1) * half)
            kv[slot, :half] = kl[part]
            kv[slot, half:rows] = vl[part]
        kv[2, :rows] = jnp.where(lane < low, ks[...].astype(f32), turn(vs)).astype(bf16)
        kv[3, :rows] = jnp.where(lane < low, turn(ks), vs[...].astype(f32)).astype(bf16)
        for shift in range(4):
            target = lax.rem(slot_ref[0] + shift, 4)

            @pl.when(target < 2)
            def _():
                q[shift][...] = ql[...]

            @pl.when(target == 2)
            def _():
                q[shift][...] = qs[...]

            @pl.when(target == 3)
            def _():
                q[shift][...] = turn(qs).astype(bf16)

        for slot, head in ((0, 2), (1, 2), (2, 0), (3, 1)):
            blocks = []
            for piece in in_pieces(g[head : head + 1, :]):
                blocks += [piece[:, i * width : (i + 1) * width] for i in range(tiles)]
                blocks.append(jnp.zeros((8 - tiles, width), f32))
            blocks.append(jnp.zeros((EXTRA - 24, width), f32))
            kv[slot, rows:] = jnp.concatenate(blocks, axis=0).astype(bf16)

    vm = pl.BlockSpec(memory_space=pltpu.VMEM)
    return pl.pallas_call(
        body,
        in_specs=[pl.BlockSpec(memory_space=pltpu.SMEM)] + [vm] * 7,
        out_specs=[vm] * 5,
        out_shape=[jax.ShapeDtypeStruct((4, rows + EXTRA, width), bf16)]
        + [jax.ShapeDtypeStruct((rows, width), bf16)] * 4,
        cost_estimate=cost_of(2.5),
    )(slot, key_small, value_small, key_large, value_large, query_small, query_large, gates)


def work_tables(calls, depth, turns):
    tables = []
    for here in range(turns):
        row = []
        for shifts in calls:
            steps = []
            for z in range(depth):
                for n, shift in enumerate(shifts):
                    there = (here + shift) % turns
                    for w in range(depth):
                        key, query = w * turns + there, z * turns + here
                        if key < query:
                            steps.append((z, n * depth + w, 0))
                for n, shift in enumerate(shifts):
                    if shift == 0:
                        steps.append((z, n * depth + z, 1))
            row.append(steps)
        tables.append(row)
    longest = [max(len(tables[h][k]) for h in range(turns)) + 1 for k in range(len(calls))]
    out = []
    for k in range(len(calls)):
        table = np.zeros((turns, longest[k] * 3 + 1), np.int32)
        for h in range(turns):
            flat = np.array(tables[h][k] + [(0, 0, 0)] * (longest[k] - len(tables[h][k])), np.int32)
            table[h, :-1] = flat.reshape(-1)
            table[h, -1] = len(tables[h][k])
        out.append(table)
    return out


def attend(where, table, queries, chunks, state, final, tensor_parts, has_diagonal, cost):
    depth = len(queries)
    rows, width = queries[0].shape
    half = rows // 2
    low = width // 2
    tiles = rows // width
    blocks = sum(c.shape[0] for c in chunks)
    columns = rows // CHUNK
    tall = width + 16
    last = table.shape[1] - 1
    own = rows // tensor_parts
    fresh = state is None

    def body(*refs):
        where_ref, table_ref = refs[:2]
        q_refs = refs[2 : 2 + depth]
        chunk_refs = refs[2 + depth : 2 + depth + len(chunks)]
        at = 2 + depth + len(chunks) + (0 if fresh else 2)
        state_in = () if fresh else refs[at - 2 : at]
        if final:
            out_ref = refs[at]
            acc, peak = refs[at + 1 : at + 3]
            scratch = refs[at + 3 :]
        else:
            acc, peak = refs[at : at + 2]
            scratch = refs[at + 2 :]
        qa, ka_small, va_small, ka_large, va_large, first = scratch
        slot = where_ref[0]
        column = where_ref[1]
        count = table_ref[column, last]

        @pl.loop(0, depth)
        def _(z):
            if fresh:
                acc[z] = jnp.zeros(acc.shape[1:], f32)
                peak[z] = jnp.full(peak.shape[1:], LOW, f32)
            else:
                acc[z] = state_in[0][z]
                peak[z] = state_in[1][z]

        def attention(small):
            d = low if small else width
            ext = d + 16
            span = rows if small else half
            tile = CHUNK if small else half
            parts = span // tile
            root = d**0.5
            rate = math.log2(math.e) / root
            ka, va = (ka_small, va_small) if small else (ka_large, va_large)
            deep = width if small else 2 * width
            lane = lax.broadcasted_iota(jnp.int32, (rows, width), 1)

            for shift, q_ref in enumerate(q_refs):
                z = lax.rem(slot + depth - shift, depth)
                q = q_ref[...]
                if small:
                    one = ((lane >= d) & (lane < d + 3)).astype(f32)
                    qa[z, :, :width] = jnp.where(lane < d, q.astype(f32), one).astype(bf16)
                else:
                    qa[z, :, :width] = q
                    qa[z, :, width:] = (lane < 3).astype(f32).astype(bf16)

            def prepare(ref, n, block):
                pieces = ref[n, rows : rows + 24].astype(f32)
                gate = pieces[0:8] + pieces[8:16] + pieces[16:24]
                bias = jnp.concatenate([gate[i : i + 1] for i in range(tiles)], axis=1) * -root
                bias = jnp.broadcast_to(bias, (8, rows))
                if not small:
                    bias = jnp.where(slot == 0, bias[:, :half], bias[:, half:])
                high, middle, rest = in_pieces(bias)
                row = lax.broadcasted_iota(jnp.int32, (8, span), 0)
                zero = jnp.zeros((8, span), f32)
                picked = jnp.where(row == 0, high, jnp.where(row == 1, middle, jnp.where(row == 2, rest, zero)))
                before = d if small else 0
                stack = [picked, jnp.zeros((width - before - 8, span), f32)]
                if before:
                    stack = [jnp.zeros((before, span), f32)] + stack
                gate_columns = jnp.concatenate(stack, axis=0).astype(bf16).T
                if small:
                    kv = ref[n, :rows]
                    ka[block] = jnp.where(lane < d, kv, gate_columns)
                    va[block, :d] = kv.T[d:]
                else:
                    ka[block, :, :width] = ref[n, :half]
                    ka[block, :, width:] = gate_columns
                    va[block, :d] = ref[n, half:rows].T
                va[block, d:] = jnp.ones((16, span), bf16)

            offset = 0
            for ref in chunk_refs:
                base = offset

                @pl.loop(0, ref.shape[0])
                def _(n):
                    prepare(ref, n, base + n)

                offset += ref.shape[0]

            def scores(z, block, c, t):
                return lax.dot_general(
                    ka[block, t * tile : (t + 1) * tile],
                    qa[z, c * CHUNK : (c + 1) * CHUNK, :deep],
                    (((1,), (1,)), ((), ())),
                    preferred_element_type=f32,
                )

            def masked(s, c, t):
                if small and t < c:
                    return s
                key = lax.broadcasted_iota(jnp.int32, (tile, CHUNK), 0) + t * tile
                if not small:
                    key = key + slot * half
                query = lax.broadcasted_iota(jnp.int32, (tile, CHUNK), 1) + c * CHUNK
                return jnp.where(key <= query, s, LOW)

            def step(n, diagonal):
                z, block = table_ref[column, 3 * n], table_ref[column, 3 * n + 1]
                next_z, next_block = table_ref[column, 3 * n + 3], table_ref[column, 3 * n + 4]
                held_count = lambda c: c + 1 if diagonal and small else parts
                held = [first[t * tile : (t + 1) * tile] for t in range(held_count(0))]
                for c in range(columns):
                    cols = slice(c * CHUNK, (c + 1) * CHUNK)
                    if diagonal:
                        held = [masked(s, c, t) for t, s in enumerate(held)]
                    top = held[0]
                    for s in held[1:]:
                        top = jnp.maximum(top, s)
                    old = peak[z, 0:1, cols]
                    new = jnp.maximum(old, jnp.max(top, axis=0, keepdims=True))
                    scaled = new * rate
                    factor = jnp.exp2(old * rate - scaled)
                    peak[z, 0:1, cols] = new
                    coming = []
                    added = None
                    following = c + 1 < columns
                    ahead = held_count(c + 1) if following else parts
                    for t in range(max(len(held), ahead)):
                        if t < ahead:
                            if following:
                                coming.append(scores(z, block, c + 1, t))
                            else:
                                first[t * tile : (t + 1) * tile] = scores(next_z, next_block, 0, t)
                        if t < len(held):
                            w = jnp.exp2(held[t] * rate - scaled).astype(bf16)
                            add = jnp.dot(
                                va[block, :, t * tile : (t + 1) * tile], w, preferred_element_type=f32
                            )
                            added = add if added is None else added + add
                    acc[z, :ext, cols] = acc[z, :ext, cols] * factor + added
                    held = coming

            for t in range(parts):
                first[t * tile : (t + 1) * tile] = scores(table_ref[column, 0], table_ref[column, 1], 0, t)

            @pl.loop(0, count)
            def _(n):
                if not has_diagonal:
                    step(n, False)
                    return
                diagonal = table_ref[column, 3 * n + 2]

                @pl.when(diagonal == 0)
                def _():
                    step(n, False)

                @pl.when(diagonal == 1)
                def _():
                    step(n, True)

            if final:

                @pl.loop(0, depth)
                def _(z):
                    total = acc[z, d : d + 1]
                    out = acc[z, :d] / total
                    if small:
                        out = jnp.concatenate([out, jnp.zeros((width - d, rows), f32)], axis=0)
                    out = out.T.astype(bf16)
                    level = peak[z, 0:1] * rate + jnp.log2(total)
                    stat = jnp.concatenate([*in_pieces(level), jnp.zeros((STAT_ROWS - 3, rows), f32)], axis=0)
                    for r in range(tensor_parts):
                        out_ref[z * tensor_parts + r, :own] = out[r * own : (r + 1) * own]
                        if not small:
                            mine = stat[:, r * own : (r + 1) * own]
                            mine = jnp.concatenate([mine, jnp.zeros((STAT_ROWS, width - own), f32)], axis=1)
                            out_ref[z * tensor_parts + r, own:] = mine.astype(bf16)
                        else:
                            out_ref[z * tensor_parts + r, own:] = jnp.zeros((STAT_ROWS, width), bf16)

        @pl.when(slot < 2)
        def _():
            attention(False)

        @pl.when(slot >= 2)
        def _():
            attention(True)

    vm = pl.BlockSpec(memory_space=pltpu.VMEM)
    sm = pl.BlockSpec(memory_space=pltpu.SMEM)
    state_shapes = [((depth, tall, rows), f32), ((depth, 8, rows), f32)]
    scratch = [pltpu.VMEM(s, t) for s, t in state_shapes] if final else []
    scratch += [
        pltpu.VMEM((depth, rows, 2 * width), bf16),
        pltpu.VMEM((blocks, rows, width), bf16),
        pltpu.VMEM((blocks, low + 16, rows), bf16),
        pltpu.VMEM((blocks, half, 2 * width), bf16),
        pltpu.VMEM((blocks, tall, half), bf16),
        pltpu.VMEM((rows, CHUNK), f32),
    ]
    if final:
        out_shape = jax.ShapeDtypeStruct((depth * tensor_parts, own + STAT_ROWS, width), bf16)
        out_specs = vm
    else:
        out_shape = [jax.ShapeDtypeStruct(s, t) for s, t in state_shapes]
        out_specs = [vm, vm]
    args = [where, table, *queries, *chunks] + ([] if fresh else list(state))
    return pl.pallas_call(
        body,
        in_specs=[sm, sm] + [vm] * (len(args) - 2),
        out_specs=out_specs,
        scratch_shapes=scratch,
        out_shape=out_shape,
        compiler_params=pltpu.CompilerParams(vmem_limit_bytes=58 * 2**20),
        cost_estimate=cost_of(cost),
    )(*args)


def mix_rows(place, arrived, mixers, residual, gain):
    own, wide = residual.shape
    width = arrived.shape[2]
    cores = 2
    turns = arrived.shape[0] // 4 // cores
    parts = turns * cores

    def body(place_ref, arrived_ref, *refs):
        mixer_refs = refs[: len(mixers)]
        residual_ref, gain_ref, out_ref, acc = refs[len(mixers) :]
        lane = lax.broadcasted_iota(jnp.int32, (own, width), 1)

        def level(index):
            pieces = arrived_ref[index, own:].astype(f32)
            line = pieces[0:1] + pieces[1:2] + pieces[2:3]
            return jnp.broadcast_to(line, (8, width)).T[:own, 0:1]

        def rows_of(part):
            second = pltpu.roll(arrived_ref[3 * parts + part, :own].astype(f32), width // 2, 1)
            small = jnp.where(lane < width // 2, arrived_ref[2 * parts + part, :own].astype(f32), second)
            share = 1.0 / (1.0 + jnp.exp2(level(part) - level(parts + part)))
            large = arrived_ref[part, :own].astype(f32) * (1.0 - share) + arrived_ref[
                parts + part, :own
            ].astype(f32) * share
            return small.astype(bf16), large.astype(bf16)

        acc[...] = residual_ref[...].astype(f32) * residual_scale
        for ref, (_, shift, other) in zip(mixer_refs, mixers):
            y = lax.rem(place_ref[0] + shift + turns, turns)
            core = place_ref[1] if other == 0 else 1 - place_ref[1]
            both = rows_of(y * cores + core)
            acc[...] += jnp.dot(jnp.concatenate(both, axis=1), ref[...], preferred_element_type=f32)
        values = acc[...]
        center = jnp.mean(values, axis=-1, keepdims=True)
        values = values - center
        spread = jnp.mean(jnp.square(values), axis=-1, keepdims=True)
        out_ref[...] = (values * lax.rsqrt(spread + epsilon) * gain_ref[...]).astype(bf16)

    vm = pl.BlockSpec(memory_space=pltpu.VMEM)
    return pl.pallas_call(
        body,
        in_specs=[pl.BlockSpec(memory_space=pltpu.SMEM)] + [vm] * (len(mixers) + 3),
        out_specs=vm,
        scratch_shapes=[pltpu.VMEM((own, wide), f32)],
        out_shape=jax.ShapeDtypeStruct((own, wide), bf16),
        compiler_params=pltpu.CompilerParams(vmem_limit_bytes=40 * 2**20),
        cost_estimate=cost_of(5.0),
    )(place, arrived, *[m[0] for m in mixers], residual, gain.reshape(1, wide))


def ups(chunks, value_weight, gate_weight, cost):
    width = value_weight.shape[1]
    rows = sum(c.shape[0] for c in chunks)

    def body(*refs):
        value_ref, gate_ref, out_value, out_gate = refs[len(chunks) :]
        x = jnp.concatenate([r[...] for r in refs[: len(chunks)]], axis=0)
        out_value[...] = jnp.dot(x, value_ref[...], preferred_element_type=f32).astype(bf16)
        out_gate[...] = jnp.dot(x, gate_ref[...], preferred_element_type=f32).astype(bf16)

    vm = pl.BlockSpec(memory_space=pltpu.VMEM)
    return pl.pallas_call(
        body,
        in_specs=[vm] * (len(chunks) + 2),
        out_specs=[vm, vm],
        out_shape=[jax.ShapeDtypeStruct((rows, width), bf16)] * 2,
        compiler_params=pltpu.CompilerParams(vmem_limit_bytes=40 * 2**20),
        cost_estimate=cost_of(cost),
    )(*chunks, value_weight, gate_weight)


LEAD = 16


def last_ups(place, chunks, value_weight, gate_weight, earlier, spots, turns, cores):
    own = chunks[0].shape[0]
    width = value_weight.shape[1]
    total = LEAD + turns * cores * own

    def body(place_ref, *refs):
        chunk_refs = refs[: len(chunks)]
        value_ref, gate_ref = refs[len(chunks) : len(chunks) + 2]
        done = refs[len(chunks) + 2 : -4]
        outs, tails = refs[-4:-2], refs[-2:]
        x = jnp.concatenate([r[...] for r in chunk_refs], axis=0)
        fresh = [
            jnp.dot(x, w[...], preferred_element_type=f32).astype(bf16) for w in (value_ref, gate_ref)
        ]
        parts = []
        for k in range(0, len(done), 2):
            for i in range(done[k].shape[0] // own):
                parts.append([done[k + side][i * own : (i + 1) * own] for side in range(2)])
        for i in range(len(chunks)):
            parts.append([f[i * own : (i + 1) * own] for f in fresh])
        for out in outs:
            out[:LEAD] = jnp.zeros((LEAD, width), bf16)
        for part, (shift, other) in zip(parts, spots):
            y = lax.rem(place_ref[0] + shift + turns, turns)
            core = place_ref[1] if other == 0 else 1 - place_ref[1]
            at = pl.multiple_of(LEAD + (y * cores + core) * own, LEAD)
            for out, rows in zip(outs, part):
                out[pl.ds(at, own)] = rows
        for out, tail in zip(outs, tails):
            tail[...] = out[total - LEAD :]

    vm = pl.BlockSpec(memory_space=pltpu.VMEM)
    flat = [a for pair in earlier for a in pair]
    return pl.pallas_call(
        body,
        in_specs=[pl.BlockSpec(memory_space=pltpu.SMEM)] + [vm] * (len(chunks) + 2 + len(flat)),
        out_specs=[vm] * 4,
        out_shape=[jax.ShapeDtypeStruct((total, width), bf16)] * 2
        + [jax.ShapeDtypeStruct((LEAD, width), bf16)] * 2,
        compiler_params=pltpu.CompilerParams(vmem_limit_bytes=50 * 2**20),
        cost_estimate=cost_of(4.0),
    )(place, *chunks, value_weight, gate_weight, *flat)


def downs(place, up_value, up_gate, halos, value_taps, gate_taps, down_weight, first, count, own, cores, cost):
    width = up_value.shape[1]
    wide = down_weight.shape[1]

    def body(place_ref, *refs):
        value_ref, gate_ref, vt_ref, gt_ref, down_ref = refs[:5]
        halo_refs = refs[5 : 5 + len(halos)]
        theirs, mine, hidden, terms = refs[5 + len(halos) :]

        def filtered(ref, taps, halo, at, start):
            rows = ref[pl.ds(at, own + LEAD)].astype(f32)
            if halo is not None:
                before = jnp.where(start, halo[...].astype(f32), rows[:LEAD])
                rows = jnp.concatenate([before, rows[LEAD:]], axis=0)
            two = pltpu.roll(rows, 2, 0)[LEAD:]
            one = pltpu.roll(rows, 1, 0)[LEAD:]
            return taps[0:1] * two + taps[1:2] * one + taps[2:3] * rows[LEAD:]

        @pl.loop(0, 2)
        def _(which):
            core = jnp.where(which == 0, 1 - place_ref[1], place_ref[1])

            @pl.loop(0, count)
            def _(i):
                part = (first + i) * cores + core
                at = pl.multiple_of(part * own, LEAD)
                start = part == 0
                value_halo, gate_halo = halo_refs if halos else (None, None)
                value = filtered(value_ref, vt_ref, value_halo, at, start)
                gate = filtered(gate_ref, gt_ref, gate_halo, at, start)
                rows = pl.ds(pl.multiple_of(i * own, LEAD), own)
                hidden[rows] = (gate / (1.0 + jnp.exp(-gate)) * value).astype(bf16)

            terms[...] = jnp.dot(hidden[...], down_ref[...], preferred_element_type=f32)
            for own_turn, out in enumerate((theirs, mine)):

                @pl.when(which == own_turn)
                def _():
                    @pl.loop(0, count)
                    def _(i):
                        rows = pl.ds(pl.multiple_of(i * own, LEAD), own)
                        out[i] = terms[rows].astype(out.dtype)


    vm = pl.BlockSpec(memory_space=pltpu.VMEM)
    shape = (count, own, wide)
    return pl.pallas_call(
        body,
        in_specs=[pl.BlockSpec(memory_space=pltpu.SMEM)] + [vm] * (5 + len(halos)),
        out_specs=[vm, vm],
        out_shape=[jax.ShapeDtypeStruct(shape, bf16), jax.ShapeDtypeStruct(shape, f32)],
        scratch_shapes=[pltpu.VMEM((count * own, width), bf16), pltpu.VMEM((count * own, wide), f32)],
        compiler_params=pltpu.CompilerParams(vmem_limit_bytes=50 * 2**20),
        cost_estimate=cost_of(cost),
    )(place, up_value, up_gate, value_taps, gate_taps, down_weight, *halos)


def paired(place, mine, theirs):
    own, wide = mine[0].shape[1:]
    turns = sum(m.shape[0] for m in mine)

    def body(place_ref, *refs):
        mine_refs, their_refs = refs[: len(mine)], refs[len(mine) : 2 * len(mine)]
        outs = refs[2 * len(mine) :]
        for k, out in enumerate(outs):
            group = lax.rem(place_ref[0] + k, turns)
            first = 0
            for m, t in zip(mine_refs, their_refs):
                at, count = group - first, m.shape[0]

                @pl.when((at >= 0) & (at < count))
                def _():
                    out[...] = (m[at] + t[at].astype(f32)).astype(out.dtype)

                first += count

    vm = pl.BlockSpec(memory_space=pltpu.VMEM)
    return pl.pallas_call(
        body,
        in_specs=[pl.BlockSpec(memory_space=pltpu.SMEM)] + [vm] * (2 * len(mine)),
        out_specs=[vm] * turns,
        out_shape=[jax.ShapeDtypeStruct((own, wide), f32 if k == 0 else bf16) for k in range(turns)],
        cost_estimate=cost_of(2.0),
    )(place, *mine, *theirs)


def finish(mixed, own, shares, gain):
    rows, wide = mixed.shape

    def body(*refs):
        mixed_ref, own_ref = refs[:2]
        gain_ref, out_ref = refs[-2:]
        total = own_ref[...]
        for r in refs[2:-2]:
            total = total + r[...].astype(f32)
        values = residual_scale * mixed_ref[...].astype(f32) + total
        center = jnp.mean(values, axis=-1, keepdims=True)
        values = values - center
        spread = jnp.mean(jnp.square(values), axis=-1, keepdims=True)
        out_ref[...] = (values * lax.rsqrt(spread + epsilon) * gain_ref[...]).astype(bf16)

    vm = pl.BlockSpec(memory_space=pltpu.VMEM)
    return pl.pallas_call(
        body,
        in_specs=[vm] * (3 + len(shares)),
        out_specs=vm,
        out_shape=jax.ShapeDtypeStruct((rows, wide), bf16),
        cost_estimate=cost_of(2.0),
    )(mixed, own, *shares, gain.reshape(1, wide))


def per_device(
    query_small,
    key_small,
    value_small,
    gates_small,
    query_large,
    key_large,
    value_large,
    gates_large,
    residual,
    mixer_small,
    mixer_large,
    mix_gain,
    value_weight,
    gate_weight,
    value_taps,
    gate_taps,
    down_weight,
    final_gain,
):
    shard_rows = query_small.shape[0]
    slot = lax.axis_index("sp_z").astype(jnp.int32)
    column = lax.axis_index("sp_x").astype(jnp.int32)
    depth, turns = lax.axis_size("sp_z"), lax.axis_size("sp_x")
    heads_small = gates_small.shape[1]
    heads_large = gates_large.shape[1]
    blank = jnp.zeros((8 - heads_small - heads_large, shard_rows), f32)
    own_gates = jnp.concatenate([gates_small.T, gates_large.T, blank], axis=0)
    packed, *asked = pack(
        slot.reshape(1),
        key_small,
        value_small,
        key_large,
        value_large,
        query_small,
        query_large,
        own_gates,
    )
    packed, value_weight, gate_weight, down_weight = lax.optimization_barrier(
        (packed, value_weight, gate_weight, down_weight)
    )
    pairs = lax.all_to_all(packed, "sp_z", split_axis=0, concat_axis=0, tiled=True)
    queries = [asked[0]] + [shifted(asked[k], "sp_z", k) for k in range(1, depth)]
    pairs, *queries = lax.optimization_barrier((pairs, *queries))
    before = shifted(pairs, "sp_x", 1)
    after = shifted(pairs, "sp_x", -1)
    mixer = jnp.concatenate([mixer_small, mixer_large], axis=0)
    mixers = [mixer, shifted(mixer, "tp_y", 1), shifted(mixer, "tp_y", -1)]
    whole_value, whole_gate, whole_down = gather_turned(
        (value_weight, gate_weight, down_weight), SP, (0, 0, 1)
    )
    calls = ((0,), (-1, 1), (2,))
    tables = work_tables(calls, depth, turns)
    place_here = jnp.stack([slot, column])
    call = lambda k, chunks, state: attend(
        place_here,
        jnp.asarray(tables[k]),
        queries,
        chunks,
        state,
        k + 1 == len(calls),
        lax.axis_size(TP),
        0 in calls[k],
        12.0 * len(calls[k]),
    )
    state = call(0, [pairs], None)
    before, state, mixers = lax.optimization_barrier((before, state, mixers))
    far = shifted(before, "sp_x", 1)
    mixers.append(shifted(mixers[1], "tp_y", 1))
    state = call(1, [before, after], state)
    far, state, mixers = lax.optimization_barrier((far, state, mixers))
    shifts = (0, -1, 1, 2)
    mixers = [(a, shift, 0) for a, shift in zip(mixers, shifts)] + [
        (shifted(a, "tp_c", 1), shift, 1) for a, shift in zip(mixers, shifts)
    ]
    state = call(2, [far], state)
    arrived = lax.all_to_all(state, ("sp_z",) + TP, split_axis=0, concat_axis=0, tiled=True)
    place = jnp.stack([lax.axis_index("tp_y"), lax.axis_index("tp_c")]).astype(jnp.int32)
    arrived, whole_value, whole_gate, whole_down = lax.optimization_barrier(
        (arrived, whole_value, whole_gate, whole_down)
    )
    mixed = mix_rows(place, arrived, mixers, residual, mix_gain)
    turns_y, cores = lax.axis_size("tp_y"), lax.axis_size("tp_c")
    near = [mixed, shifted(mixed, "tp_c", 1)]
    next_ones = [shifted(mixed, "tp_y", 1), shifted(mixed, "tp_y", -1)]
    opposite = shifted(mixed, "tp_y", 2)
    next_ones += [shifted(a, "tp_c", 1) for a in next_ones]
    last_ones = [opposite, shifted(opposite, "tp_c", 1)]
    spots = [(0, 0), (0, 1), (-1, 0), (1, 0), (-1, 1), (1, 1), (2, 0), (2, 1)]
    earlier = [ups(near, whole_value, whole_gate, 3.0), ups(next_ones, whole_value, whole_gate, 4.0)]
    up_value, up_gate, *tails = last_ups(
        place, last_ones, whole_value, whole_gate, earlier, spots, turns_y, cores
    )
    halos = [passed_along(t, SP, 1) for t in tails]
    down = lambda halo, first, count, cost: downs(
        place,
        up_value,
        up_gate,
        halo,
        value_taps,
        gate_taps,
        whole_down,
        first,
        count,
        mixed.shape[0],
        cores,
        cost,
    )
    theirs, mine = zip(down([], 1, turns_y - 1, 5.0), down(halos, 0, 1, 2.0))
    came = [shifted(t, "tp_c", 1) for t in theirs]
    own, *leaving = paired(place, mine[::-1], came[::-1])
    shares = [shifted(a, "tp_y", k + 1) for k, a in enumerate(leaving)]
    return finish(mixed, own, shares, final_gain)


def solution(mesh):
    split = Mesh(mesh.devices.reshape(4, 4, 4, 2), ALL)
    placed = (P(SP, TP),) * 8 + (
        P(ALL, None),
        P(TP, None),
        P(TP, None),
        P(),
        P(SP, TP),
        P(SP, TP),
        P(None, TP),
        P(None, TP),
        P(TP, SP),
        P(),
    )
    return jax.shard_map(
        per_device, mesh=split, in_specs=placed, out_specs=P(ALL, None), check_vma=False
    )
```

```python
import math

import jax
import jax.numpy as jnp
import numpy as np
from jax import lax
from jax.experimental import pallas as pl
from jax.experimental.pallas import tpu as pltpu
from jax.sharding import Mesh
from jax.sharding import PartitionSpec as P


SP = ("sp_z", "sp_x")
TP = ("tp_y", "tp_c")
ALL = SP + TP
bf16 = jnp.bfloat16
f32 = jnp.float32
residual_scale = 2.0**0.5
epsilon = 1e-05


def shifted(value, axis, steps):
    count = lax.axis_size(axis)
    return lax.ppermute(value, axis, [(i, (i + steps) % count) for i in range(count)])


def passed_along(value, axis, steps):
    count = lax.axis_size(axis)
    first, last = (max(0, -steps), min(count, count - steps))
    return lax.ppermute(value, axis, [(source, source + steps) for source in range(first, last)])


LOW = -1e30
CHUNK = 256
EXTRA = 32
STAT_ROWS = 16
RATE = 250e6


def in_pieces(value):
    high = value.astype(bf16).astype(f32)
    middle = (value - high).astype(bf16).astype(f32)
    return high, middle, value - high - middle


def cost_of(us):
    return pl.CostEstimate(flops=int(us * RATE), transcendentals=0, bytes_accessed=0)


def pack(slot, key_small, value_small, key_large, value_large, query_small, query_large, gates):
    rows, width = key_small.shape
    half = rows // 2
    low = width // 2
    tiles = rows // width

    def body(slot_ref, ks, vs, kl, vl, qs, ql, g, kv, *q):
        lane = lax.broadcasted_iota(jnp.int32, (rows, width), 1)
        turn = lambda ref: pltpu.roll(ref[...].astype(f32), low, 1)
        for slot in range(2):
            part = slice(slot * half, (slot + 1) * half)
            kv[slot, :half] = kl[part]
            kv[slot, half:rows] = vl[part]
        kv[2, :rows] = jnp.where(lane < low, ks[...].astype(f32), turn(vs)).astype(bf16)
        kv[3, :rows] = jnp.where(lane < low, turn(ks), vs[...].astype(f32)).astype(bf16)
        for shift in range(4):
            target = lax.rem(slot_ref[0] + shift, 4)

            @pl.when(target < 2)
            def _():
                q[shift][...] = ql[...]

            @pl.when(target == 2)
            def _():
                q[shift][...] = qs[...]

            @pl.when(target == 3)
            def _():
                q[shift][...] = turn(qs).astype(bf16)

        for slot, head in ((0, 2), (1, 2), (2, 0), (3, 1)):
            blocks = []
            for piece in in_pieces(g[head : head + 1, :]):
                blocks += [piece[:, i * width : (i + 1) * width] for i in range(tiles)]
                blocks.append(jnp.zeros((8 - tiles, width), f32))
            blocks.append(jnp.zeros((EXTRA - 24, width), f32))
            kv[slot, rows:] = jnp.concatenate(blocks, axis=0).astype(bf16)

    vm = pl.BlockSpec(memory_space=pltpu.VMEM)
    return pl.pallas_call(
        body,
        in_specs=[pl.BlockSpec(memory_space=pltpu.SMEM)] + [vm] * 7,
        out_specs=[vm] * 5,
        out_shape=[jax.ShapeDtypeStruct((4, rows + EXTRA, width), bf16)]
        + [jax.ShapeDtypeStruct((rows, width), bf16)] * 4,
        cost_estimate=cost_of(2.5),
    )(slot, key_small, value_small, key_large, value_large, query_small, query_large, gates)


def work_tables(calls, depth, turns):
    tables = []
    for here in range(turns):
        row = []
        for shifts in calls:
            steps = []
            for z in range(depth):
                for n, shift in enumerate(shifts):
                    there = (here + shift) % turns
                    for w in range(depth):
                        key, query = w * turns + there, z * turns + here
                        if key < query:
                            steps.append((z, n * depth + w, 0))
                for n, shift in enumerate(shifts):
                    if shift == 0:
                        steps.append((z, n * depth + z, 1))
            row.append(steps)
        tables.append(row)
    longest = [max(len(tables[h][k]) for h in range(turns)) + 1 for k in range(len(calls))]
    out = []
    for k in range(len(calls)):
        table = np.zeros((turns, longest[k] * 3 + 1), np.int32)
        for h in range(turns):
            flat = np.array(tables[h][k] + [(0, 0, 0)] * (longest[k] - len(tables[h][k])), np.int32)
            table[h, :-1] = flat.reshape(-1)
            table[h, -1] = len(tables[h][k])
        out.append(table)
    return out


def attend(where, table, queries, chunks, state, final, tensor_parts, has_diagonal, cost):
    depth = len(queries)
    rows, width = queries[0].shape
    half = rows // 2
    low = width // 2
    tiles = rows // width
    blocks = sum(c.shape[0] for c in chunks)
    columns = rows // CHUNK
    tall = width + 16
    last = table.shape[1] - 1
    own = rows // tensor_parts
    fresh = state is None

    def body(*refs):
        where_ref, table_ref = refs[:2]
        q_refs = refs[2 : 2 + depth]
        chunk_refs = refs[2 + depth : 2 + depth + len(chunks)]
        at = 2 + depth + len(chunks) + (0 if fresh else 2)
        state_in = () if fresh else refs[at - 2 : at]
        if final:
            out_ref = refs[at]
            acc, peak = refs[at + 1 : at + 3]
            scratch = refs[at + 3 :]
        else:
            acc, peak = refs[at : at + 2]
            scratch = refs[at + 2 :]
        qa, ka_small, va_small, ka_large, va_large, first = scratch
        slot = where_ref[0]
        column = where_ref[1]
        count = table_ref[column, last]

        @pl.loop(0, depth)
        def _(z):
            if fresh:
                acc[z] = jnp.zeros(acc.shape[1:], f32)
                peak[z] = jnp.full(peak.shape[1:], LOW, f32)
            else:
                acc[z] = state_in[0][z]
                peak[z] = state_in[1][z]

        def attention(small):
            d = low if small else width
            ext = d + 16
            span = rows if small else half
            tile = CHUNK if small else half
            parts = span // tile
            root = d**0.5
            rate = math.log2(math.e) / root
            ka, va = (ka_small, va_small) if small else (ka_large, va_large)
            deep = width if small else 2 * width
            lane = lax.broadcasted_iota(jnp.int32, (rows, width), 1)

            for shift, q_ref in enumerate(q_refs):
                z = lax.rem(slot + depth - shift, depth)
                q = q_ref[...]
                if small:
                    one = ((lane >= d) & (lane < d + 3)).astype(f32)
                    qa[z, :, :width] = jnp.where(lane < d, q.astype(f32), one).astype(bf16)
                else:
                    qa[z, :, :width] = q
                    qa[z, :, width:] = (lane < 3).astype(f32).astype(bf16)

            def prepare(ref, n, block):
                pieces = ref[n, rows : rows + 24].astype(f32)
                gate = pieces[0:8] + pieces[8:16] + pieces[16:24]
                bias = jnp.concatenate([gate[i : i + 1] for i in range(tiles)], axis=1) * -root
                bias = jnp.broadcast_to(bias, (8, rows))
                if not small:
                    bias = jnp.where(slot == 0, bias[:, :half], bias[:, half:])
                high, middle, rest = in_pieces(bias)
                row = lax.broadcasted_iota(jnp.int32, (8, span), 0)
                zero = jnp.zeros((8, span), f32)
                picked = jnp.where(row == 0, high, jnp.where(row == 1, middle, jnp.where(row == 2, rest, zero)))
                before = d if small else 0
                stack = [picked, jnp.zeros((width - before - 8, span), f32)]
                if before:
                    stack = [jnp.zeros((before, span), f32)] + stack
                gate_columns = jnp.concatenate(stack, axis=0).astype(bf16).T
                if small:
                    kv = ref[n, :rows]
                    ka[block] = jnp.where(lane < d, kv, gate_columns)
                    va[block, :d] = kv.T[d:]
                else:
                    ka[block, :, :width] = ref[n, :half]
                    ka[block, :, width:] = gate_columns
                    va[block, :d] = ref[n, half:rows].T
                va[block, d:] = jnp.ones((16, span), bf16)

            offset = 0
            for ref in chunk_refs:
                base = offset

                @pl.loop(0, ref.shape[0])
                def _(n):
                    prepare(ref, n, base + n)

                offset += ref.shape[0]

            def scores(z, block, c, t):
                return lax.dot_general(
                    ka[block, t * tile : (t + 1) * tile],
                    qa[z, c * CHUNK : (c + 1) * CHUNK, :deep],
                    (((1,), (1,)), ((), ())),
                    preferred_element_type=f32,
                )

            def masked(s, c, t, flag):
                if small and t < c:
                    return s
                key = lax.broadcasted_iota(jnp.int32, (tile, CHUNK), 0) + t * tile
                if not small:
                    key = key + slot * half
                    key = jnp.where(flag == 0, 0, key)
                query = lax.broadcasted_iota(jnp.int32, (tile, CHUNK), 1) + c * CHUNK
                return jnp.where(key <= query, s, LOW)

            def step(n, diagonal):
                z, block = table_ref[column, 3 * n], table_ref[column, 3 * n + 1]
                next_z, next_block = table_ref[column, 3 * n + 3], table_ref[column, 3 * n + 4]
                held_count = lambda c: c + 1 if diagonal and small else parts
                held = [first[t * tile : (t + 1) * tile] for t in range(held_count(0))]
                for c in range(columns):
                    cols = slice(c * CHUNK, (c + 1) * CHUNK)
                    if diagonal:
                        held = [masked(s, c, t, table_ref[column, 3 * n + 2]) for t, s in enumerate(held)]
                    top = held[0]
                    for s in held[1:]:
                        top = jnp.maximum(top, s)
                    old = peak[z, 0:1, cols]
                    new = jnp.maximum(old, jnp.max(top, axis=0, keepdims=True))
                    scaled = new * rate
                    factor = jnp.exp2(old * rate - scaled)
                    peak[z, 0:1, cols] = new
                    coming = []
                    added = None
                    following = c + 1 < columns
                    ahead = held_count(c + 1) if following else parts
                    for t in range(max(len(held), ahead)):
                        if t < ahead:
                            if following:
                                coming.append(scores(z, block, c + 1, t))
                            else:
                                first[t * tile : (t + 1) * tile] = scores(next_z, next_block, 0, t)
                        if t < len(held):
                            w = jnp.exp2(held[t] * rate - scaled).astype(bf16)
                            add = jnp.dot(
                                va[block, :, t * tile : (t + 1) * tile], w, preferred_element_type=f32
                            )
                            added = add if added is None else added + add
                    acc[z, :ext, cols] = acc[z, :ext, cols] * factor + added
                    held = coming

            for t in range(parts):
                first[t * tile : (t + 1) * tile] = scores(table_ref[column, 0], table_ref[column, 1], 0, t)

            @pl.loop(0, count)
            def _(n):
                if not has_diagonal or not small:
                    step(n, has_diagonal)
                    return
                diagonal = table_ref[column, 3 * n + 2]

                @pl.when(diagonal == 0)
                def _():
                    step(n, False)

                @pl.when(diagonal == 1)
                def _():
                    step(n, True)

            if final:

                @pl.loop(0, depth)
                def _(z):
                    total = acc[z, d : d + 1]
                    out = acc[z, :d] / total
                    if small:
                        out = jnp.concatenate([out, jnp.zeros((width - d, rows), f32)], axis=0)
                    out = out.T.astype(bf16)
                    level = peak[z, 0:1] * rate + jnp.log2(total)
                    stat = jnp.concatenate([*in_pieces(level), jnp.zeros((STAT_ROWS - 3, rows), f32)], axis=0)
                    for r in range(tensor_parts):
                        out_ref[z * tensor_parts + r, :own] = out[r * own : (r + 1) * own]
                        if not small:
                            mine = stat[:, r * own : (r + 1) * own]
                            mine = jnp.concatenate([mine, jnp.zeros((STAT_ROWS, width - own), f32)], axis=1)
                            out_ref[z * tensor_parts + r, own:] = mine.astype(bf16)
                        else:
                            out_ref[z * tensor_parts + r, own:] = jnp.zeros((STAT_ROWS, width), bf16)

        @pl.when(slot < 2)
        def _():
            attention(False)

        @pl.when(slot >= 2)
        def _():
            attention(True)

    vm = pl.BlockSpec(memory_space=pltpu.VMEM)
    sm = pl.BlockSpec(memory_space=pltpu.SMEM)
    state_shapes = [((depth, tall, rows), f32), ((depth, 8, rows), f32)]
    scratch = [pltpu.VMEM(s, t) for s, t in state_shapes] if final else []
    scratch += [
        pltpu.VMEM((depth, rows, 2 * width), bf16),
        pltpu.VMEM((blocks, rows, width), bf16),
        pltpu.VMEM((blocks, low + 16, rows), bf16),
        pltpu.VMEM((blocks, half, 2 * width), bf16),
        pltpu.VMEM((blocks, tall, half), bf16),
        pltpu.VMEM((rows, CHUNK), f32),
    ]
    if final:
        out_shape = jax.ShapeDtypeStruct((depth * tensor_parts, own + STAT_ROWS, width), bf16)
        out_specs = vm
    else:
        out_shape = [jax.ShapeDtypeStruct(s, t) for s, t in state_shapes]
        out_specs = [vm, vm]
    args = [where, table, *queries, *chunks] + ([] if fresh else list(state))
    return pl.pallas_call(
        body,
        in_specs=[sm, sm] + [vm] * (len(args) - 2),
        out_specs=out_specs,
        scratch_shapes=scratch,
        out_shape=out_shape,
        compiler_params=pltpu.CompilerParams(vmem_limit_bytes=58 * 2**20),
        cost_estimate=cost_of(cost),
    )(*args)


def mix_rows(place, arrived, mixers, residual, gain):
    own, wide = residual.shape
    width = arrived.shape[2]
    cores = 2
    turns = arrived.shape[0] // 4 // cores
    parts = turns * cores

    def body(place_ref, arrived_ref, *refs):
        mixer_refs = refs[: len(mixers)]
        residual_ref, gain_ref, out_ref, acc = refs[len(mixers) :]
        lane = lax.broadcasted_iota(jnp.int32, (own, width), 1)

        def level(index):
            pieces = arrived_ref[index, own:].astype(f32)
            line = pieces[0:1] + pieces[1:2] + pieces[2:3]
            return jnp.broadcast_to(line, (8, width)).T[:own, 0:1]

        def rows_of(part):
            second = pltpu.roll(arrived_ref[3 * parts + part, :own].astype(f32), width // 2, 1)
            small = jnp.where(lane < width // 2, arrived_ref[2 * parts + part, :own].astype(f32), second)
            share = 1.0 / (1.0 + jnp.exp2(level(part) - level(parts + part)))
            large = arrived_ref[part, :own].astype(f32) * (1.0 - share) + arrived_ref[
                parts + part, :own
            ].astype(f32) * share
            return small.astype(bf16), large.astype(bf16)

        acc[...] = residual_ref[...].astype(f32) * residual_scale
        for ref, (_, shift, other) in zip(mixer_refs, mixers):
            y = lax.rem(place_ref[0] + shift + turns, turns)
            core = place_ref[1] if other == 0 else 1 - place_ref[1]
            both = rows_of(y * cores + core)
            acc[...] += jnp.dot(jnp.concatenate(both, axis=1), ref[...], preferred_element_type=f32)
        values = acc[...]
        center = jnp.mean(values, axis=-1, keepdims=True)
        values = values - center
        spread = jnp.mean(jnp.square(values), axis=-1, keepdims=True)
        out_ref[...] = (values * lax.rsqrt(spread + epsilon) * gain_ref[...]).astype(bf16)

    vm = pl.BlockSpec(memory_space=pltpu.VMEM)
    return pl.pallas_call(
        body,
        in_specs=[pl.BlockSpec(memory_space=pltpu.SMEM)] + [vm] * (len(mixers) + 3),
        out_specs=vm,
        scratch_shapes=[pltpu.VMEM((own, wide), f32)],
        out_shape=jax.ShapeDtypeStruct((own, wide), bf16),
        compiler_params=pltpu.CompilerParams(vmem_limit_bytes=40 * 2**20),
        cost_estimate=cost_of(5.0),
    )(place, arrived, *[m[0] for m in mixers], residual, gain.reshape(1, wide))


BLOCK = 768
LEAD = 16


def pack_weights(value_weight, gate_weight, down_weight):
    rows, width = value_weight.shape

    def body(v, g, d, out):
        for k, part in enumerate((v[...], g[...], d[...].T)):
            out[:, k * BLOCK : k * BLOCK + width] = part
            out[:, k * BLOCK + width : (k + 1) * BLOCK] = jnp.zeros((rows, BLOCK - width), bf16)

    vm = pl.BlockSpec(memory_space=pltpu.VMEM)
    return pl.pallas_call(
        body,
        in_specs=[vm] * 3,
        out_specs=vm,
        out_shape=jax.ShapeDtypeStruct((rows, 3 * BLOCK), bf16),
        cost_estimate=cost_of(1.5),
    )(value_weight, gate_weight, down_weight)


def window(array, k):
    return pl.BlockSpec((array.shape[0], BLOCK), lambda i: (0, k))


def whole(array):
    return pl.BlockSpec(array.shape, lambda i: (0,) * array.ndim)


def ups(chunks, weights, width, cost):
    rows = sum(c.shape[0] for c in chunks)

    def body(*refs):
        value_ref, gate_ref, out_value, out_gate = refs[len(chunks) :]
        x = jnp.concatenate([r[...] for r in refs[: len(chunks)]], axis=0)
        for ref, out in ((value_ref, out_value), (gate_ref, out_gate)):
            out[...] = jnp.dot(x, ref[:, :width], preferred_element_type=f32).astype(bf16)

    shape = jax.ShapeDtypeStruct((rows, width), bf16)
    return pl.pallas_call(
        body,
        grid=(1,),
        in_specs=[whole(c) for c in chunks] + [window(weights, 0), window(weights, 1)],
        out_specs=[whole(shape)] * 2,
        out_shape=[shape] * 2,
        compiler_params=pltpu.CompilerParams(vmem_limit_bytes=40 * 2**20),
        cost_estimate=cost_of(cost),
    )(*chunks, weights, weights)


def ends(place, pieces, spots, own, turns, cores):
    width = pieces[0][0].shape[1]

    def body(place_ref, *refs):
        outs, leaving = refs[-3:-1], refs[-1]
        spot = 0
        for k in range(0, len(refs) - 3, 2):
            for i in range(refs[k].shape[0] // own):
                shift, other = spots[spot]
                spot += 1
                y = lax.rem(place_ref[0] + shift + turns, turns)
                core = place_ref[1] if other == 0 else 1 - place_ref[1]
                for side in range(2):
                    outs[side][y * cores + core] = refs[k + side][(i + 1) * own - LEAD : (i + 1) * own]
        for side in range(2):
            leaving[side * LEAD : (side + 1) * LEAD] = outs[side][turns * cores - 1]

    vm = pl.BlockSpec(memory_space=pltpu.VMEM)
    flat = [a for pair in pieces for a in pair]
    return pl.pallas_call(
        body,
        in_specs=[pl.BlockSpec(memory_space=pltpu.SMEM)] + [vm] * len(flat),
        out_specs=[vm] * 3,
        out_shape=[jax.ShapeDtypeStruct((turns * cores, LEAD, width), bf16)] * 2
        + [jax.ShapeDtypeStruct((2 * LEAD, width), bf16)],
        cost_estimate=cost_of(1.5),
    )(place, *flat)


def downs(place, pieces, groups, tails, halo, value_taps, gate_taps, weights, own, turns, cores, cost):
    width = pieces[0][0].shape[1]
    wide = weights.shape[0]
    count = len(groups)

    def body(place_ref, *refs):
        vt_ref, gt_ref, down_ref, halo_ref = refs[:4]
        tail_refs = refs[4:6]
        up_refs = refs[6 : 6 + 2 * len(pieces)]
        theirs, mine, hidden, terms = refs[6 + 2 * len(pieces) :]

        def filtered(ref, taps, tail, side, at, part):
            halo_rows = halo_ref[side * LEAD : (side + 1) * LEAD].astype(f32)
            before = tail[jnp.maximum(part - 1, 0)].astype(f32)
            before = jnp.where(part == 0, halo_rows, before)
            here = ref[pl.ds(pl.multiple_of(at * own, LEAD), own)].astype(f32)
            rows = jnp.concatenate([before, here], axis=0)
            two = pltpu.roll(rows, 2, 0)[LEAD:]
            one = pltpu.roll(rows, 1, 0)[LEAD:]
            return taps[0:1] * two + taps[1:2] * one + taps[2:3] * rows[LEAD:]

        @pl.loop(0, 2)
        def _(turn):
            core = jnp.where(turn == 0, 1 - place_ref[1], place_ref[1])
            for i, (piece, at_own, at_other, shift) in enumerate(groups):
                at = jnp.where(turn == 0, at_other, at_own)
                part = lax.rem(place_ref[0] + shift + turns, turns) * cores + core
                value = filtered(up_refs[2 * piece], vt_ref, tail_refs[0], 0, at, part)
                gate = filtered(up_refs[2 * piece + 1], gt_ref, tail_refs[1], 1, at, part)
                hidden[i * own : (i + 1) * own] = (gate / (1.0 + jnp.exp(-gate)) * value).astype(bf16)
            terms[...] = lax.dot_general(
                hidden[...],
                down_ref[:, :width],
                (((1,), (1,)), ((), ())),
                preferred_element_type=f32,
            )
            for own_turn, out in enumerate((theirs, mine)):

                @pl.when(turn == own_turn)
                def _():
                    @pl.loop(0, count)
                    def _(i):
                        out[i] = terms[pl.ds(pl.multiple_of(i * own, LEAD), own)].astype(out.dtype)

    shapes = [jax.ShapeDtypeStruct((count, own, wide), t) for t in (bf16, f32)]
    flat = [a for pair in pieces for a in pair]
    return pl.pallas_call(
        body,
        grid=(1,),
        in_specs=[pl.BlockSpec(memory_space=pltpu.SMEM), whole(value_taps), whole(gate_taps)]
        + [window(weights, 2), whole(halo), whole(tails[0]), whole(tails[1])]
        + [whole(a) for a in flat],
        out_specs=[whole(x) for x in shapes],
        out_shape=shapes,
        scratch_shapes=[
            pltpu.VMEM((count * own, width), bf16),
            pltpu.VMEM((count * own, wide), f32),
        ],
        compiler_params=pltpu.CompilerParams(vmem_limit_bytes=50 * 2**20),
        cost_estimate=cost_of(cost),
    )(place, value_taps, gate_taps, weights, halo, *tails, *flat)


def paired(mine, theirs, kinds):
    count, own, wide = mine.shape

    def body(mine_ref, their_ref, *outs):
        for i, out in enumerate(outs):
            out[...] = (mine_ref[i] + their_ref[i].astype(f32)).astype(out.dtype)

    vm = pl.BlockSpec(memory_space=pltpu.VMEM)
    return pl.pallas_call(
        body,
        in_specs=[vm] * 2,
        out_specs=[vm] * count,
        out_shape=[jax.ShapeDtypeStruct((own, wide), kind) for kind in kinds],
        cost_estimate=cost_of(0.7 * count),
    )(mine, theirs)


def finish(mixed, own, shares, gain):
    rows, wide = mixed.shape

    def body(*refs):
        mixed_ref, own_ref = refs[:2]
        gain_ref, out_ref = refs[-2:]
        total = own_ref[...]
        for r in refs[2:-2]:
            total = total + r[...].astype(f32)
        values = residual_scale * mixed_ref[...].astype(f32) + total
        center = jnp.mean(values, axis=-1, keepdims=True)
        values = values - center
        spread = jnp.mean(jnp.square(values), axis=-1, keepdims=True)
        out_ref[...] = (values * lax.rsqrt(spread + epsilon) * gain_ref[...]).astype(bf16)

    vm = pl.BlockSpec(memory_space=pltpu.VMEM)
    return pl.pallas_call(
        body,
        in_specs=[vm] * (3 + len(shares)),
        out_specs=vm,
        out_shape=jax.ShapeDtypeStruct((rows, wide), bf16),
        cost_estimate=cost_of(2.0),
    )(mixed, own, *shares, gain.reshape(1, wide))


def per_device(
    query_small,
    key_small,
    value_small,
    gates_small,
    query_large,
    key_large,
    value_large,
    gates_large,
    residual,
    mixer_small,
    mixer_large,
    mix_gain,
    value_weight,
    gate_weight,
    value_taps,
    gate_taps,
    down_weight,
    final_gain,
):
    shard_rows = query_small.shape[0]
    slot = lax.axis_index("sp_z").astype(jnp.int32)
    column = lax.axis_index("sp_x").astype(jnp.int32)
    depth, turns = lax.axis_size("sp_z"), lax.axis_size("sp_x")
    heads_small = gates_small.shape[1]
    heads_large = gates_large.shape[1]
    blank = jnp.zeros((8 - heads_small - heads_large, shard_rows), f32)
    own_gates = jnp.concatenate([gates_small.T, gates_large.T, blank], axis=0)
    packed, *asked = pack(
        slot.reshape(1),
        key_small,
        value_small,
        key_large,
        value_large,
        query_small,
        query_large,
        own_gates,
    )
    shards = pack_weights(value_weight, gate_weight, down_weight)
    packed, shards = lax.optimization_barrier((packed, shards))
    weights = lax.all_gather(shards, SP, axis=0, tiled=True)
    pairs = lax.all_to_all(packed, "sp_z", split_axis=0, concat_axis=0, tiled=True)
    queries = [asked[0]] + [shifted(asked[k], "sp_z", k) for k in range(1, depth)]
    pairs, *queries = lax.optimization_barrier((pairs, *queries))
    before = shifted(pairs, "sp_x", 1)
    after = shifted(pairs, "sp_x", -1)
    mixer = jnp.concatenate([mixer_small, mixer_large], axis=0)
    mixers = [mixer, shifted(mixer, "tp_y", 1), shifted(mixer, "tp_y", -1)]
    calls = ((0,), (-1, 1), (2,))
    tables = work_tables(calls, depth, turns)
    place_here = jnp.stack([slot, column])
    call = lambda k, chunks, state: attend(
        place_here,
        jnp.asarray(tables[k]),
        queries,
        chunks,
        state,
        k + 1 == len(calls),
        lax.axis_size(TP),
        0 in calls[k],
        12.0 * len(calls[k]),
    )
    state = call(0, [pairs], None)
    before, after, state, mixers = lax.optimization_barrier((before, after, state, mixers))
    far = [
        shifted(before[: depth // 2], "sp_x", 1),
        shifted(after[depth // 2 :], "sp_x", -1),
    ]
    mixers.append(shifted(mixers[1], "tp_y", 1))
    state = call(1, [before, after], state)
    state = call(2, far, state)
    state, mixers, weights = lax.optimization_barrier((state, mixers, weights))
    arrived = lax.all_to_all(state, ("sp_z",) + TP, split_axis=0, concat_axis=0, tiled=True)
    shifts = (0, -1, 1, 2)
    mixers = [(a, shift, 0) for a, shift in zip(mixers, shifts)] + [
        (shifted(a, "tp_c", 1), shift, 1) for a, shift in zip(mixers, shifts)
    ]
    place = jnp.stack([lax.axis_index("tp_y"), lax.axis_index("tp_c")]).astype(jnp.int32)
    mixed = mix_rows(place, arrived, mixers, residual, mix_gain)
    turns_y, cores = lax.axis_size("tp_y"), lax.axis_size("tp_c")
    own_rows = mixed.shape[0]
    half = own_rows // 2
    width = value_weight.shape[1]
    spots = [(0, 0), (0, 1), (-1, 0), (1, 0), (-1, 1), (1, 1), (2, 0), (2, 1)]
    last_one, next_one = shifted(mixed, "tp_y", 1), shifted(mixed, "tp_y", -1)
    near = ups([mixed, shifted(mixed, "tp_c", 1)], weights, width, 3.0)
    near, last_one, next_one = lax.optimization_barrier((near, last_one, next_one))
    opposite = [shifted(last_one[:half], "tp_y", 1), shifted(next_one[half:], "tp_y", -1)]
    beside = [last_one, next_one] + [shifted(a, "tp_c", 1) for a in (last_one, next_one)]
    beside = ups(beside, weights, width, 4.0)
    beside, opposite = lax.optimization_barrier((beside, opposite))
    opposite = ups(opposite + [shifted(a, "tp_c", 1) for a in opposite], weights, width, 3.0)
    pieces = [near, beside, opposite]
    *tails, leaving = ends(place, pieces, spots, own_rows, turns_y, cores)
    halo = passed_along(leaving, SP, 1)
    down = lambda chosen, groups, cost: downs(
        place,
        chosen,
        groups,
        tails,
        halo,
        value_taps,
        gate_taps,
        weights,
        own_rows,
        turns_y,
        cores,
        cost,
    )
    theirs, mine = down([opposite], [(0, 0, 1, 2)], 4.0)
    (distant,) = paired(mine, shifted(theirs, "tp_c", 1), [bf16])
    near, beside, distant = lax.optimization_barrier((near, beside, distant))
    shares = [shifted(distant, "tp_y", 2)]
    theirs, mine = down([near, beside], [(0, 0, 1, 0), (1, 0, 2, -1), (1, 1, 3, 1)], 8.0)
    own, before, after = paired(mine, shifted(theirs, "tp_c", 1), [f32, bf16, bf16])
    shares += [shifted(before, "tp_y", -1), shifted(after, "tp_y", 1)]
    return finish(mixed, own, shares, final_gain)


def solution(mesh):
    split = Mesh(mesh.devices.reshape(4, 4, 4, 2), ALL)
    placed = (P(SP, TP),) * 8 + (
        P(ALL, None),
        P(TP, None),
        P(TP, None),
        P(),
        P(SP, TP),
        P(SP, TP),
        P(None, TP),
        P(None, TP),
        P(TP, SP),
        P(),
    )

    return jax.shard_map(per_device, mesh=split, in_specs=placed, out_specs=P(ALL, None), check_vma=False)
```

```python
import math

import jax
import jax.numpy as jnp
import numpy as np
from jax import lax
from jax.experimental import pallas as pl
from jax.experimental.pallas import tpu as pltpu
from jax.sharding import Mesh
from jax.sharding import PartitionSpec as P


SP = ("sp_z", "sp_x")
TP = ("tp_y", "tp_c")
ALL = SP + TP
bf16 = jnp.bfloat16
f32 = jnp.float32
residual_scale = 2.0**0.5
epsilon = 1e-05


def shifted(value, axis, steps):
    count = lax.axis_size(axis)
    return lax.ppermute(value, axis, [(i, (i + steps) % count) for i in range(count)])


def passed_along(value, axis, steps):
    count = lax.axis_size(axis)
    first, last = (max(0, -steps), min(count, count - steps))
    return lax.ppermute(value, axis, [(source, source + steps) for source in range(first, last)])


LOW = -1e30
CHUNK = 256
EXTRA = 32
STAT_ROWS = 16
RATE = 250e6


def in_pieces(value):
    high = value.astype(bf16).astype(f32)
    middle = (value - high).astype(bf16).astype(f32)
    return high, middle, value - high - middle


def cost_of(us):
    return pl.CostEstimate(flops=int(us * RATE), transcendentals=0, bytes_accessed=0)


def pack(slot, key_small, value_small, key_large, value_large, query_small, query_large, gates_small, gates_large):
    rows, width = key_small.shape
    half = rows // 2
    low = width // 2
    tiles = rows // width

    def body(slot_ref, ks, vs, kl, vl, qs, ql, gs, gl, kv, *q):
        lane = lax.broadcasted_iota(jnp.int32, (rows, width), 1)
        turn = lambda ref: pltpu.roll(ref[...].astype(f32), low, 1)
        for slot in range(2):
            part = slice(slot * half, (slot + 1) * half)
            kv[slot, :half] = kl[part]
            kv[slot, half:rows] = vl[part]
        kv[2, :rows] = jnp.where(lane < low, ks[...].astype(f32), turn(vs)).astype(bf16)
        kv[3, :rows] = jnp.where(lane < low, turn(ks), vs[...].astype(f32)).astype(bf16)
        for shift in range(4):
            target = lax.rem(slot_ref[0] + shift, 4)

            @pl.when(target < 2)
            def _():
                q[shift][...] = ql[...]

            @pl.when(target == 2)
            def _():
                q[shift][...] = qs[...]

            @pl.when(target == 3)
            def _():
                q[shift][...] = turn(qs).astype(bf16)

        for slot, gate in ((0, gl[0:1]), (1, gl[0:1]), (2, gs[0:1]), (3, gs[1:2])):
            blocks = []
            for piece in in_pieces(gate):
                blocks += [piece[:, i * width : (i + 1) * width] for i in range(tiles)]
                blocks.append(jnp.zeros((8 - tiles, width), f32))
            blocks.append(jnp.zeros((EXTRA - 24, width), f32))
            kv[slot, rows:] = jnp.concatenate(blocks, axis=0).astype(bf16)

    vm = pl.BlockSpec(memory_space=pltpu.VMEM)
    return pl.pallas_call(
        body,
        in_specs=[pl.BlockSpec(memory_space=pltpu.SMEM)] + [vm] * 8,
        out_specs=[vm] * 5,
        out_shape=[jax.ShapeDtypeStruct((4, rows + EXTRA, width), bf16)]
        + [jax.ShapeDtypeStruct((rows, width), bf16)] * 4,
        cost_estimate=cost_of(2.5),
    )(slot, key_small, value_small, key_large, value_large, query_small, query_large, gates_small, gates_large)


def work_tables(calls, depth, turns):
    tables = []
    for here in range(turns):
        row = []
        for shifts in calls:
            steps = []
            for z in range(depth):
                for n, shift in enumerate(shifts):
                    there = (here + shift) % turns
                    for w in range(depth):
                        key, query = w * turns + there, z * turns + here
                        if key < query:
                            steps.append((z, n * depth + w, 0))
                for n, shift in enumerate(shifts):
                    if shift == 0:
                        steps.append((z, n * depth + z, 1))
            row.append(steps)
        tables.append(row)
    longest = [max(len(tables[h][k]) for h in range(turns)) + 1 for k in range(len(calls))]
    out = []
    for k in range(len(calls)):
        table = np.zeros((turns, longest[k] * 3 + 1), np.int32)
        for h in range(turns):
            flat = np.array(tables[h][k] + [(0, 0, 0)] * (longest[k] - len(tables[h][k])), np.int32)
            table[h, :-1] = flat.reshape(-1)
            table[h, -1] = len(tables[h][k])
        out.append(table)
    return out


def attend(where, table, queries, chunks, state, final, tensor_parts, has_diagonal, cost):
    depth = len(queries)
    rows, width = queries[0].shape
    half = rows // 2
    low = width // 2
    tiles = rows // width
    blocks = sum(c.shape[0] for c in chunks)
    columns = rows // CHUNK
    tall = width + 16
    last = table.shape[1] - 1
    own = rows // tensor_parts
    fresh = state is None

    def body(*refs):
        where_ref, table_ref = refs[:2]
        q_refs = refs[2 : 2 + depth]
        chunk_refs = refs[2 + depth : 2 + depth + len(chunks)]
        at = 2 + depth + len(chunks) + (0 if fresh else 2)
        state_in = () if fresh else refs[at - 2 : at]
        if final:
            out_ref = refs[at]
            acc, peak = refs[at + 1 : at + 3]
            scratch = refs[at + 3 :]
        else:
            acc, peak = refs[at : at + 2]
            scratch = refs[at + 2 :]
        qa, ka_small, va_small, ka_large, va_large, first = scratch
        slot = where_ref[0]
        column = where_ref[1]
        count = table_ref[column, last]

        @pl.loop(0, depth)
        def _(z):
            if fresh:
                acc[z] = jnp.zeros(acc.shape[1:], f32)
                peak[z] = jnp.full(peak.shape[1:], LOW, f32)
            else:
                acc[z] = state_in[0][z]
                peak[z] = state_in[1][z]

        def attention(small):
            d = low if small else width
            ext = d + 16
            span = rows if small else half
            tile = CHUNK if small else half
            parts = span // tile
            root = d**0.5
            rate = math.log2(math.e) / root
            ka, va = (ka_small, va_small) if small else (ka_large, va_large)
            deep = width if small else 2 * width
            lane = lax.broadcasted_iota(jnp.int32, (rows, width), 1)

            for shift, q_ref in enumerate(q_refs):
                z = lax.rem(slot + depth - shift, depth)
                q = q_ref[...]
                if small:
                    one = ((lane >= d) & (lane < d + 3)).astype(f32)
                    qa[z, :, :width] = jnp.where(lane < d, q.astype(f32), one).astype(bf16)
                else:
                    qa[z, :, :width] = q
                    qa[z, :, width:] = (lane < 3).astype(f32).astype(bf16)

            def prepare(ref, n, block):
                pieces = ref[n, rows : rows + 24].astype(f32)
                gate = pieces[0:8] + pieces[8:16] + pieces[16:24]
                bias = jnp.concatenate([gate[i : i + 1] for i in range(tiles)], axis=1) * -root
                bias = jnp.broadcast_to(bias, (8, rows))
                if not small:
                    bias = jnp.where(slot == 0, bias[:, :half], bias[:, half:])
                high, middle, rest = in_pieces(bias)
                row = lax.broadcasted_iota(jnp.int32, (8, span), 0)
                zero = jnp.zeros((8, span), f32)
                picked = jnp.where(row == 0, high, jnp.where(row == 1, middle, jnp.where(row == 2, rest, zero)))
                before = d if small else 0
                stack = [picked, jnp.zeros((width - before - 8, span), f32)]
                if before:
                    stack = [jnp.zeros((before, span), f32)] + stack
                gate_columns = jnp.concatenate(stack, axis=0).astype(bf16).T
                if small:
                    kv = ref[n, :rows]
                    ka[block] = jnp.where(lane < d, kv, gate_columns)
                    va[block, :d] = kv.T[d:]
                else:
                    ka[block, :, :width] = ref[n, :half]
                    ka[block, :, width:] = gate_columns
                    va[block, :d] = ref[n, half:rows].T
                va[block, d:] = jnp.ones((16, span), bf16)

            offset = 0
            for ref in chunk_refs:
                base = offset

                @pl.loop(0, ref.shape[0])
                def _(n):
                    prepare(ref, n, base + n)

                offset += ref.shape[0]

            def scores(z, block, c, t):
                return lax.dot_general(
                    ka[block, t * tile : (t + 1) * tile],
                    qa[z, c * CHUNK : (c + 1) * CHUNK, :deep],
                    (((1,), (1,)), ((), ())),
                    preferred_element_type=f32,
                )

            def masked(s, c, t, flag):
                if small and t < c:
                    return s
                key = lax.broadcasted_iota(jnp.int32, (tile, CHUNK), 0) + t * tile
                if not small:
                    key = key + slot * half
                    key = jnp.where(flag == 0, 0, key)
                query = lax.broadcasted_iota(jnp.int32, (tile, CHUNK), 1) + c * CHUNK
                return jnp.where(key <= query, s, LOW)

            def step(n, diagonal):
                z, block = table_ref[column, 3 * n], table_ref[column, 3 * n + 1]
                next_z, next_block = table_ref[column, 3 * n + 3], table_ref[column, 3 * n + 4]
                held_count = lambda c: c + 1 if diagonal and small else parts
                held = [first[t * tile : (t + 1) * tile] for t in range(held_count(0))]
                for c in range(columns):
                    cols = slice(c * CHUNK, (c + 1) * CHUNK)
                    if diagonal:
                        held = [masked(s, c, t, table_ref[column, 3 * n + 2]) for t, s in enumerate(held)]
                    top = held[0]
                    for s in held[1:]:
                        top = jnp.maximum(top, s)
                    old = peak[z, 0:1, cols]
                    new = jnp.maximum(old, jnp.max(top, axis=0, keepdims=True))
                    scaled = new * rate
                    factor = jnp.exp2(old * rate - scaled)
                    peak[z, 0:1, cols] = new
                    coming = []
                    added = None
                    following = c + 1 < columns
                    ahead = held_count(c + 1) if following else parts
                    for t in range(max(len(held), ahead)):
                        if t < ahead:
                            if following:
                                coming.append(scores(z, block, c + 1, t))
                            else:
                                first[t * tile : (t + 1) * tile] = scores(next_z, next_block, 0, t)
                        if t < len(held):
                            w = jnp.exp2(held[t] * rate - scaled).astype(bf16)
                            add = jnp.dot(
                                va[block, :, t * tile : (t + 1) * tile], w, preferred_element_type=f32
                            )
                            added = add if added is None else added + add
                    acc[z, :ext, cols] = acc[z, :ext, cols] * factor + added
                    held = coming

            for t in range(parts):
                first[t * tile : (t + 1) * tile] = scores(table_ref[column, 0], table_ref[column, 1], 0, t)

            @pl.loop(0, count)
            def _(n):
                if not has_diagonal or not small:
                    step(n, has_diagonal)
                    return
                diagonal = table_ref[column, 3 * n + 2]

                @pl.when(diagonal == 0)
                def _():
                    step(n, False)

                @pl.when(diagonal == 1)
                def _():
                    step(n, True)

            if final:

                @pl.loop(0, depth)
                def _(z):
                    total = acc[z, d : d + 1]
                    out = acc[z, :d] / total
                    if small:
                        out = jnp.concatenate([out, jnp.zeros((width - d, rows), f32)], axis=0)
                    out = out.T.astype(bf16)
                    level = peak[z, 0:1] * rate + jnp.log2(total)
                    stat = jnp.concatenate([*in_pieces(level), jnp.zeros((STAT_ROWS - 3, rows), f32)], axis=0)
                    for r in range(tensor_parts):
                        out_ref[z * tensor_parts + r, :own] = out[r * own : (r + 1) * own]
                        if not small:
                            mine = stat[:, r * own : (r + 1) * own]
                            mine = jnp.concatenate([mine, jnp.zeros((STAT_ROWS, width - own), f32)], axis=1)
                            out_ref[z * tensor_parts + r, own:] = mine.astype(bf16)
                        else:
                            out_ref[z * tensor_parts + r, own:] = jnp.zeros((STAT_ROWS, width), bf16)

        @pl.when(slot < 2)
        def _():
            attention(False)

        @pl.when(slot >= 2)
        def _():
            attention(True)

    vm = pl.BlockSpec(memory_space=pltpu.VMEM)
    sm = pl.BlockSpec(memory_space=pltpu.SMEM)
    state_shapes = [((depth, tall, rows), f32), ((depth, 8, rows), f32)]
    scratch = [pltpu.VMEM(s, t) for s, t in state_shapes] if final else []
    scratch += [
        pltpu.VMEM((depth, rows, 2 * width), bf16),
        pltpu.VMEM((blocks, rows, width), bf16),
        pltpu.VMEM((blocks, low + 16, rows), bf16),
        pltpu.VMEM((blocks, half, 2 * width), bf16),
        pltpu.VMEM((blocks, tall, half), bf16),
        pltpu.VMEM((rows, CHUNK), f32),
    ]
    if final:
        out_shape = jax.ShapeDtypeStruct((depth * tensor_parts, own + STAT_ROWS, width), bf16)
        out_specs = vm
    else:
        out_shape = [jax.ShapeDtypeStruct(s, t) for s, t in state_shapes]
        out_specs = [vm, vm]
    args = [where, table, *queries, *chunks] + ([] if fresh else list(state))
    return pl.pallas_call(
        body,
        in_specs=[sm, sm] + [vm] * (len(args) - 2),
        out_specs=out_specs,
        scratch_shapes=scratch,
        out_shape=out_shape,
        compiler_params=pltpu.CompilerParams(vmem_limit_bytes=58 * 2**20),
        cost_estimate=cost_of(cost),
    )(*args)


def mix_rows(place, arrived, mixers, residual, gain):
    own, wide = residual.shape
    width = arrived.shape[2]
    cores = 2
    turns = arrived.shape[0] // 4 // cores
    parts = turns * cores

    def body(place_ref, arrived_ref, *refs):
        mixer_refs = refs[: len(mixers)]
        residual_ref, gain_ref, out_ref, acc = refs[len(mixers) :]
        lane = lax.broadcasted_iota(jnp.int32, (own, width), 1)

        def level(index):
            pieces = arrived_ref[index, own:].astype(f32)
            line = pieces[0:1] + pieces[1:2] + pieces[2:3]
            return jnp.broadcast_to(line, (8, width)).T[:own, 0:1]

        def rows_of(part):
            second = pltpu.roll(arrived_ref[3 * parts + part, :own].astype(f32), width // 2, 1)
            small = jnp.where(lane < width // 2, arrived_ref[2 * parts + part, :own].astype(f32), second)
            share = 1.0 / (1.0 + jnp.exp2(level(part) - level(parts + part)))
            large = arrived_ref[part, :own].astype(f32) * (1.0 - share) + arrived_ref[
                parts + part, :own
            ].astype(f32) * share
            return small.astype(bf16), large.astype(bf16)

        acc[...] = residual_ref[...].astype(f32) * residual_scale
        for ref, (_, shift, other) in zip(mixer_refs, mixers):
            y = lax.rem(place_ref[0] + shift + turns, turns)
            core = place_ref[1] if other == 0 else 1 - place_ref[1]
            both = rows_of(y * cores + core)
            acc[...] += jnp.dot(jnp.concatenate(both, axis=1), ref[...], preferred_element_type=f32)
        values = acc[...]
        center = jnp.mean(values, axis=-1, keepdims=True)
        values = values - center
        spread = jnp.mean(jnp.square(values), axis=-1, keepdims=True)
        out_ref[...] = (values * lax.rsqrt(spread + epsilon) * gain_ref[...]).astype(bf16)

    vm = pl.BlockSpec(memory_space=pltpu.VMEM)
    return pl.pallas_call(
        body,
        in_specs=[pl.BlockSpec(memory_space=pltpu.SMEM)] + [vm] * (len(mixers) + 3),
        out_specs=vm,
        scratch_shapes=[pltpu.VMEM((own, wide), f32)],
        out_shape=jax.ShapeDtypeStruct((own, wide), bf16),
        compiler_params=pltpu.CompilerParams(vmem_limit_bytes=40 * 2**20),
        cost_estimate=cost_of(5.0),
    )(place, arrived, *[m[0] for m in mixers], residual, gain.reshape(1, wide))


BLOCK = 768
LEAD = 16


def pack_weights(value_weight, gate_weight, down_weight):
    width, rows = value_weight.shape

    def body(v, g, d, out):
        for k, part in enumerate((v, g, d)):
            out[:, k * BLOCK : k * BLOCK + width] = part[...].T
            out[:, k * BLOCK + width : (k + 1) * BLOCK] = jnp.zeros((rows, BLOCK - width), bf16)

    vm = pl.BlockSpec(memory_space=pltpu.VMEM)
    return pl.pallas_call(
        body,
        in_specs=[vm] * 3,
        out_specs=vm,
        out_shape=jax.ShapeDtypeStruct((rows, 3 * BLOCK), bf16),
        cost_estimate=cost_of(1.5),
    )(value_weight, gate_weight, down_weight)


def window(array, k):
    return pl.BlockSpec((array.shape[0], BLOCK), lambda i: (0, k))


def whole(array):
    return pl.BlockSpec(array.shape, lambda i: (0,) * array.ndim)


def ups(chunks, weights, width, cost):
    rows = sum(c.shape[0] for c in chunks)

    def body(*refs):
        value_ref, gate_ref, out_value, out_gate = refs[len(chunks) :]
        x = jnp.concatenate([r[...] for r in refs[: len(chunks)]], axis=0)
        for ref, out in ((value_ref, out_value), (gate_ref, out_gate)):
            out[...] = jnp.dot(x, ref[:, :width], preferred_element_type=f32).astype(bf16)

    shape = jax.ShapeDtypeStruct((rows, width), bf16)
    return pl.pallas_call(
        body,
        grid=(1,),
        in_specs=[whole(c) for c in chunks] + [window(weights, 0), window(weights, 1)],
        out_specs=[whole(shape)] * 2,
        out_shape=[shape] * 2,
        compiler_params=pltpu.CompilerParams(vmem_limit_bytes=40 * 2**20),
        cost_estimate=cost_of(cost),
    )(*chunks, weights, weights)


def ends(place, pieces, spots, own, turns, cores):
    width = pieces[0][0].shape[1]

    def body(place_ref, *refs):
        outs, leaving = refs[-3:-1], refs[-1]
        spot = 0
        for k in range(0, len(refs) - 3, 2):
            for i in range(refs[k].shape[0] // own):
                shift, other = spots[spot]
                spot += 1
                y = lax.rem(place_ref[0] + shift + turns, turns)
                core = place_ref[1] if other == 0 else 1 - place_ref[1]
                for side in range(2):
                    outs[side][y * cores + core] = refs[k + side][(i + 1) * own - LEAD : (i + 1) * own]
        for side in range(2):
            leaving[side * LEAD : (side + 1) * LEAD] = outs[side][turns * cores - 1]

    vm = pl.BlockSpec(memory_space=pltpu.VMEM)
    flat = [a for pair in pieces for a in pair]
    return pl.pallas_call(
        body,
        in_specs=[pl.BlockSpec(memory_space=pltpu.SMEM)] + [vm] * len(flat),
        out_specs=[vm] * 3,
        out_shape=[jax.ShapeDtypeStruct((turns * cores, LEAD, width), bf16)] * 2
        + [jax.ShapeDtypeStruct((2 * LEAD, width), bf16)],
        cost_estimate=cost_of(1.5),
    )(place, *flat)


def downs(place, pieces, groups, tails, halo, value_taps, gate_taps, weights, own, turns, cores, cost):
    width = pieces[0][0].shape[1]
    wide = weights.shape[0]
    count = len(groups)

    def body(place_ref, *refs):
        vt_ref, gt_ref, down_ref, halo_ref = refs[:4]
        tail_refs = refs[4:6]
        up_refs = refs[6 : 6 + 2 * len(pieces)]
        theirs, mine, hidden, terms = refs[6 + 2 * len(pieces) :]

        def filtered(ref, taps, tail, side, at, part):
            halo_rows = halo_ref[side * LEAD : (side + 1) * LEAD].astype(f32)
            before = tail[jnp.maximum(part - 1, 0)].astype(f32)
            before = jnp.where(part == 0, halo_rows, before)
            here = ref[pl.ds(pl.multiple_of(at * own, LEAD), own)].astype(f32)
            rows = jnp.concatenate([before, here], axis=0)
            two = pltpu.roll(rows, 2, 0)[LEAD:]
            one = pltpu.roll(rows, 1, 0)[LEAD:]
            return taps[0:1] * two + taps[1:2] * one + taps[2:3] * rows[LEAD:]

        @pl.loop(0, 2)
        def _(turn):
            core = jnp.where(turn == 0, 1 - place_ref[1], place_ref[1])
            for i, (piece, at_own, at_other, shift) in enumerate(groups):
                at = jnp.where(turn == 0, at_other, at_own)
                part = lax.rem(place_ref[0] + shift + turns, turns) * cores + core
                value = filtered(up_refs[2 * piece], vt_ref, tail_refs[0], 0, at, part)
                gate = filtered(up_refs[2 * piece + 1], gt_ref, tail_refs[1], 1, at, part)
                hidden[i * own : (i + 1) * own] = (gate / (1.0 + jnp.exp(-gate)) * value).astype(bf16)
            terms[...] = lax.dot_general(
                hidden[...],
                down_ref[:, :width],
                (((1,), (1,)), ((), ())),
                preferred_element_type=f32,
            )
            for own_turn, out in enumerate((theirs, mine)):

                @pl.when(turn == own_turn)
                def _():
                    @pl.loop(0, count)
                    def _(i):
                        out[i] = terms[pl.ds(pl.multiple_of(i * own, LEAD), own)].astype(out.dtype)

    shapes = [jax.ShapeDtypeStruct((count, own, wide), t) for t in (bf16, f32)]
    flat = [a for pair in pieces for a in pair]
    return pl.pallas_call(
        body,
        grid=(1,),
        in_specs=[pl.BlockSpec(memory_space=pltpu.SMEM), whole(value_taps), whole(gate_taps)]
        + [window(weights, 2), whole(halo), whole(tails[0]), whole(tails[1])]
        + [whole(a) for a in flat],
        out_specs=[whole(x) for x in shapes],
        out_shape=shapes,
        scratch_shapes=[
            pltpu.VMEM((count * own, width), bf16),
            pltpu.VMEM((count * own, wide), f32),
        ],
        compiler_params=pltpu.CompilerParams(vmem_limit_bytes=50 * 2**20),
        cost_estimate=cost_of(cost),
    )(place, value_taps, gate_taps, weights, halo, *tails, *flat)


def paired(mine, theirs, kinds):
    count, own, wide = mine.shape

    def body(mine_ref, their_ref, *outs):
        for i, out in enumerate(outs):
            out[...] = (mine_ref[i] + their_ref[i].astype(f32)).astype(out.dtype)

    vm = pl.BlockSpec(memory_space=pltpu.VMEM)
    return pl.pallas_call(
        body,
        in_specs=[vm] * 2,
        out_specs=[vm] * count,
        out_shape=[jax.ShapeDtypeStruct((own, wide), kind) for kind in kinds],
        cost_estimate=cost_of(0.7 * count),
    )(mine, theirs)


def finish(mixed, own, shares, gain):
    rows, wide = mixed.shape

    def body(*refs):
        mixed_ref, own_ref = refs[:2]
        gain_ref, out_ref = refs[-2:]
        total = own_ref[...]
        for r in refs[2:-2]:
            total = total + r[...].astype(f32)
        values = residual_scale * mixed_ref[...].astype(f32) + total
        center = jnp.mean(values, axis=-1, keepdims=True)
        values = values - center
        spread = jnp.mean(jnp.square(values), axis=-1, keepdims=True)
        out_ref[...] = (values * lax.rsqrt(spread + epsilon) * gain_ref[...]).astype(bf16)

    vm = pl.BlockSpec(memory_space=pltpu.VMEM)
    return pl.pallas_call(
        body,
        in_specs=[vm] * (3 + len(shares)),
        out_specs=vm,
        out_shape=jax.ShapeDtypeStruct((rows, wide), bf16),
        cost_estimate=cost_of(2.0),
    )(mixed, own, *shares, gain.reshape(1, wide))


def per_device(
    query_small,
    key_small,
    value_small,
    gates_small,
    query_large,
    key_large,
    value_large,
    gates_large,
    residual,
    mixer_small,
    mixer_large,
    mix_gain,
    value_weight,
    gate_weight,
    value_taps,
    gate_taps,
    down_weight,
    final_gain,
):
    slot = lax.axis_index("sp_z").astype(jnp.int32)
    column = lax.axis_index("sp_x").astype(jnp.int32)
    depth, turns = lax.axis_size("sp_z"), lax.axis_size("sp_x")
    packed, *asked = pack(
        slot.reshape(1),
        key_small,
        value_small,
        key_large,
        value_large,
        query_small,
        query_large,
        gates_small.T,
        gates_large.T,
    )
    packed, value_turned, gate_turned, down_turned = lax.optimization_barrier(
        (packed, value_weight.T, gate_weight.T, down_weight)
    )
    pairs = lax.all_to_all(packed, "sp_z", split_axis=0, concat_axis=0, tiled=True)
    shards = pack_weights(value_turned, gate_turned, down_turned)
    pairs, shards, asked = lax.optimization_barrier((pairs, shards, asked))
    weights = lax.all_gather(shards, SP, axis=0, tiled=True)
    before = shifted(pairs, "sp_x", 1)
    after = shifted(pairs, "sp_x", -1)
    queries = [asked[0]] + [shifted(asked[k], "sp_z", k) for k in range(1, depth)]
    mixer = jnp.concatenate([mixer_small, mixer_large], axis=0)
    mixers = [mixer, shifted(mixer, "tp_y", 1), shifted(mixer, "tp_y", -1)]
    calls = ((0,), (-1, 1), (2,))
    tables = work_tables(calls, depth, turns)
    place_here = jnp.stack([slot, column])
    call = lambda k, chunks, state: attend(
        place_here,
        jnp.asarray(tables[k]),
        queries,
        chunks,
        state,
        k + 1 == len(calls),
        lax.axis_size(TP),
        0 in calls[k],
        12.0 * len(calls[k]),
    )
    state = call(0, [pairs], None)
    before, after, state, mixers = lax.optimization_barrier((before, after, state, mixers))
    far = [
        shifted(before[: depth // 2], "sp_x", 1),
        shifted(after[depth // 2 :], "sp_x", -1),
    ]
    mixers.append(shifted(mixers[1], "tp_y", 1))
    state = call(1, [before, after], state)
    far, state, mixers = lax.optimization_barrier((far, state, mixers))
    shifts = (0, -1, 1, 2)
    mixers = [(a, shift, 0) for a, shift in zip(mixers, shifts)] + [
        (shifted(a, "tp_c", 1), shift, 1) for a, shift in zip(mixers, shifts)
    ]
    state = call(2, far, state)
    arrived = lax.all_to_all(state, ("sp_z",) + TP, split_axis=0, concat_axis=0, tiled=True)
    place = jnp.stack([lax.axis_index("tp_y"), lax.axis_index("tp_c")]).astype(jnp.int32)
    mixed = mix_rows(place, arrived, mixers, residual, mix_gain)
    turns_y, cores = lax.axis_size("tp_y"), lax.axis_size("tp_c")
    own_rows = mixed.shape[0]
    half = own_rows // 2
    width = value_weight.shape[1]
    spots = [(0, 0), (0, 1), (-1, 0), (1, 0), (-1, 1), (1, 1), (2, 0), (2, 1)]
    last_one, next_one = shifted(mixed, "tp_y", 1), shifted(mixed, "tp_y", -1)
    near = ups([mixed, shifted(mixed, "tp_c", 1)], weights, width, 3.0)
    near, last_one, next_one = lax.optimization_barrier((near, last_one, next_one))
    opposite = [shifted(last_one[:half], "tp_y", 1), shifted(next_one[half:], "tp_y", -1)]
    beside = [last_one, next_one] + [shifted(a, "tp_c", 1) for a in (last_one, next_one)]
    beside = ups(beside, weights, width, 4.0)
    beside, opposite = lax.optimization_barrier((beside, opposite))
    opposite = ups(opposite + [shifted(a, "tp_c", 1) for a in opposite], weights, width, 3.0)
    pieces = [near, beside, opposite]
    *tails, leaving = ends(place, pieces, spots, own_rows, turns_y, cores)
    halo = passed_along(leaving, SP, 1)
    down = lambda chosen, groups, cost: downs(
        place,
        chosen,
        groups,
        tails,
        halo,
        value_taps,
        gate_taps,
        weights,
        own_rows,
        turns_y,
        cores,
        cost,
    )
    theirs, mine = down([opposite], [(0, 0, 1, 2)], 4.0)
    (distant,) = paired(mine, shifted(theirs, "tp_c", 1), [bf16])
    near, beside, distant = lax.optimization_barrier((near, beside, distant))
    shares = [shifted(distant, "tp_y", 2)]
    theirs, mine = down([near, beside], [(0, 0, 1, 0), (1, 0, 2, -1), (1, 1, 3, 1)], 8.0)
    own, before, after = paired(mine, shifted(theirs, "tp_c", 1), [f32, bf16, bf16])
    shares += [shifted(before, "tp_y", -1), shifted(after, "tp_y", 1)]
    return finish(mixed, own, shares, final_gain)


def solution(mesh):
    split = Mesh(mesh.devices.reshape(4, 4, 4, 2), ALL)
    placed = (P(SP, TP),) * 8 + (
        P(ALL, None),
        P(TP, None),
        P(TP, None),
        P(),
        P(SP, TP),
        P(SP, TP),
        P(None, TP),
        P(None, TP),
        P(TP, SP),
        P(),
    )

    return jax.shard_map(per_device, mesh=split, in_specs=placed, out_specs=P(ALL, None), check_vma=False)
```

```python
import math

import jax
import jax.numpy as jnp
import numpy as np
from jax import lax
from jax.experimental import pallas as pl
from jax.experimental.pallas import tpu as pltpu
from jax.sharding import Mesh
from jax.sharding import PartitionSpec as P


SP = ("sp_z", "sp_x")
TP = ("tp_y", "tp_c")
ALL = SP + TP
bf16 = jnp.bfloat16
f32 = jnp.float32
residual_scale = 2.0**0.5
epsilon = 1e-05


def shifted(value, axis, steps):
    count = lax.axis_size(axis)
    return lax.ppermute(value, axis, [(i, (i + steps) % count) for i in range(count)])


def passed_along(value, axis, steps):
    count = lax.axis_size(axis)
    first, last = (max(0, -steps), min(count, count - steps))
    return lax.ppermute(value, axis, [(source, source + steps) for source in range(first, last)])


LOW = -1e30
CHUNK = 256
EXTRA = 32
STAT_ROWS = 16
RATE = 250e6


def in_pieces(value):
    high = value.astype(bf16).astype(f32)
    middle = (value - high).astype(bf16).astype(f32)
    return high, middle, value - high - middle


def cost_of(us):
    return pl.CostEstimate(flops=int(us * RATE), transcendentals=0, bytes_accessed=0)


def pack(slot, key_small, value_small, key_large, value_large, query_small, query_large, gates_small, gates_large):
    rows, width = key_small.shape
    half = rows // 2
    low = width // 2
    tiles = rows // width

    def body(slot_ref, ks, vs, kl, vl, qs, ql, gs, gl, kv, *q):
        lane = lax.broadcasted_iota(jnp.int32, (rows, width), 1)
        turn = lambda ref: pltpu.roll(ref[...].astype(f32), low, 1)
        for slot in range(2):
            part = slice(slot * half, (slot + 1) * half)
            kv[slot, :half] = kl[part]
            kv[slot, half:rows] = vl[part]
        kv[2, :rows] = jnp.where(lane < low, ks[...].astype(f32), turn(vs)).astype(bf16)
        kv[3, :rows] = jnp.where(lane < low, turn(ks), vs[...].astype(f32)).astype(bf16)
        for shift in range(4):
            target = lax.rem(slot_ref[0] + shift, 4)

            @pl.when(target < 2)
            def _():
                q[shift][...] = ql[...]

            @pl.when(target == 2)
            def _():
                q[shift][...] = qs[...]

            @pl.when(target == 3)
            def _():
                q[shift][...] = turn(qs).astype(bf16)

        for slot, gate in ((0, gl[0:1]), (1, gl[0:1]), (2, gs[0:1]), (3, gs[1:2])):
            blocks = []
            for piece in in_pieces(gate):
                blocks += [piece[:, i * width : (i + 1) * width] for i in range(tiles)]
                blocks.append(jnp.zeros((8 - tiles, width), f32))
            blocks.append(jnp.zeros((EXTRA - 24, width), f32))
            kv[slot, rows:] = jnp.concatenate(blocks, axis=0).astype(bf16)

    vm = pl.BlockSpec(memory_space=pltpu.VMEM)
    return pl.pallas_call(
        body,
        in_specs=[pl.BlockSpec(memory_space=pltpu.SMEM)] + [vm] * 8,
        out_specs=[vm] * 5,
        out_shape=[jax.ShapeDtypeStruct((4, rows + EXTRA, width), bf16)]
        + [jax.ShapeDtypeStruct((rows, width), bf16)] * 4,
        cost_estimate=cost_of(2.5),
    )(slot, key_small, value_small, key_large, value_large, query_small, query_large, gates_small, gates_large)


def work_tables(calls, depth, turns):
    tables = []
    for here in range(turns):
        row = []
        for shifts in calls:
            steps = []
            for z in range(depth):
                for n, shift in enumerate(shifts):
                    there = (here + shift) % turns
                    for w in range(depth):
                        key, query = w * turns + there, z * turns + here
                        if key < query:
                            steps.append((z, n * depth + w, 0))
                for n, shift in enumerate(shifts):
                    if shift == 0:
                        steps.append((z, n * depth + z, 1))
            row.append(steps)
        tables.append(row)
    longest = [max(len(tables[h][k]) for h in range(turns)) + 1 for k in range(len(calls))]
    out = []
    for k in range(len(calls)):
        table = np.zeros((turns, longest[k] * 3 + 1), np.int32)
        for h in range(turns):
            flat = np.array(tables[h][k] + [(0, 0, 0)] * (longest[k] - len(tables[h][k])), np.int32)
            table[h, :-1] = flat.reshape(-1)
            table[h, -1] = len(tables[h][k])
        out.append(table)
    return out


def attend(where, table, queries, chunks, state, final, tensor_parts, has_diagonal, cost):
    depth = len(queries)
    rows, width = queries[0].shape
    half = rows // 2
    low = width // 2
    tiles = rows // width
    blocks = sum(c.shape[0] for c in chunks)
    columns = rows // CHUNK
    tall = width + 16
    last = table.shape[1] - 1
    own = rows // tensor_parts
    fresh = state is None

    def body(*refs):
        where_ref, table_ref = refs[:2]
        q_refs = refs[2 : 2 + depth]
        chunk_refs = refs[2 + depth : 2 + depth + len(chunks)]
        at = 2 + depth + len(chunks) + (0 if fresh else 2)
        state_in = () if fresh else refs[at - 2 : at]
        if final:
            out_ref = refs[at]
            acc, peak = refs[at + 1 : at + 3]
            scratch = refs[at + 3 :]
        else:
            acc, peak = refs[at : at + 2]
            scratch = refs[at + 2 :]
        qa, ka_small, va_small, ka_large, va_large, first = scratch
        slot = where_ref[0]
        column = where_ref[1]
        count = table_ref[column, last]

        @pl.loop(0, depth)
        def _(z):
            if fresh:
                acc[z] = jnp.zeros(acc.shape[1:], f32)
                peak[z] = jnp.full(peak.shape[1:], LOW, f32)
            else:
                acc[z] = state_in[0][z]
                peak[z] = state_in[1][z]

        def attention(small):
            d = low if small else width
            ext = d + 16
            span = rows if small else half
            tile = CHUNK if small else half
            parts = span // tile
            root = d**0.5
            rate = math.log2(math.e) / root
            ka, va = (ka_small, va_small) if small else (ka_large, va_large)
            deep = width if small else 2 * width
            lane = lax.broadcasted_iota(jnp.int32, (rows, width), 1)

            for shift, q_ref in enumerate(q_refs):
                z = lax.rem(slot + depth - shift, depth)
                q = q_ref[...]
                if small:
                    one = ((lane >= d) & (lane < d + 3)).astype(f32)
                    qa[z, :, :width] = jnp.where(lane < d, q.astype(f32), one).astype(bf16)
                else:
                    qa[z, :, :width] = q
                    qa[z, :, width:] = (lane < 3).astype(f32).astype(bf16)

            def prepare(ref, n, block):
                pieces = ref[n, rows : rows + 24].astype(f32)
                gate = pieces[0:8] + pieces[8:16] + pieces[16:24]
                bias = jnp.concatenate([gate[i : i + 1] for i in range(tiles)], axis=1) * -root
                bias = jnp.broadcast_to(bias, (8, rows))
                if not small:
                    bias = jnp.where(slot == 0, bias[:, :half], bias[:, half:])
                high, middle, rest = in_pieces(bias)
                row = lax.broadcasted_iota(jnp.int32, (8, span), 0)
                zero = jnp.zeros((8, span), f32)
                picked = jnp.where(row == 0, high, jnp.where(row == 1, middle, jnp.where(row == 2, rest, zero)))
                before = d if small else 0
                stack = [picked, jnp.zeros((width - before - 8, span), f32)]
                if before:
                    stack = [jnp.zeros((before, span), f32)] + stack
                gate_columns = jnp.concatenate(stack, axis=0).astype(bf16).T
                if small:
                    kv = ref[n, :rows]
                    ka[block] = jnp.where(lane < d, kv, gate_columns)
                    va[block, :d] = kv.T[d:]
                else:
                    ka[block, :, :width] = ref[n, :half]
                    ka[block, :, width:] = gate_columns
                    va[block, :d] = ref[n, half:rows].T
                va[block, d:] = jnp.ones((16, span), bf16)

            offset = 0
            for ref in chunk_refs:
                base = offset

                @pl.loop(0, ref.shape[0])
                def _(n):
                    prepare(ref, n, base + n)

                offset += ref.shape[0]

            def scores(z, block, c, t):
                return lax.dot_general(
                    ka[block, t * tile : (t + 1) * tile],
                    qa[z, c * CHUNK : (c + 1) * CHUNK, :deep],
                    (((1,), (1,)), ((), ())),
                    preferred_element_type=f32,
                )

            def masked(s, c, t, flag):
                if small and t < c:
                    return s
                key = lax.broadcasted_iota(jnp.int32, (tile, CHUNK), 0) + t * tile
                if not small:
                    key = key + slot * half
                    key = jnp.where(flag == 0, 0, key)
                query = lax.broadcasted_iota(jnp.int32, (tile, CHUNK), 1) + c * CHUNK
                return jnp.where(key <= query, s, LOW)

            def step(n, diagonal):
                z, block = table_ref[column, 3 * n], table_ref[column, 3 * n + 1]
                next_z, next_block = table_ref[column, 3 * n + 3], table_ref[column, 3 * n + 4]
                held_count = lambda c: c + 1 if diagonal and small else parts
                held = [first[t * tile : (t + 1) * tile] for t in range(held_count(0))]
                for c in range(columns):
                    cols = slice(c * CHUNK, (c + 1) * CHUNK)
                    if diagonal:
                        held = [masked(s, c, t, table_ref[column, 3 * n + 2]) for t, s in enumerate(held)]
                    top = held[0]
                    for s in held[1:]:
                        top = jnp.maximum(top, s)
                    old = peak[z, 0:1, cols]
                    new = jnp.maximum(old, jnp.max(top, axis=0, keepdims=True))
                    scaled = new * rate
                    factor = jnp.exp2(old * rate - scaled)
                    peak[z, 0:1, cols] = new
                    coming = []
                    added = None
                    following = c + 1 < columns
                    ahead = held_count(c + 1) if following else parts
                    for t in range(max(len(held), ahead)):
                        if t < ahead:
                            if following:
                                coming.append(scores(z, block, c + 1, t))
                            else:
                                first[t * tile : (t + 1) * tile] = scores(next_z, next_block, 0, t)
                        if t < len(held):
                            w = jnp.exp2(held[t] * rate - scaled).astype(bf16)
                            add = jnp.dot(
                                va[block, :, t * tile : (t + 1) * tile], w, preferred_element_type=f32
                            )
                            added = add if added is None else added + add
                    acc[z, :ext, cols] = acc[z, :ext, cols] * factor + added
                    held = coming

            for t in range(parts):
                first[t * tile : (t + 1) * tile] = scores(table_ref[column, 0], table_ref[column, 1], 0, t)

            @pl.loop(0, count)
            def _(n):
                if not has_diagonal or not small:
                    step(n, has_diagonal)
                    return
                diagonal = table_ref[column, 3 * n + 2]

                @pl.when(diagonal == 0)
                def _():
                    step(n, False)

                @pl.when(diagonal == 1)
                def _():
                    step(n, True)

            if final:

                @pl.loop(0, depth)
                def _(z):
                    total = acc[z, d : d + 1]
                    out = acc[z, :d] / total
                    if small:
                        out = jnp.concatenate([out, jnp.zeros((width - d, rows), f32)], axis=0)
                    out = out.T.astype(bf16)
                    level = peak[z, 0:1] * rate + jnp.log2(total)
                    stat = jnp.concatenate([*in_pieces(level), jnp.zeros((STAT_ROWS - 3, rows), f32)], axis=0)
                    for r in range(tensor_parts):
                        out_ref[z * tensor_parts + r, :own] = out[r * own : (r + 1) * own]
                        if not small:
                            mine = stat[:, r * own : (r + 1) * own]
                            mine = jnp.concatenate([mine, jnp.zeros((STAT_ROWS, width - own), f32)], axis=1)
                            out_ref[z * tensor_parts + r, own:] = mine.astype(bf16)
                        else:
                            out_ref[z * tensor_parts + r, own:] = jnp.zeros((STAT_ROWS, width), bf16)

        @pl.when(slot < 2)
        def _():
            attention(False)

        @pl.when(slot >= 2)
        def _():
            attention(True)

    vm = pl.BlockSpec(memory_space=pltpu.VMEM)
    sm = pl.BlockSpec(memory_space=pltpu.SMEM)
    state_shapes = [((depth, tall, rows), f32), ((depth, 8, rows), f32)]
    scratch = [pltpu.VMEM(s, t) for s, t in state_shapes] if final else []
    scratch += [
        pltpu.VMEM((depth, rows, 2 * width), bf16),
        pltpu.VMEM((blocks, rows, width), bf16),
        pltpu.VMEM((blocks, low + 16, rows), bf16),
        pltpu.VMEM((blocks, half, 2 * width), bf16),
        pltpu.VMEM((blocks, tall, half), bf16),
        pltpu.VMEM((rows, CHUNK), f32),
    ]
    if final:
        out_shape = jax.ShapeDtypeStruct((depth * tensor_parts, own + STAT_ROWS, width), bf16)
        out_specs = vm
    else:
        out_shape = [jax.ShapeDtypeStruct(s, t) for s, t in state_shapes]
        out_specs = [vm, vm]
    args = [where, table, *queries, *chunks] + ([] if fresh else list(state))
    return pl.pallas_call(
        body,
        in_specs=[sm, sm] + [vm] * (len(args) - 2),
        out_specs=out_specs,
        scratch_shapes=scratch,
        out_shape=out_shape,
        compiler_params=pltpu.CompilerParams(vmem_limit_bytes=30 * 2**20),
        cost_estimate=cost_of(cost),
    )(*args)


def mix_rows(place, arrived, mixers, residual, gain):
    own, wide = residual.shape
    width = arrived.shape[2]
    cores = 2
    turns = arrived.shape[0] // 4 // cores
    parts = turns * cores

    def body(place_ref, arrived_ref, *refs):
        mixer_refs = refs[: len(mixers)]
        residual_ref, gain_ref, out_ref, acc = refs[len(mixers) :]
        lane = lax.broadcasted_iota(jnp.int32, (own, width), 1)

        def level(index):
            pieces = arrived_ref[index, own:].astype(f32)
            line = pieces[0:1] + pieces[1:2] + pieces[2:3]
            return jnp.broadcast_to(line, (8, width)).T[:own, 0:1]

        def rows_of(part):
            second = pltpu.roll(arrived_ref[3 * parts + part, :own].astype(f32), width // 2, 1)
            small = jnp.where(lane < width // 2, arrived_ref[2 * parts + part, :own].astype(f32), second)
            share = 1.0 / (1.0 + jnp.exp2(level(part) - level(parts + part)))
            large = arrived_ref[part, :own].astype(f32) * (1.0 - share) + arrived_ref[
                parts + part, :own
            ].astype(f32) * share
            return small.astype(bf16), large.astype(bf16)

        acc[...] = residual_ref[...].astype(f32) * residual_scale
        for ref, (_, shift, other) in zip(mixer_refs, mixers):
            y = lax.rem(place_ref[0] + shift + turns, turns)
            core = place_ref[1] if other == 0 else 1 - place_ref[1]
            both = rows_of(y * cores + core)
            acc[...] += jnp.dot(jnp.concatenate(both, axis=1), ref[...], preferred_element_type=f32)
        values = acc[...]
        center = jnp.mean(values, axis=-1, keepdims=True)
        values = values - center
        spread = jnp.mean(jnp.square(values), axis=-1, keepdims=True)
        out_ref[...] = (values * lax.rsqrt(spread + epsilon) * gain_ref[...]).astype(bf16)

    vm = pl.BlockSpec(memory_space=pltpu.VMEM)
    return pl.pallas_call(
        body,
        in_specs=[pl.BlockSpec(memory_space=pltpu.SMEM)] + [vm] * (len(mixers) + 3),
        out_specs=vm,
        scratch_shapes=[pltpu.VMEM((own, wide), f32)],
        out_shape=jax.ShapeDtypeStruct((own, wide), bf16),
        compiler_params=pltpu.CompilerParams(vmem_limit_bytes=24 * 2**20),
        cost_estimate=cost_of(5.0),
    )(place, arrived, *[m[0] for m in mixers], residual, gain.reshape(1, wide))


BLOCK = 768
LEAD = 16


def pack_weights(value_weight, gate_weight, down_weight):
    width, rows = value_weight.shape

    def body(v, g, d, out):
        for k, part in enumerate((v, g, d)):
            out[:, k * BLOCK : k * BLOCK + width] = part[...].T
            out[:, k * BLOCK + width : (k + 1) * BLOCK] = jnp.zeros((rows, BLOCK - width), bf16)

    vm = pl.BlockSpec(memory_space=pltpu.VMEM)
    return pl.pallas_call(
        body,
        in_specs=[vm] * 3,
        out_specs=vm,
        out_shape=jax.ShapeDtypeStruct((rows, 3 * BLOCK), bf16),
        cost_estimate=cost_of(1.5),
    )(value_weight, gate_weight, down_weight)


def window(array, k):
    return pl.BlockSpec((array.shape[0], BLOCK), lambda i: (0, k))


def whole(array):
    return pl.BlockSpec(array.shape, lambda i: (0,) * array.ndim)


def ups(chunks, weights, width, cost, earlier=(), place=None, spots=(), turns=0, cores=0):
    rows = sum(c.shape[0] for c in chunks)
    own = chunks[0].shape[0] * len(chunks) // 2 if earlier else 0
    flat = [a for pair in earlier for a in pair]

    def body(*refs):
        place_ref, chunk_refs = refs[0], refs[1 : 1 + len(chunks)]
        value_ref, gate_ref = refs[1 + len(chunks) : 3 + len(chunks)]
        done = refs[3 + len(chunks) : 3 + len(chunks) + len(flat)]
        outs = refs[3 + len(chunks) + len(flat) :]
        x = jnp.concatenate([r[...] for r in chunk_refs], axis=0)
        for ref, out in ((value_ref, outs[0]), (gate_ref, outs[1])):
            out[...] = jnp.dot(x, ref[:, :width], preferred_element_type=f32).astype(bf16)
        if not earlier:
            return
        tails, leaving = outs[2:4], outs[4]
        pieces = (*done, *outs[:2])
        spot = 0
        for k in range(0, len(pieces), 2):
            for i in range(pieces[k].shape[0] // own):
                shift, other = spots[spot]
                spot += 1
                y = lax.rem(place_ref[0] + shift + turns, turns)
                core = place_ref[1] if other == 0 else 1 - place_ref[1]
                for side in range(2):
                    tails[side][y * cores + core] = pieces[k + side][(i + 1) * own - LEAD : (i + 1) * own]
        for side in range(2):
            leaving[side * LEAD : (side + 1) * LEAD] = tails[side][turns * cores - 1]

    shapes = [jax.ShapeDtypeStruct((rows, width), bf16)] * 2
    if earlier:
        shapes += [jax.ShapeDtypeStruct((turns * cores, LEAD, width), bf16)] * 2
        shapes.append(jax.ShapeDtypeStruct((2 * LEAD, width), bf16))
    return pl.pallas_call(
        body,
        grid=(1,),
        in_specs=[pl.BlockSpec(memory_space=pltpu.SMEM)]
        + [whole(c) for c in chunks]
        + [window(weights, 0), window(weights, 1)]
        + [whole(a) for a in flat],
        out_specs=[whole(x) for x in shapes],
        out_shape=shapes,
        compiler_params=pltpu.CompilerParams(vmem_limit_bytes=24 * 2**20),
        cost_estimate=cost_of(cost),
    )(place, *chunks, weights, weights, *flat)


def downs(place, pieces, groups, tails, halo, value_taps, gate_taps, weights, own, turns, cores, cost):
    width = pieces[0][0].shape[1]
    wide = weights.shape[0]
    count = len(groups)

    def body(place_ref, *refs):
        vt_ref, gt_ref, down_ref, halo_ref = refs[:4]
        tail_refs = refs[4:6]
        up_refs = refs[6 : 6 + 2 * len(pieces)]
        theirs, mine, hidden, terms = refs[6 + 2 * len(pieces) :]

        def filtered(ref, taps, tail, side, at, part):
            halo_rows = halo_ref[side * LEAD : (side + 1) * LEAD].astype(f32)
            before = tail[jnp.maximum(part - 1, 0)].astype(f32)
            before = jnp.where(part == 0, halo_rows, before)
            here = ref[pl.ds(pl.multiple_of(at * own, LEAD), own)].astype(f32)
            rows = jnp.concatenate([before, here], axis=0)
            two = pltpu.roll(rows, 2, 0)[LEAD:]
            one = pltpu.roll(rows, 1, 0)[LEAD:]
            return taps[0:1] * two + taps[1:2] * one + taps[2:3] * rows[LEAD:]

        @pl.loop(0, 2)
        def _(turn):
            core = jnp.where(turn == 0, 1 - place_ref[1], place_ref[1])
            for i, (piece, at_own, at_other, shift) in enumerate(groups):
                at = jnp.where(turn == 0, at_other, at_own)
                part = lax.rem(place_ref[0] + shift + turns, turns) * cores + core
                value = filtered(up_refs[2 * piece], vt_ref, tail_refs[0], 0, at, part)
                gate = filtered(up_refs[2 * piece + 1], gt_ref, tail_refs[1], 1, at, part)
                hidden[i * own : (i + 1) * own] = (gate / (1.0 + jnp.exp(-gate)) * value).astype(bf16)
            terms[...] = lax.dot_general(
                hidden[...],
                down_ref[:, :width],
                (((1,), (1,)), ((), ())),
                preferred_element_type=f32,
            )
            for own_turn, out in enumerate((theirs, mine)):

                @pl.when(turn == own_turn)
                def _():
                    @pl.loop(0, count)
                    def _(i):
                        out[i] = terms[pl.ds(pl.multiple_of(i * own, LEAD), own)].astype(out.dtype)

    shapes = [jax.ShapeDtypeStruct((count, own, wide), t) for t in (bf16, f32)]
    flat = [a for pair in pieces for a in pair]
    return pl.pallas_call(
        body,
        grid=(1,),
        in_specs=[pl.BlockSpec(memory_space=pltpu.SMEM), whole(value_taps), whole(gate_taps)]
        + [window(weights, 2), whole(halo), whole(tails[0]), whole(tails[1])]
        + [whole(a) for a in flat],
        out_specs=[whole(x) for x in shapes],
        out_shape=shapes,
        scratch_shapes=[
            pltpu.VMEM((count * own, width), bf16),
            pltpu.VMEM((count * own, wide), f32),
        ],
        compiler_params=pltpu.CompilerParams(vmem_limit_bytes=24 * 2**20),
        cost_estimate=cost_of(cost),
    )(place, value_taps, gate_taps, weights, halo, *tails, *flat)


def paired(mine, theirs, kinds):
    count, own, wide = mine.shape

    def body(mine_ref, their_ref, *outs):
        for i, out in enumerate(outs):
            out[...] = (mine_ref[i] + their_ref[i].astype(f32)).astype(out.dtype)

    vm = pl.BlockSpec(memory_space=pltpu.VMEM)
    return pl.pallas_call(
        body,
        in_specs=[vm] * 2,
        out_specs=[vm] * count,
        out_shape=[jax.ShapeDtypeStruct((own, wide), kind) for kind in kinds],
        cost_estimate=cost_of(0.7 * count),
    )(mine, theirs)


def finish(mixed, own, shares, gain):
    rows, wide = mixed.shape

    def body(*refs):
        mixed_ref, own_ref = refs[:2]
        gain_ref, out_ref = refs[-2:]
        total = own_ref[...]
        for r in refs[2:-2]:
            total = total + r[...].astype(f32)
        values = residual_scale * mixed_ref[...].astype(f32) + total
        center = jnp.mean(values, axis=-1, keepdims=True)
        values = values - center
        spread = jnp.mean(jnp.square(values), axis=-1, keepdims=True)
        out_ref[...] = (values * lax.rsqrt(spread + epsilon) * gain_ref[...]).astype(bf16)

    vm = pl.BlockSpec(memory_space=pltpu.VMEM)
    return pl.pallas_call(
        body,
        in_specs=[vm] * (3 + len(shares)),
        out_specs=vm,
        out_shape=jax.ShapeDtypeStruct((rows, wide), bf16),
        cost_estimate=cost_of(2.0),
    )(mixed, own, *shares, gain.reshape(1, wide))


def per_device(
    query_small,
    key_small,
    value_small,
    gates_small,
    query_large,
    key_large,
    value_large,
    gates_large,
    residual,
    mixer_small,
    mixer_large,
    mix_gain,
    value_weight,
    gate_weight,
    value_taps,
    gate_taps,
    down_weight,
    final_gain,
):
    slot = lax.axis_index("sp_z").astype(jnp.int32)
    column = lax.axis_index("sp_x").astype(jnp.int32)
    depth, turns = lax.axis_size("sp_z"), lax.axis_size("sp_x")
    packed, *asked = pack(
        slot.reshape(1),
        key_small,
        value_small,
        key_large,
        value_large,
        query_small,
        query_large,
        gates_small.T,
        gates_large.T,
    )
    packed, value_turned, gate_turned, down_turned = lax.optimization_barrier(
        (packed, value_weight.T, gate_weight.T, down_weight)
    )
    pairs = lax.all_to_all(packed, "sp_z", split_axis=0, concat_axis=0, tiled=True)
    shards = pack_weights(value_turned, gate_turned, down_turned)
    pairs, shards, asked = lax.optimization_barrier((pairs, shards, asked))
    weights = lax.all_gather(shards, SP, axis=0, tiled=True)
    before = shifted(pairs, "sp_x", 1)
    after = shifted(pairs, "sp_x", -1)
    queries = [asked[0]] + [shifted(asked[k], "sp_z", k) for k in range(1, depth)]
    mixer = jnp.concatenate([mixer_small, mixer_large], axis=0)
    mixers = [mixer] + [shifted(mixer, "tp_y", k) for k in (1, -1, 2)]
    calls = ((0,), (-1, 1), (2,))
    tables = work_tables(calls, depth, turns)
    place_here = jnp.stack([slot, column])
    call = lambda k, chunks, state: attend(
        place_here,
        jnp.asarray(tables[k]),
        queries,
        chunks,
        state,
        k + 1 == len(calls),
        lax.axis_size(TP),
        0 in calls[k],
        12.0 * len(calls[k]),
    )
    state = call(0, [pairs], None)
    pairs, before, after, state = lax.optimization_barrier((pairs, before, after, state))
    far = shifted(pairs, "sp_x", 2)
    state = call(1, [before, after], state)
    far, state, mixers = lax.optimization_barrier((far, state, mixers))
    shifts = (0, -1, 1, 2)
    mixers = [(a, shift, 0) for a, shift in zip(mixers, shifts)] + [
        (shifted(a, "tp_c", 1), shift, 1) for a, shift in zip(mixers, shifts)
    ]
    state = call(2, [far], state)
    arrived = lax.all_to_all(state, ("sp_z",) + TP, split_axis=0, concat_axis=0, tiled=True)
    place = jnp.stack([lax.axis_index("tp_y"), lax.axis_index("tp_c")]).astype(jnp.int32)
    arrived, weights = lax.optimization_barrier((arrived, weights))
    mixed = mix_rows(place, arrived, mixers, residual, mix_gain)
    turns_y, cores = lax.axis_size("tp_y"), lax.axis_size("tp_c")
    own_rows = mixed.shape[0]
    half = own_rows // 2
    width = value_weight.shape[1]
    spots = [(0, 0), (0, 1), (-1, 0), (1, 0), (-1, 1), (1, 1), (2, 0), (2, 1)]
    last_one, next_one = shifted(mixed, "tp_y", 1), shifted(mixed, "tp_y", -1)
    near = ups([mixed, shifted(mixed, "tp_c", 1)], weights, width, 3.0, place=place)
    near, last_one, next_one = lax.optimization_barrier((near, last_one, next_one))
    opposite = [shifted(last_one[:half], "tp_y", 1), shifted(next_one[half:], "tp_y", -1)]
    beside = [last_one, next_one] + [shifted(a, "tp_c", 1) for a in (last_one, next_one)]
    beside = ups(beside, weights, width, 4.0, place=place)
    beside, opposite = lax.optimization_barrier((beside, opposite))
    opposite += [shifted(a, "tp_c", 1) for a in opposite]
    up_value, up_gate, *tails, leaving = ups(
        opposite, weights, width, 3.0, (near, beside), place, spots, turns_y, cores
    )
    opposite = [up_value, up_gate]
    halo = passed_along(leaving, SP, 1)
    down = lambda chosen, groups, cost: downs(
        place,
        chosen,
        groups,
        tails,
        halo,
        value_taps,
        gate_taps,
        weights,
        own_rows,
        turns_y,
        cores,
        cost,
    )
    theirs, mine = down([opposite], [(0, 0, 1, 2)], 4.0)
    (distant,) = paired(mine, shifted(theirs, "tp_c", 1), [bf16])
    near, beside, distant = lax.optimization_barrier((near, beside, distant))
    shares = [shifted(distant, "tp_y", 2)]
    theirs, mine = down([near, beside], [(0, 0, 1, 0), (1, 0, 2, -1), (1, 1, 3, 1)], 8.0)
    own, before, after = paired(mine, shifted(theirs, "tp_c", 1), [f32, bf16, bf16])
    shares += [shifted(before, "tp_y", -1), shifted(after, "tp_y", 1)]
    return finish(mixed, own, shares, final_gain)


def solution(mesh):
    split = Mesh(mesh.devices.reshape(4, 4, 4, 2), ALL)
    placed = (P(SP, TP),) * 8 + (
        P(ALL, None),
        P(TP, None),
        P(TP, None),
        P(),
        P(SP, TP),
        P(SP, TP),
        P(None, TP),
        P(None, TP),
        P(TP, SP),
        P(),
    )

    return jax.shard_map(per_device, mesh=split, in_specs=placed, out_specs=P(ALL, None), check_vma=False)
```

```python
import math

import jax
import jax.numpy as jnp
import numpy as np
from jax import lax
from jax.experimental import pallas as pl
from jax.experimental.pallas import tpu as pltpu
from jax.sharding import Mesh
from jax.sharding import PartitionSpec as P


SP = ("sp_z", "sp_x")
TP = ("tp_y", "tp_c")
ALL = SP + TP
bf16 = jnp.bfloat16
f32 = jnp.float32
residual_scale = 2.0**0.5
epsilon = 1e-05


def shifted(value, axis, steps):
    count = lax.axis_size(axis)
    return lax.ppermute(value, axis, [(i, (i + steps) % count) for i in range(count)])


def passed_along(value, axis, steps):
    count = lax.axis_size(axis)
    first, last = (max(0, -steps), min(count, count - steps))
    return lax.ppermute(value, axis, [(source, source + steps) for source in range(first, last)])


LOW = -1e30
CHUNK = 256
EXTRA = 32
STAT_ROWS = 16
RATE = 250e6


def in_pieces(value):
    high = value.astype(bf16).astype(f32)
    middle = (value - high).astype(bf16).astype(f32)
    return high, middle, value - high - middle


def cost_of(us):
    return pl.CostEstimate(flops=int(us * RATE), transcendentals=0, bytes_accessed=0)


def pack(slot, key_small, value_small, key_large, value_large, query_small, query_large, gates_small, gates_large):
    rows, width = key_small.shape
    half = rows // 2
    low = width // 2
    tiles = rows // width

    def body(slot_ref, ks, vs, kl, vl, qs, ql, gs, gl, kv, *q):
        lane = lax.broadcasted_iota(jnp.int32, (rows, width), 1)
        turn = lambda ref: pltpu.roll(ref[...].astype(f32), low, 1)
        for slot in range(2):
            part = slice(slot * half, (slot + 1) * half)
            kv[slot, :half] = kl[part]
            kv[slot, half:rows] = vl[part]
        kv[2, :rows] = jnp.where(lane < low, ks[...].astype(f32), turn(vs)).astype(bf16)
        kv[3, :rows] = jnp.where(lane < low, turn(ks), vs[...].astype(f32)).astype(bf16)
        for shift in range(4):
            target = lax.rem(slot_ref[0] + shift, 4)

            @pl.when(target < 2)
            def _():
                q[shift][...] = ql[...]

            @pl.when(target == 2)
            def _():
                q[shift][...] = qs[...]

            @pl.when(target == 3)
            def _():
                q[shift][...] = turn(qs).astype(bf16)

        for slot, gate in ((0, gl[0:1]), (1, gl[0:1]), (2, gs[0:1]), (3, gs[1:2])):
            blocks = []
            for piece in in_pieces(gate):
                blocks += [piece[:, i * width : (i + 1) * width] for i in range(tiles)]
                blocks.append(jnp.zeros((8 - tiles, width), f32))
            blocks.append(jnp.zeros((EXTRA - 24, width), f32))
            kv[slot, rows:] = jnp.concatenate(blocks, axis=0).astype(bf16)

    vm = pl.BlockSpec(memory_space=pltpu.VMEM)
    return pl.pallas_call(
        body,
        in_specs=[pl.BlockSpec(memory_space=pltpu.SMEM)] + [vm] * 8,
        out_specs=[vm] * 5,
        out_shape=[jax.ShapeDtypeStruct((4, rows + EXTRA, width), bf16)]
        + [jax.ShapeDtypeStruct((rows, width), bf16)] * 4,
        cost_estimate=cost_of(2.5),
    )(slot, key_small, value_small, key_large, value_large, query_small, query_large, gates_small, gates_large)


def work_tables(calls, depth, turns):
    tables = []
    for here in range(turns):
        row = []
        for shifts in calls:
            steps = []
            for z in range(depth):
                for n, shift in enumerate(shifts):
                    there = (here + shift) % turns
                    for w in range(depth):
                        key, query = w * turns + there, z * turns + here
                        if key < query:
                            steps.append((z, n * depth + w, 0))
                for n, shift in enumerate(shifts):
                    if shift == 0:
                        steps.append((z, n * depth + z, 1))
            row.append(steps)
        tables.append(row)
    longest = [max(len(tables[h][k]) for h in range(turns)) + 1 for k in range(len(calls))]
    out = []
    for k in range(len(calls)):
        table = np.zeros((turns, longest[k] * 3 + 1), np.int32)
        for h in range(turns):
            flat = np.array(tables[h][k] + [(0, 0, 0)] * (longest[k] - len(tables[h][k])), np.int32)
            table[h, :-1] = flat.reshape(-1)
            table[h, -1] = len(tables[h][k])
        out.append(table)
    return out


def attend(where, table, queries, chunks, state, final, tensor_parts, has_diagonal, cost):
    depth = len(queries)
    rows, width = queries[0].shape
    half = rows // 2
    low = width // 2
    tiles = rows // width
    blocks = sum(c.shape[0] for c in chunks)
    columns = rows // CHUNK
    tall = width + 16
    last = table.shape[1] - 1
    own = rows // tensor_parts
    fresh = state is None

    def body(*refs):
        where_ref, table_ref = refs[:2]
        q_refs = refs[2 : 2 + depth]
        chunk_refs = refs[2 + depth : 2 + depth + len(chunks)]
        at = 2 + depth + len(chunks) + (0 if fresh else 2)
        state_in = () if fresh else refs[at - 2 : at]
        if final:
            out_ref = refs[at]
            acc, peak = refs[at + 1 : at + 3]
            scratch = refs[at + 3 :]
        else:
            acc, peak = refs[at : at + 2]
            scratch = refs[at + 2 :]
        qa, ka_small, va_small, ka_large, va_large, first = scratch
        slot = where_ref[0]
        column = where_ref[1]
        count = table_ref[column, last]

        @pl.loop(0, depth)
        def _(z):
            if fresh:
                acc[z] = jnp.zeros(acc.shape[1:], f32)
                peak[z] = jnp.full(peak.shape[1:], LOW, f32)
            else:
                acc[z] = state_in[0][z]
                peak[z] = state_in[1][z]

        def attention(small):
            d = low if small else width
            ext = d + 16
            span = rows if small else half
            tile = CHUNK if small else half
            parts = span // tile
            root = d**0.5
            rate = math.log2(math.e) / root
            ka, va = (ka_small, va_small) if small else (ka_large, va_large)
            deep = width if small else 2 * width
            lane = lax.broadcasted_iota(jnp.int32, (rows, width), 1)

            for shift, q_ref in enumerate(q_refs):
                z = lax.rem(slot + depth - shift, depth)
                q = q_ref[...]
                if small:
                    one = ((lane >= d) & (lane < d + 3)).astype(f32)
                    qa[z, :, :width] = jnp.where(lane < d, q.astype(f32), one).astype(bf16)
                else:
                    qa[z, :, :width] = q
                    qa[z, :, width:] = (lane < 3).astype(f32).astype(bf16)

            def prepare(ref, n, block):
                pieces = ref[n, rows : rows + 24].astype(f32)
                gate = pieces[0:8] + pieces[8:16] + pieces[16:24]
                bias = jnp.concatenate([gate[i : i + 1] for i in range(tiles)], axis=1) * -root
                bias = jnp.broadcast_to(bias, (8, rows))
                if not small:
                    bias = jnp.where(slot == 0, bias[:, :half], bias[:, half:])
                high, middle, rest = in_pieces(bias)
                row = lax.broadcasted_iota(jnp.int32, (8, span), 0)
                zero = jnp.zeros((8, span), f32)
                picked = jnp.where(row == 0, high, jnp.where(row == 1, middle, jnp.where(row == 2, rest, zero)))
                before = d if small else 0
                stack = [picked, jnp.zeros((width - before - 8, span), f32)]
                if before:
                    stack = [jnp.zeros((before, span), f32)] + stack
                gate_columns = jnp.concatenate(stack, axis=0).astype(bf16).T
                if small:
                    kv = ref[n, :rows]
                    ka[block] = jnp.where(lane < d, kv, gate_columns)
                    va[block, :d] = kv.T[d:]
                else:
                    ka[block, :, :width] = ref[n, :half]
                    ka[block, :, width:] = gate_columns
                    va[block, :d] = ref[n, half:rows].T
                va[block, d:] = jnp.ones((16, span), bf16)

            offset = 0
            for ref in chunk_refs:
                base = offset

                @pl.loop(0, ref.shape[0])
                def _(n):
                    prepare(ref, n, base + n)

                offset += ref.shape[0]

            def scores(z, block, c, t):
                return lax.dot_general(
                    ka[block, t * tile : (t + 1) * tile],
                    qa[z, c * CHUNK : (c + 1) * CHUNK, :deep],
                    (((1,), (1,)), ((), ())),
                    preferred_element_type=f32,
                )

            def masked(s, c, t, flag):
                if small and t < c:
                    return s
                key = lax.broadcasted_iota(jnp.int32, (tile, CHUNK), 0) + t * tile
                if not small:
                    key = key + slot * half
                    key = jnp.where(flag == 0, 0, key)
                query = lax.broadcasted_iota(jnp.int32, (tile, CHUNK), 1) + c * CHUNK
                return jnp.where(key <= query, s, LOW)

            def step(n, diagonal):
                z, block = table_ref[column, 3 * n], table_ref[column, 3 * n + 1]
                next_z, next_block = table_ref[column, 3 * n + 3], table_ref[column, 3 * n + 4]
                held_count = lambda c: c + 1 if diagonal and small else parts
                held = [first[t * tile : (t + 1) * tile] for t in range(held_count(0))]
                for c in range(columns):
                    cols = slice(c * CHUNK, (c + 1) * CHUNK)
                    if diagonal:
                        held = [masked(s, c, t, table_ref[column, 3 * n + 2]) for t, s in enumerate(held)]
                    top = held[0]
                    for s in held[1:]:
                        top = jnp.maximum(top, s)
                    old = peak[z, 0:1, cols]
                    new = jnp.maximum(old, jnp.max(top, axis=0, keepdims=True))
                    scaled = new * rate
                    factor = jnp.exp2(old * rate - scaled)
                    peak[z, 0:1, cols] = new
                    coming = []
                    added = None
                    following = c + 1 < columns
                    ahead = held_count(c + 1) if following else parts
                    for t in range(max(len(held), ahead)):
                        if t < ahead:
                            if following:
                                coming.append(scores(z, block, c + 1, t))
                            else:
                                first[t * tile : (t + 1) * tile] = scores(next_z, next_block, 0, t)
                        if t < len(held):
                            w = jnp.exp2(held[t] * rate - scaled).astype(bf16)
                            add = jnp.dot(
                                va[block, :, t * tile : (t + 1) * tile], w, preferred_element_type=f32
                            )
                            added = add if added is None else added + add
                    acc[z, :ext, cols] = acc[z, :ext, cols] * factor + added
                    held = coming

            for t in range(parts):
                first[t * tile : (t + 1) * tile] = scores(table_ref[column, 0], table_ref[column, 1], 0, t)

            @pl.loop(0, count)
            def _(n):
                if not has_diagonal or not small:
                    step(n, has_diagonal)
                    return
                diagonal = table_ref[column, 3 * n + 2]

                @pl.when(diagonal == 0)
                def _():
                    step(n, False)

                @pl.when(diagonal == 1)
                def _():
                    step(n, True)

            if final:

                @pl.loop(0, depth)
                def _(z):
                    total = acc[z, d : d + 1]
                    out = acc[z, :d] / total
                    if small:
                        out = jnp.concatenate([out, jnp.zeros((width - d, rows), f32)], axis=0)
                    out = out.T.astype(bf16)
                    level = peak[z, 0:1] * rate + jnp.log2(total)
                    stat = jnp.concatenate([*in_pieces(level), jnp.zeros((STAT_ROWS - 3, rows), f32)], axis=0)
                    for r in range(tensor_parts):
                        out_ref[z * tensor_parts + r, :own] = out[r * own : (r + 1) * own]
                        if not small:
                            mine = stat[:, r * own : (r + 1) * own]
                            mine = jnp.concatenate([mine, jnp.zeros((STAT_ROWS, width - own), f32)], axis=1)
                            out_ref[z * tensor_parts + r, own:] = mine.astype(bf16)
                        else:
                            out_ref[z * tensor_parts + r, own:] = jnp.zeros((STAT_ROWS, width), bf16)

        @pl.when(slot < 2)
        def _():
            attention(False)

        @pl.when(slot >= 2)
        def _():
            attention(True)

    vm = pl.BlockSpec(memory_space=pltpu.VMEM)
    sm = pl.BlockSpec(memory_space=pltpu.SMEM)
    state_shapes = [((depth, tall, rows), f32), ((depth, 8, rows), f32)]
    scratch = [pltpu.VMEM(s, t) for s, t in state_shapes] if final else []
    scratch += [
        pltpu.VMEM((depth, rows, 2 * width), bf16),
        pltpu.VMEM((blocks, rows, width), bf16),
        pltpu.VMEM((blocks, low + 16, rows), bf16),
        pltpu.VMEM((blocks, half, 2 * width), bf16),
        pltpu.VMEM((blocks, tall, half), bf16),
        pltpu.VMEM((rows, CHUNK), f32),
    ]
    if final:
        out_shape = jax.ShapeDtypeStruct((depth * tensor_parts, own + STAT_ROWS, width), bf16)
        out_specs = vm
    else:
        out_shape = [jax.ShapeDtypeStruct(s, t) for s, t in state_shapes]
        out_specs = [vm, vm]
    args = [where, table, *queries, *chunks] + ([] if fresh else list(state))
    return pl.pallas_call(
        body,
        in_specs=[sm, sm] + [vm] * (len(args) - 2),
        out_specs=out_specs,
        scratch_shapes=scratch,
        out_shape=out_shape,
        compiler_params=pltpu.CompilerParams(vmem_limit_bytes=30 * 2**20),
        cost_estimate=cost_of(cost),
    )(*args)


def mix_rows(place, arrived, mixers, residual, gain):
    own, wide = residual.shape
    width = arrived.shape[2]
    cores = 2
    turns = arrived.shape[0] // 4 // cores
    parts = turns * cores

    def body(place_ref, arrived_ref, *refs):
        mixer_refs = refs[: len(mixers)]
        residual_ref, gain_ref, out_ref, acc = refs[len(mixers) :]
        lane = lax.broadcasted_iota(jnp.int32, (own, width), 1)

        def level(index):
            pieces = arrived_ref[index, own:].astype(f32)
            line = pieces[0:1] + pieces[1:2] + pieces[2:3]
            return jnp.broadcast_to(line, (8, width)).T[:own, 0:1]

        def rows_of(part):
            second = pltpu.roll(arrived_ref[3 * parts + part, :own].astype(f32), width // 2, 1)
            small = jnp.where(lane < width // 2, arrived_ref[2 * parts + part, :own].astype(f32), second)
            share = 1.0 / (1.0 + jnp.exp2(level(part) - level(parts + part)))
            large = arrived_ref[part, :own].astype(f32) * (1.0 - share) + arrived_ref[
                parts + part, :own
            ].astype(f32) * share
            return small.astype(bf16), large.astype(bf16)

        acc[...] = residual_ref[...].astype(f32) * residual_scale
        for ref, (_, shift, other) in zip(mixer_refs, mixers):
            y = lax.rem(place_ref[0] + shift + turns, turns)
            core = place_ref[1] if other == 0 else 1 - place_ref[1]
            both = rows_of(y * cores + core)
            acc[...] += jnp.dot(jnp.concatenate(both, axis=1), ref[...], preferred_element_type=f32)
        values = acc[...]
        center = jnp.mean(values, axis=-1, keepdims=True)
        values = values - center
        spread = jnp.mean(jnp.square(values), axis=-1, keepdims=True)
        out_ref[...] = (values * lax.rsqrt(spread + epsilon) * gain_ref[...]).astype(bf16)

    vm = pl.BlockSpec(memory_space=pltpu.VMEM)
    return pl.pallas_call(
        body,
        in_specs=[pl.BlockSpec(memory_space=pltpu.SMEM)] + [vm] * (len(mixers) + 3),
        out_specs=vm,
        scratch_shapes=[pltpu.VMEM((own, wide), f32)],
        out_shape=jax.ShapeDtypeStruct((own, wide), bf16),
        compiler_params=pltpu.CompilerParams(vmem_limit_bytes=24 * 2**20),
        cost_estimate=cost_of(5.0),
    )(place, arrived, *[m[0] for m in mixers], residual, gain.reshape(1, wide))


BLOCK = 768
LEAD = 16


def pack_weights(value_weight, gate_weight, down_weight):
    width, rows = value_weight.shape

    def body(v, g, d, ups_out, down_out):
        for out, k, part in ((ups_out, 0, v), (ups_out, 1, g), (down_out, 0, d)):
            out[:, k * BLOCK : k * BLOCK + width] = part[...].T
            out[:, k * BLOCK + width : (k + 1) * BLOCK] = jnp.zeros((rows, BLOCK - width), bf16)

    vm = pl.BlockSpec(memory_space=pltpu.VMEM)
    return pl.pallas_call(
        body,
        in_specs=[vm] * 3,
        out_specs=[vm, vm],
        out_shape=[jax.ShapeDtypeStruct((rows, k * BLOCK), bf16) for k in (2, 1)],
        cost_estimate=cost_of(1.5),
    )(value_weight, gate_weight, down_weight)


def window(array, k):
    return pl.BlockSpec((array.shape[0], BLOCK), lambda i: (0, k))


def whole(array):
    return pl.BlockSpec(array.shape, lambda i: (0,) * array.ndim)


def ups(chunks, weights, width, cost, earlier=(), place=None, spots=(), turns=0, cores=0):
    rows = sum(c.shape[0] for c in chunks)
    own = chunks[0].shape[0] * len(chunks) // 2 if earlier else 0
    flat = [a for pair in earlier for a in pair]

    def body(*refs):
        place_ref, chunk_refs = refs[0], refs[1 : 1 + len(chunks)]
        value_ref, gate_ref = refs[1 + len(chunks) : 3 + len(chunks)]
        done = refs[3 + len(chunks) : 3 + len(chunks) + len(flat)]
        outs = refs[3 + len(chunks) + len(flat) :]
        x = jnp.concatenate([r[...] for r in chunk_refs], axis=0)
        for ref, out in ((value_ref, outs[0]), (gate_ref, outs[1])):
            out[...] = jnp.dot(x, ref[:, :width], preferred_element_type=f32).astype(bf16)
        if not earlier:
            return
        tails, leaving = outs[2:4], outs[4]
        pieces = (*done, *outs[:2])
        spot = 0
        for k in range(0, len(pieces), 2):
            for i in range(pieces[k].shape[0] // own):
                shift, other = spots[spot]
                spot += 1
                y = lax.rem(place_ref[0] + shift + turns, turns)
                core = place_ref[1] if other == 0 else 1 - place_ref[1]
                for side in range(2):
                    tails[side][y * cores + core] = pieces[k + side][(i + 1) * own - LEAD : (i + 1) * own]
        for side in range(2):
            leaving[side * LEAD : (side + 1) * LEAD] = tails[side][turns * cores - 1]

    shapes = [jax.ShapeDtypeStruct((rows, width), bf16)] * 2
    if earlier:
        shapes += [jax.ShapeDtypeStruct((turns * cores, LEAD, width), bf16)] * 2
        shapes.append(jax.ShapeDtypeStruct((2 * LEAD, width), bf16))
    return pl.pallas_call(
        body,
        grid=(1,),
        in_specs=[pl.BlockSpec(memory_space=pltpu.SMEM)]
        + [whole(c) for c in chunks]
        + [window(weights, 0), window(weights, 1)]
        + [whole(a) for a in flat],
        out_specs=[whole(x) for x in shapes],
        out_shape=shapes,
        compiler_params=pltpu.CompilerParams(vmem_limit_bytes=24 * 2**20),
        cost_estimate=cost_of(cost),
    )(place, *chunks, weights, weights, *flat)


def downs(place, pieces, groups, tails, halo, value_taps, gate_taps, weights, own, turns, cores, cost):
    width = pieces[0][0].shape[1]
    wide = weights.shape[0]
    count = len(groups)

    def body(place_ref, *refs):
        vt_ref, gt_ref, down_ref, halo_ref = refs[:4]
        tail_refs = refs[4:6]
        up_refs = refs[6 : 6 + 2 * len(pieces)]
        theirs, mine, hidden, terms = refs[6 + 2 * len(pieces) :]

        def filtered(ref, taps, tail, side, at, part):
            halo_rows = halo_ref[side * LEAD : (side + 1) * LEAD].astype(f32)
            before = tail[jnp.maximum(part - 1, 0)].astype(f32)
            before = jnp.where(part == 0, halo_rows, before)
            here = ref[pl.ds(pl.multiple_of(at * own, LEAD), own)].astype(f32)
            rows = jnp.concatenate([before, here], axis=0)
            two = pltpu.roll(rows, 2, 0)[LEAD:]
            one = pltpu.roll(rows, 1, 0)[LEAD:]
            return taps[0:1] * two + taps[1:2] * one + taps[2:3] * rows[LEAD:]

        @pl.loop(0, 2)
        def _(turn):
            core = jnp.where(turn == 0, 1 - place_ref[1], place_ref[1])
            for i, (piece, at_own, at_other, shift) in enumerate(groups):
                at = jnp.where(turn == 0, at_other, at_own)
                part = lax.rem(place_ref[0] + shift + turns, turns) * cores + core
                value = filtered(up_refs[2 * piece], vt_ref, tail_refs[0], 0, at, part)
                gate = filtered(up_refs[2 * piece + 1], gt_ref, tail_refs[1], 1, at, part)
                hidden[i * own : (i + 1) * own] = (gate / (1.0 + jnp.exp(-gate)) * value).astype(bf16)
            terms[...] = lax.dot_general(
                hidden[...],
                down_ref[:, :width],
                (((1,), (1,)), ((), ())),
                preferred_element_type=f32,
            )
            for own_turn, out in enumerate((theirs, mine)):

                @pl.when(turn == own_turn)
                def _():
                    @pl.loop(0, count)
                    def _(i):
                        out[i] = terms[pl.ds(pl.multiple_of(i * own, LEAD), own)].astype(out.dtype)

    shapes = [jax.ShapeDtypeStruct((count, own, wide), t) for t in (bf16, f32)]
    flat = [a for pair in pieces for a in pair]
    return pl.pallas_call(
        body,
        grid=(1,),
        in_specs=[pl.BlockSpec(memory_space=pltpu.SMEM), whole(value_taps), whole(gate_taps)]
        + [whole(weights), whole(halo), whole(tails[0]), whole(tails[1])]
        + [whole(a) for a in flat],
        out_specs=[whole(x) for x in shapes],
        out_shape=shapes,
        scratch_shapes=[
            pltpu.VMEM((count * own, width), bf16),
            pltpu.VMEM((count * own, wide), f32),
        ],
        compiler_params=pltpu.CompilerParams(vmem_limit_bytes=24 * 2**20),
        cost_estimate=cost_of(cost),
    )(place, value_taps, gate_taps, weights, halo, *tails, *flat)


def paired(mine, theirs, kinds):
    count, own, wide = mine.shape

    def body(mine_ref, their_ref, *outs):
        for i, out in enumerate(outs):
            out[...] = (mine_ref[i] + their_ref[i].astype(f32)).astype(out.dtype)

    vm = pl.BlockSpec(memory_space=pltpu.VMEM)
    return pl.pallas_call(
        body,
        in_specs=[vm] * 2,
        out_specs=[vm] * count,
        out_shape=[jax.ShapeDtypeStruct((own, wide), kind) for kind in kinds],
        cost_estimate=cost_of(0.7 * count),
    )(mine, theirs)


def finish(mixed, own, shares, gain):
    rows, wide = mixed.shape

    def body(*refs):
        mixed_ref, own_ref = refs[:2]
        gain_ref, out_ref = refs[-2:]
        total = own_ref[...]
        for r in refs[2:-2]:
            total = total + r[...].astype(f32)
        values = residual_scale * mixed_ref[...].astype(f32) + total
        center = jnp.mean(values, axis=-1, keepdims=True)
        values = values - center
        spread = jnp.mean(jnp.square(values), axis=-1, keepdims=True)
        out_ref[...] = (values * lax.rsqrt(spread + epsilon) * gain_ref[...]).astype(bf16)

    vm = pl.BlockSpec(memory_space=pltpu.VMEM)
    return pl.pallas_call(
        body,
        in_specs=[vm] * (3 + len(shares)),
        out_specs=vm,
        out_shape=jax.ShapeDtypeStruct((rows, wide), bf16),
        cost_estimate=cost_of(2.0),
    )(mixed, own, *shares, gain.reshape(1, wide))


def per_device(
    query_small,
    key_small,
    value_small,
    gates_small,
    query_large,
    key_large,
    value_large,
    gates_large,
    residual,
    mixer_small,
    mixer_large,
    mix_gain,
    value_weight,
    gate_weight,
    value_taps,
    gate_taps,
    down_weight,
    final_gain,
):
    slot = lax.axis_index("sp_z").astype(jnp.int32)
    column = lax.axis_index("sp_x").astype(jnp.int32)
    depth, turns = lax.axis_size("sp_z"), lax.axis_size("sp_x")
    packed, *asked = pack(
        slot.reshape(1),
        key_small,
        value_small,
        key_large,
        value_large,
        query_small,
        query_large,
        gates_small.T,
        gates_large.T,
    )
    packed, value_turned, gate_turned, down_turned = lax.optimization_barrier(
        (packed, value_weight.T, gate_weight.T, down_weight)
    )
    pairs = lax.all_to_all(packed, "sp_z", split_axis=0, concat_axis=0, tiled=True)
    shards = pack_weights(value_turned, gate_turned, down_turned)
    pairs, shards, asked = lax.optimization_barrier((pairs, shards, asked))
    weights = lax.all_gather(shards[0], SP, axis=0, tiled=True)
    before = shifted(pairs, "sp_x", 1)
    after = shifted(pairs, "sp_x", -1)
    queries = [asked[0]] + [shifted(asked[k], "sp_z", k) for k in range(1, depth)]
    mixer = jnp.concatenate([mixer_small, mixer_large], axis=0)
    mixers = [mixer] + [shifted(mixer, "tp_y", k) for k in (1, -1, 2)]
    calls = ((0,), (-1, 1), (2,))
    tables = work_tables(calls, depth, turns)
    place_here = jnp.stack([slot, column])
    call = lambda k, chunks, state: attend(
        place_here,
        jnp.asarray(tables[k]),
        queries,
        chunks,
        state,
        k + 1 == len(calls),
        lax.axis_size(TP),
        0 in calls[k],
        12.0 * len(calls[k]),
    )
    state = call(0, [pairs], None)
    pairs, before, after, state, down_shard = lax.optimization_barrier(
        (pairs, before, after, state, shards[1])
    )
    down_weights = lax.all_gather(down_shard, SP, axis=0, tiled=True)
    far = shifted(pairs, "sp_x", 2)
    state = call(1, [before, after], state)
    far, state, mixers = lax.optimization_barrier((far, state, mixers))
    shifts = (0, -1, 1, 2)
    mixers = [(a, shift, 0) for a, shift in zip(mixers, shifts)] + [
        (shifted(a, "tp_c", 1), shift, 1) for a, shift in zip(mixers, shifts)
    ]
    state = call(2, [far], state)
    arrived = lax.all_to_all(state, ("sp_z",) + TP, split_axis=0, concat_axis=0, tiled=True)
    place = jnp.stack([lax.axis_index("tp_y"), lax.axis_index("tp_c")]).astype(jnp.int32)
    mixed = mix_rows(place, arrived, mixers, residual, mix_gain)
    turns_y, cores = lax.axis_size("tp_y"), lax.axis_size("tp_c")
    own_rows = mixed.shape[0]
    half = own_rows // 2
    width = value_weight.shape[1]
    spots = [(0, 0), (0, 1), (-1, 0), (1, 0), (-1, 1), (1, 1), (2, 0), (2, 1)]
    last_one, next_one = shifted(mixed, "tp_y", 1), shifted(mixed, "tp_y", -1)
    near = [mixed, shifted(mixed, "tp_c", 1)]
    opposite = [shifted(last_one[:half], "tp_y", 1), shifted(next_one[half:], "tp_y", -1)]
    beside = [last_one, next_one] + [shifted(a, "tp_c", 1) for a in (last_one, next_one)]
    first_six = ups(near + beside, weights, width, 5.0, place=place)
    first_six, opposite = lax.optimization_barrier((first_six, opposite))
    opposite += [shifted(a, "tp_c", 1) for a in opposite]
    up_value, up_gate, *tails, leaving = ups(
        opposite, weights, width, 3.0, (first_six,), place, spots, turns_y, cores
    )
    opposite = [up_value, up_gate]
    halo = passed_along(leaving, SP, 1)
    down = lambda chosen, groups, cost: downs(
        place,
        chosen,
        groups,
        tails,
        halo,
        value_taps,
        gate_taps,
        down_weights,
        own_rows,
        turns_y,
        cores,
        cost,
    )
    theirs, mine = down([opposite], [(0, 0, 1, 2)], 4.0)
    (distant,) = paired(mine, shifted(theirs, "tp_c", 1), [bf16])
    first_six, distant = lax.optimization_barrier((first_six, distant))
    shares = [shifted(distant, "tp_y", 2)]
    theirs, mine = down([first_six], [(0, 0, 1, 0), (0, 2, 4, -1), (0, 3, 5, 1)], 8.0)
    own, before, after = paired(mine, shifted(theirs, "tp_c", 1), [f32, bf16, bf16])
    shares += [shifted(before, "tp_y", -1), shifted(after, "tp_y", 1)]
    return finish(mixed, own, shares, final_gain)


def solution(mesh):
    split = Mesh(mesh.devices.reshape(4, 4, 4, 2), ALL)
    placed = (P(SP, TP),) * 8 + (
        P(ALL, None),
        P(TP, None),
        P(TP, None),
        P(),
        P(SP, TP),
        P(SP, TP),
        P(None, TP),
        P(None, TP),
        P(TP, SP),
        P(),
    )

    return jax.shard_map(per_device, mesh=split, in_specs=placed, out_specs=P(ALL, None), check_vma=False)
```

```python
import math

import jax
import jax.numpy as jnp
import numpy as np
from jax import lax
from jax.experimental import pallas as pl
from jax.experimental.pallas import tpu as pltpu
from jax.sharding import Mesh
from jax.sharding import PartitionSpec as P


SP = ("sp_z", "sp_x")
TP = ("tp_y", "tp_c")
ALL = SP + TP
bf16 = jnp.bfloat16
f32 = jnp.float32
residual_scale = 2.0**0.5
epsilon = 1e-05


def shifted(value, axis, steps):
    count = lax.axis_size(axis)
    return lax.ppermute(value, axis, [(i, (i + steps) % count) for i in range(count)])


def passed_along(value, axis, steps):
    count = lax.axis_size(axis)
    first, last = (max(0, -steps), min(count, count - steps))
    return lax.ppermute(value, axis, [(source, source + steps) for source in range(first, last)])


LOW = -1e30
CHUNK = 256
EXTRA = 32
STAT_ROWS = 16
RATE = 250e6


def in_pieces(value):
    high = value.astype(bf16).astype(f32)
    middle = (value - high).astype(bf16).astype(f32)
    return high, middle, value - high - middle


def cost_of(us):
    return pl.CostEstimate(flops=int(us * RATE), transcendentals=0, bytes_accessed=0)


def pack(slot, key_small, value_small, key_large, value_large, query_small, query_large, gates_small, gates_large):
    rows, width = key_small.shape
    half = rows // 2
    low = width // 2
    tiles = rows // width

    def body(slot_ref, ks, vs, kl, vl, qs, ql, gs, gl, kv, *q):
        lane = lax.broadcasted_iota(jnp.int32, (rows, width), 1)
        turn = lambda ref: pltpu.roll(ref[...].astype(f32), low, 1)
        for slot in range(2):
            part = slice(slot * half, (slot + 1) * half)
            kv[slot, :half] = kl[part]
            kv[slot, half:rows] = vl[part]
        kv[2, :rows] = jnp.where(lane < low, ks[...].astype(f32), turn(vs)).astype(bf16)
        kv[3, :rows] = jnp.where(lane < low, turn(ks), vs[...].astype(f32)).astype(bf16)
        for shift in range(4):
            target = lax.rem(slot_ref[0] + shift, 4)

            @pl.when(target < 2)
            def _():
                q[shift][...] = ql[...]

            @pl.when(target == 2)
            def _():
                q[shift][...] = qs[...]

            @pl.when(target == 3)
            def _():
                q[shift][...] = turn(qs).astype(bf16)

        for slot, gate in ((0, gl[0:1]), (1, gl[0:1]), (2, gs[0:1]), (3, gs[1:2])):
            blocks = []
            for piece in in_pieces(gate):
                blocks += [piece[:, i * width : (i + 1) * width] for i in range(tiles)]
                blocks.append(jnp.zeros((8 - tiles, width), f32))
            blocks.append(jnp.zeros((EXTRA - 24, width), f32))
            kv[slot, rows:] = jnp.concatenate(blocks, axis=0).astype(bf16)

    vm = pl.BlockSpec(memory_space=pltpu.VMEM)
    return pl.pallas_call(
        body,
        in_specs=[pl.BlockSpec(memory_space=pltpu.SMEM)] + [vm] * 8,
        out_specs=[vm] * 5,
        out_shape=[jax.ShapeDtypeStruct((4, rows + EXTRA, width), bf16)]
        + [jax.ShapeDtypeStruct((rows, width), bf16)] * 4,
        cost_estimate=cost_of(2.5),
    )(slot, key_small, value_small, key_large, value_large, query_small, query_large, gates_small, gates_large)


def work_tables(calls, depth, turns):
    tables = []
    for here in range(turns):
        row = []
        for shifts in calls:
            steps = []
            for z in range(depth):
                for n, shift in enumerate(shifts):
                    there = (here + shift) % turns
                    for w in range(depth):
                        key, query = w * turns + there, z * turns + here
                        if key < query:
                            steps.append((z, n * depth + w, 0))
                for n, shift in enumerate(shifts):
                    if shift == 0:
                        steps.append((z, n * depth + z, 1))
            row.append(steps)
        tables.append(row)
    longest = [max(len(tables[h][k]) for h in range(turns)) + 1 for k in range(len(calls))]
    out = []
    for k in range(len(calls)):
        table = np.zeros((turns, longest[k] * 3 + 1), np.int32)
        for h in range(turns):
            flat = np.array(tables[h][k] + [(0, 0, 0)] * (longest[k] - len(tables[h][k])), np.int32)
            table[h, :-1] = flat.reshape(-1)
            table[h, -1] = len(tables[h][k])
        out.append(table)
    return out


def attend(where, table, queries, chunks, state, final, tensor_parts, has_diagonal, cost):
    depth = len(queries)
    rows, width = queries[0].shape
    half = rows // 2
    low = width // 2
    tiles = rows // width
    blocks = sum(c.shape[0] for c in chunks)
    columns = rows // CHUNK
    tall = width + 16
    last = table.shape[1] - 1
    own = rows // tensor_parts
    fresh = state is None

    def body(*refs):
        where_ref, table_ref = refs[:2]
        q_refs = refs[2 : 2 + depth]
        chunk_refs = refs[2 + depth : 2 + depth + len(chunks)]
        at = 2 + depth + len(chunks) + (0 if fresh else 2)
        state_in = () if fresh else refs[at - 2 : at]
        if final:
            out_ref = refs[at]
            acc, peak = refs[at + 1 : at + 3]
            scratch = refs[at + 3 :]
        else:
            acc, peak = refs[at : at + 2]
            scratch = refs[at + 2 :]
        qa, ka_small, va_small, ka_large, va_large, first = scratch
        slot = where_ref[0]
        column = where_ref[1]
        count = table_ref[column, last]

        @pl.loop(0, depth)
        def _(z):
            if fresh:
                acc[z] = jnp.zeros(acc.shape[1:], f32)
                peak[z] = jnp.full(peak.shape[1:], LOW, f32)
            else:
                acc[z] = state_in[0][z]
                peak[z] = state_in[1][z]

        def attention(small):
            d = low if small else width
            ext = d + 16
            span = rows if small else half
            tile = CHUNK if small else half
            parts = span // tile
            root = d**0.5
            rate = math.log2(math.e) / root
            ka, va = (ka_small, va_small) if small else (ka_large, va_large)
            deep = width if small else 2 * width
            lane = lax.broadcasted_iota(jnp.int32, (rows, width), 1)

            for shift, q_ref in enumerate(q_refs):
                z = lax.rem(slot + depth - shift, depth)
                q = q_ref[...]
                if small:
                    one = ((lane >= d) & (lane < d + 3)).astype(f32)
                    qa[z, :, :width] = jnp.where(lane < d, q.astype(f32), one).astype(bf16)
                else:
                    qa[z, :, :width] = q
                    qa[z, :, width:] = (lane < 3).astype(f32).astype(bf16)

            def prepare(ref, n, block):
                pieces = ref[n, rows : rows + 24].astype(f32)
                gate = pieces[0:8] + pieces[8:16] + pieces[16:24]
                bias = jnp.concatenate([gate[i : i + 1] for i in range(tiles)], axis=1) * -root
                bias = jnp.broadcast_to(bias, (8, rows))
                if not small:
                    bias = jnp.where(slot == 0, bias[:, :half], bias[:, half:])
                high, middle, rest = in_pieces(bias)
                row = lax.broadcasted_iota(jnp.int32, (8, span), 0)
                zero = jnp.zeros((8, span), f32)
                picked = jnp.where(row == 0, high, jnp.where(row == 1, middle, jnp.where(row == 2, rest, zero)))
                before = d if small else 0
                stack = [picked, jnp.zeros((width - before - 8, span), f32)]
                if before:
                    stack = [jnp.zeros((before, span), f32)] + stack
                gate_columns = jnp.concatenate(stack, axis=0).astype(bf16).T
                if small:
                    kv = ref[n, :rows]
                    ka[block] = jnp.where(lane < d, kv, gate_columns)
                    va[block, :d] = kv.T[d:]
                else:
                    ka[block, :, :width] = ref[n, :half]
                    ka[block, :, width:] = gate_columns
                    va[block, :d] = ref[n, half:rows].T
                va[block, d:] = jnp.ones((16, span), bf16)

            offset = 0
            for ref in chunk_refs:
                base = offset

                @pl.loop(0, ref.shape[0])
                def _(n):
                    prepare(ref, n, base + n)

                offset += ref.shape[0]

            def scores(z, block, c, t):
                return lax.dot_general(
                    ka[block, t * tile : (t + 1) * tile],
                    qa[z, c * CHUNK : (c + 1) * CHUNK, :deep],
                    (((1,), (1,)), ((), ())),
                    preferred_element_type=f32,
                )

            def masked(s, c, t, flag):
                if small and t < c:
                    return s
                key = lax.broadcasted_iota(jnp.int32, (tile, CHUNK), 0) + t * tile
                if not small:
                    key = key + slot * half
                    key = jnp.where(flag == 0, 0, key)
                query = lax.broadcasted_iota(jnp.int32, (tile, CHUNK), 1) + c * CHUNK
                return jnp.where(key <= query, s, LOW)

            def step(n, diagonal):
                z, block = table_ref[column, 3 * n], table_ref[column, 3 * n + 1]
                next_z, next_block = table_ref[column, 3 * n + 3], table_ref[column, 3 * n + 4]
                held_count = lambda c: c + 1 if diagonal and small else parts
                held = [first[t * tile : (t + 1) * tile] for t in range(held_count(0))]
                for c in range(columns):
                    cols = slice(c * CHUNK, (c + 1) * CHUNK)
                    if diagonal:
                        held = [masked(s, c, t, table_ref[column, 3 * n + 2]) for t, s in enumerate(held)]
                    top = held[0]
                    for s in held[1:]:
                        top = jnp.maximum(top, s)
                    old = peak[z, 0:1, cols]
                    new = jnp.maximum(old, jnp.max(top, axis=0, keepdims=True))
                    scaled = new * rate
                    factor = jnp.exp2(old * rate - scaled)
                    peak[z, 0:1, cols] = new
                    coming = []
                    added = None
                    following = c + 1 < columns
                    ahead = held_count(c + 1) if following else parts
                    for t in range(max(len(held), ahead)):
                        if t < ahead:
                            if following:
                                coming.append(scores(z, block, c + 1, t))
                            else:
                                first[t * tile : (t + 1) * tile] = scores(next_z, next_block, 0, t)
                        if t < len(held):
                            w = jnp.exp2(held[t] * rate - scaled).astype(bf16)
                            add = jnp.dot(
                                va[block, :, t * tile : (t + 1) * tile], w, preferred_element_type=f32
                            )
                            added = add if added is None else added + add
                    acc[z, :ext, cols] = acc[z, :ext, cols] * factor + added
                    held = coming

            for t in range(parts):
                first[t * tile : (t + 1) * tile] = scores(table_ref[column, 0], table_ref[column, 1], 0, t)

            @pl.loop(0, count)
            def _(n):
                if not has_diagonal or not small:
                    step(n, has_diagonal)
                    return
                diagonal = table_ref[column, 3 * n + 2]

                @pl.when(diagonal == 0)
                def _():
                    step(n, False)

                @pl.when(diagonal == 1)
                def _():
                    step(n, True)

            if final:

                @pl.loop(0, depth)
                def _(z):
                    total = acc[z, d : d + 1]
                    out = acc[z, :d] / total
                    if small:
                        out = jnp.concatenate([out, jnp.zeros((width - d, rows), f32)], axis=0)
                    out = out.T.astype(bf16)
                    level = peak[z, 0:1] * rate + jnp.log2(total)
                    stat = jnp.concatenate([*in_pieces(level), jnp.zeros((STAT_ROWS - 3, rows), f32)], axis=0)
                    for r in range(tensor_parts):
                        out_ref[z * tensor_parts + r, :own] = out[r * own : (r + 1) * own]
                        if not small:
                            mine = stat[:, r * own : (r + 1) * own]
                            mine = jnp.concatenate([mine, jnp.zeros((STAT_ROWS, width - own), f32)], axis=1)
                            out_ref[z * tensor_parts + r, own:] = mine.astype(bf16)
                        else:
                            out_ref[z * tensor_parts + r, own:] = jnp.zeros((STAT_ROWS, width), bf16)

        @pl.when(slot < 2)
        def _():
            attention(False)

        @pl.when(slot >= 2)
        def _():
            attention(True)

    vm = pl.BlockSpec(memory_space=pltpu.VMEM)
    sm = pl.BlockSpec(memory_space=pltpu.SMEM)
    state_shapes = [((depth, tall, rows), f32), ((depth, 8, rows), f32)]
    scratch = [pltpu.VMEM(s, t) for s, t in state_shapes] if final else []
    scratch += [
        pltpu.VMEM((depth, rows, 2 * width), bf16),
        pltpu.VMEM((blocks, rows, width), bf16),
        pltpu.VMEM((blocks, low + 16, rows), bf16),
        pltpu.VMEM((blocks, half, 2 * width), bf16),
        pltpu.VMEM((blocks, tall, half), bf16),
        pltpu.VMEM((rows, CHUNK), f32),
    ]
    if final:
        out_shape = jax.ShapeDtypeStruct((depth * tensor_parts, own + STAT_ROWS, width), bf16)
        out_specs = vm
    else:
        out_shape = [jax.ShapeDtypeStruct(s, t) for s, t in state_shapes]
        out_specs = [vm, vm]
    args = [where, table, *queries, *chunks] + ([] if fresh else list(state))
    return pl.pallas_call(
        body,
        in_specs=[sm, sm] + [vm] * (len(args) - 2),
        out_specs=out_specs,
        scratch_shapes=scratch,
        out_shape=out_shape,
        compiler_params=pltpu.CompilerParams(vmem_limit_bytes=30 * 2**20),
        cost_estimate=cost_of(cost),
    )(*args)


def mix_rows(place, arrived, mixers, residual, gain):
    own, wide = residual.shape
    width = arrived.shape[2]
    cores = 2
    turns = arrived.shape[0] // 4 // cores
    parts = turns * cores

    def body(place_ref, arrived_ref, *refs):
        mixer_refs = refs[: len(mixers)]
        residual_ref, gain_ref, out_ref, acc = refs[len(mixers) :]
        lane = lax.broadcasted_iota(jnp.int32, (own, width), 1)

        def level(index):
            pieces = arrived_ref[index, own:].astype(f32)
            line = pieces[0:1] + pieces[1:2] + pieces[2:3]
            return jnp.broadcast_to(line, (8, width)).T[:own, 0:1]

        def rows_of(part):
            second = pltpu.roll(arrived_ref[3 * parts + part, :own].astype(f32), width // 2, 1)
            small = jnp.where(lane < width // 2, arrived_ref[2 * parts + part, :own].astype(f32), second)
            share = 1.0 / (1.0 + jnp.exp2(level(part) - level(parts + part)))
            large = arrived_ref[part, :own].astype(f32) * (1.0 - share) + arrived_ref[
                parts + part, :own
            ].astype(f32) * share
            return small.astype(bf16), large.astype(bf16)

        acc[...] = residual_ref[...].astype(f32) * residual_scale
        for ref, (_, shift, other) in zip(mixer_refs, mixers):
            y = lax.rem(place_ref[0] + shift + turns, turns)
            core = place_ref[1] if other == 0 else 1 - place_ref[1]
            both = rows_of(y * cores + core)
            acc[...] += jnp.dot(jnp.concatenate(both, axis=1), ref[...], preferred_element_type=f32)
        values = acc[...]
        center = jnp.mean(values, axis=-1, keepdims=True)
        values = values - center
        spread = jnp.mean(jnp.square(values), axis=-1, keepdims=True)
        out_ref[...] = (values * lax.rsqrt(spread + epsilon) * gain_ref[...]).astype(bf16)

    vm = pl.BlockSpec(memory_space=pltpu.VMEM)
    return pl.pallas_call(
        body,
        in_specs=[pl.BlockSpec(memory_space=pltpu.SMEM)] + [vm] * (len(mixers) + 3),
        out_specs=vm,
        scratch_shapes=[pltpu.VMEM((own, wide), f32)],
        out_shape=jax.ShapeDtypeStruct((own, wide), bf16),
        compiler_params=pltpu.CompilerParams(vmem_limit_bytes=24 * 2**20),
        cost_estimate=cost_of(5.0),
    )(place, arrived, *[m[0] for m in mixers], residual, gain.reshape(1, wide))


BLOCK = 768
LEAD = 16


def pack_weights(value_weight, gate_weight, down_weight):
    width, rows = value_weight.shape

    def body(v, g, d, ups_out, down_out):
        for out, k, part in ((ups_out, 0, v), (ups_out, 1, g), (down_out, 0, d)):
            out[:, k * BLOCK : k * BLOCK + width] = part[...].T
            out[:, k * BLOCK + width : (k + 1) * BLOCK] = jnp.zeros((rows, BLOCK - width), bf16)

    vm = pl.BlockSpec(memory_space=pltpu.VMEM)
    return pl.pallas_call(
        body,
        in_specs=[vm] * 3,
        out_specs=[vm, vm],
        out_shape=[jax.ShapeDtypeStruct((rows, k * BLOCK), bf16) for k in (2, 1)],
        cost_estimate=cost_of(1.5),
    )(value_weight, gate_weight, down_weight)


def window(array, k):
    return pl.BlockSpec((array.shape[0], BLOCK), lambda i: (0, k))


def whole(array):
    return pl.BlockSpec(array.shape, lambda i: (0,) * array.ndim)


def ups(chunks, weights, width, cost, earlier=(), place=None, spots=(), turns=0, cores=0):
    rows = sum(c.shape[0] for c in chunks)
    own = chunks[0].shape[0] * len(chunks) // 2 if earlier else 0
    flat = [a for pair in earlier for a in pair]

    def body(*refs):
        place_ref, chunk_refs = refs[0], refs[1 : 1 + len(chunks)]
        value_ref, gate_ref = refs[1 + len(chunks) : 3 + len(chunks)]
        done = refs[3 + len(chunks) : 3 + len(chunks) + len(flat)]
        outs = refs[3 + len(chunks) + len(flat) :]
        x = jnp.concatenate([r[...] for r in chunk_refs], axis=0)
        for ref, out in ((value_ref, outs[0]), (gate_ref, outs[1])):
            out[...] = jnp.dot(x, ref[:, :width], preferred_element_type=f32).astype(bf16)
        if not earlier:
            return
        tails, leaving = outs[2:4], outs[4]
        pieces = (*done, *outs[:2])
        spot = 0
        for k in range(0, len(pieces), 2):
            for i in range(pieces[k].shape[0] // own):
                shift, other = spots[spot]
                spot += 1
                y = lax.rem(place_ref[0] + shift + turns, turns)
                core = place_ref[1] if other == 0 else 1 - place_ref[1]
                for side in range(2):
                    tails[side][y * cores + core] = pieces[k + side][(i + 1) * own - LEAD : (i + 1) * own]
        for side in range(2):
            leaving[side * LEAD : (side + 1) * LEAD] = tails[side][turns * cores - 1]

    shapes = [jax.ShapeDtypeStruct((rows, width), bf16)] * 2
    if earlier:
        shapes += [jax.ShapeDtypeStruct((turns * cores, LEAD, width), bf16)] * 2
        shapes.append(jax.ShapeDtypeStruct((2 * LEAD, width), bf16))
    return pl.pallas_call(
        body,
        grid=(1,),
        in_specs=[pl.BlockSpec(memory_space=pltpu.SMEM)]
        + [whole(c) for c in chunks]
        + [window(weights, 0), window(weights, 1)]
        + [whole(a) for a in flat],
        out_specs=[whole(x) for x in shapes],
        out_shape=shapes,
        compiler_params=pltpu.CompilerParams(vmem_limit_bytes=24 * 2**20),
        cost_estimate=cost_of(cost),
    )(place, *chunks, weights, weights, *flat)


def downs(place, pieces, groups, tails, halo, value_taps, gate_taps, weights, own, turns, cores, cost):
    width = pieces[0][0].shape[1]
    wide = weights.shape[0]
    count = len(groups)

    def body(place_ref, *refs):
        vt_ref, gt_ref, down_ref, halo_ref = refs[:4]
        tail_refs = refs[4:6]
        up_refs = refs[6 : 6 + 2 * len(pieces)]
        theirs, mine, hidden, terms = refs[6 + 2 * len(pieces) :]

        def filtered(ref, taps, tail, side, at, part):
            halo_rows = halo_ref[side * LEAD : (side + 1) * LEAD].astype(f32)
            before = tail[jnp.maximum(part - 1, 0)].astype(f32)
            before = jnp.where(part == 0, halo_rows, before)
            here = ref[pl.ds(pl.multiple_of(at * own, LEAD), own)].astype(f32)
            rows = jnp.concatenate([before, here], axis=0)
            two = pltpu.roll(rows, 2, 0)[LEAD:]
            one = pltpu.roll(rows, 1, 0)[LEAD:]
            return taps[0:1] * two + taps[1:2] * one + taps[2:3] * rows[LEAD:]

        @pl.loop(0, 2)
        def _(turn):
            core = jnp.where(turn == 0, 1 - place_ref[1], place_ref[1])
            for i, (piece, at_own, at_other, shift) in enumerate(groups):
                at = jnp.where(turn == 0, at_other, at_own)
                part = lax.rem(place_ref[0] + shift + turns, turns) * cores + core
                value = filtered(up_refs[2 * piece], vt_ref, tail_refs[0], 0, at, part)
                gate = filtered(up_refs[2 * piece + 1], gt_ref, tail_refs[1], 1, at, part)
                hidden[i * own : (i + 1) * own] = (gate / (1.0 + jnp.exp(-gate)) * value).astype(bf16)
            terms[...] = lax.dot_general(
                hidden[...],
                down_ref[:, :width],
                (((1,), (1,)), ((), ())),
                preferred_element_type=f32,
            )
            for own_turn, out in enumerate((theirs, mine)):

                @pl.when(turn == own_turn)
                def _():
                    @pl.loop(0, count)
                    def _(i):
                        out[i] = terms[pl.ds(pl.multiple_of(i * own, LEAD), own)].astype(out.dtype)

    shapes = [jax.ShapeDtypeStruct((count, own, wide), t) for t in (bf16, f32)]
    flat = [a for pair in pieces for a in pair]
    return pl.pallas_call(
        body,
        grid=(1,),
        in_specs=[pl.BlockSpec(memory_space=pltpu.SMEM), whole(value_taps), whole(gate_taps)]
        + [whole(weights), whole(halo), whole(tails[0]), whole(tails[1])]
        + [whole(a) for a in flat],
        out_specs=[whole(x) for x in shapes],
        out_shape=shapes,
        scratch_shapes=[
            pltpu.VMEM((count * own, width), bf16),
            pltpu.VMEM((count * own, wide), f32),
        ],
        compiler_params=pltpu.CompilerParams(vmem_limit_bytes=24 * 2**20),
        cost_estimate=cost_of(cost),
    )(place, value_taps, gate_taps, weights, halo, *tails, *flat)


def paired(mine, theirs, kinds):
    count, own, wide = mine.shape

    def body(mine_ref, their_ref, *outs):
        for i, out in enumerate(outs):
            out[...] = (mine_ref[i] + their_ref[i].astype(f32)).astype(out.dtype)

    vm = pl.BlockSpec(memory_space=pltpu.VMEM)
    return pl.pallas_call(
        body,
        in_specs=[vm] * 2,
        out_specs=[vm] * count,
        out_shape=[jax.ShapeDtypeStruct((own, wide), kind) for kind in kinds],
        cost_estimate=cost_of(0.7 * count),
    )(mine, theirs)


def finish(mixed, own, shares, gain):
    rows, wide = mixed.shape

    def body(*refs):
        mixed_ref, own_ref = refs[:2]
        gain_ref, out_ref = refs[-2:]
        total = own_ref[...]
        for r in refs[2:-2]:
            total = total + r[...].astype(f32)
        values = residual_scale * mixed_ref[...].astype(f32) + total
        center = jnp.mean(values, axis=-1, keepdims=True)
        values = values - center
        spread = jnp.mean(jnp.square(values), axis=-1, keepdims=True)
        out_ref[...] = (values * lax.rsqrt(spread + epsilon) * gain_ref[...]).astype(bf16)

    vm = pl.BlockSpec(memory_space=pltpu.VMEM)
    return pl.pallas_call(
        body,
        in_specs=[vm] * (3 + len(shares)),
        out_specs=vm,
        out_shape=jax.ShapeDtypeStruct((rows, wide), bf16),
        cost_estimate=cost_of(2.0),
    )(mixed, own, *shares, gain.reshape(1, wide))


def per_device(
    query_small,
    key_small,
    value_small,
    gates_small,
    query_large,
    key_large,
    value_large,
    gates_large,
    residual,
    mixer_small,
    mixer_large,
    mix_gain,
    value_weight,
    gate_weight,
    value_taps,
    gate_taps,
    down_weight,
    final_gain,
):
    slot = lax.axis_index("sp_z").astype(jnp.int32)
    column = lax.axis_index("sp_x").astype(jnp.int32)
    depth, turns = lax.axis_size("sp_z"), lax.axis_size("sp_x")
    packed, *asked = pack(
        slot.reshape(1),
        key_small,
        value_small,
        key_large,
        value_large,
        query_small,
        query_large,
        gates_small.T,
        gates_large.T,
    )
    packed, value_turned, gate_turned, down_turned = lax.optimization_barrier(
        (packed, value_weight.T, gate_weight.T, down_weight)
    )
    pairs = lax.all_to_all(packed, "sp_z", split_axis=0, concat_axis=0, tiled=True)
    shards = pack_weights(value_turned, gate_turned, down_turned)
    pairs, shards, asked = lax.optimization_barrier((pairs, shards, asked))
    weights = lax.all_gather(shards[0], SP, axis=0, tiled=True)
    before = shifted(pairs, "sp_x", 1)
    after = shifted(pairs, "sp_x", -1)
    queries = [asked[0]] + [shifted(asked[k], "sp_z", k) for k in range(1, depth)]
    mixer = jnp.concatenate([mixer_small, mixer_large], axis=0)
    mixer, down_shard = lax.optimization_barrier((mixer, shards[1]))
    down_weights = lax.all_gather(down_shard, SP, axis=0, tiled=True)
    mixers = [mixer]
    for k in (1, -1, 2):
        mixers.append(shifted(mixer, "tp_y", k))
    calls = ((0,), (-1, 1), (2,))
    tables = work_tables(calls, depth, turns)
    place_here = jnp.stack([slot, column])
    call = lambda k, chunks, state: attend(
        place_here,
        jnp.asarray(tables[k]),
        queries,
        chunks,
        state,
        k + 1 == len(calls),
        lax.axis_size(TP),
        0 in calls[k],
        12.0 * len(calls[k]),
    )
    state = call(0, [pairs], None)
    pairs, before, after, state = lax.optimization_barrier((pairs, before, after, state))
    far = shifted(pairs, "sp_x", 2)
    state = call(1, [before, after], state)
    far, state, mixers = lax.optimization_barrier((far, state, mixers))
    shifts = (0, -1, 1, 2)
    mixers = [(a, shift, 0) for a, shift in zip(mixers, shifts)] + [
        (shifted(a, "tp_c", 1), shift, 1) for a, shift in zip(mixers, shifts)
    ]
    state = call(2, [far], state)
    arrived = lax.all_to_all(state, ("sp_z",) + TP, split_axis=0, concat_axis=0, tiled=True)
    place = jnp.stack([lax.axis_index("tp_y"), lax.axis_index("tp_c")]).astype(jnp.int32)
    mixed = mix_rows(place, arrived, mixers, residual, mix_gain)
    turns_y, cores = lax.axis_size("tp_y"), lax.axis_size("tp_c")
    own_rows = mixed.shape[0]
    half = own_rows // 2
    width = value_weight.shape[1]
    spots = [(0, 0), (0, 1), (-1, 0), (1, 0), (-1, 1), (1, 1), (2, 0), (2, 1)]
    last_one, next_one = shifted(mixed, "tp_y", 1), shifted(mixed, "tp_y", -1)
    near = [mixed, shifted(mixed, "tp_c", 1)]
    opposite = [shifted(last_one[:half], "tp_y", 1), shifted(next_one[half:], "tp_y", -1)]
    beside = [last_one, next_one] + [shifted(a, "tp_c", 1) for a in (last_one, next_one)]
    first_six = ups(near + beside, weights, width, 5.0, place=place)
    first_six, opposite = lax.optimization_barrier((first_six, opposite))
    opposite += [shifted(a, "tp_c", 1) for a in opposite]
    up_value, up_gate, *tails, leaving = ups(
        opposite, weights, width, 3.0, (first_six,), place, spots, turns_y, cores
    )
    opposite = [up_value, up_gate]
    halo = passed_along(leaving, SP, 1)
    down = lambda chosen, groups, cost: downs(
        place,
        chosen,
        groups,
        tails,
        halo,
        value_taps,
        gate_taps,
        down_weights,
        own_rows,
        turns_y,
        cores,
        cost,
    )
    theirs, mine = down([opposite], [(0, 0, 1, 2)], 4.0)
    (distant,) = paired(mine, shifted(theirs, "tp_c", 1), [bf16])
    first_six, distant = lax.optimization_barrier((first_six, distant))
    shares = [shifted(distant, "tp_y", 2)]
    theirs, mine = down([first_six], [(0, 0, 1, 0), (0, 2, 4, -1), (0, 3, 5, 1)], 8.0)
    own, before, after = paired(mine, shifted(theirs, "tp_c", 1), [f32, bf16, bf16])
    shares += [shifted(before, "tp_y", -1), shifted(after, "tp_y", 1)]
    return finish(mixed, own, shares, final_gain)


def solution(mesh):
    split = Mesh(mesh.devices.reshape(4, 4, 4, 2), ALL)
    placed = (P(SP, TP),) * 8 + (
        P(ALL, None),
        P(TP, None),
        P(TP, None),
        P(),
        P(SP, TP),
        P(SP, TP),
        P(None, TP),
        P(None, TP),
        P(TP, SP),
        P(),
    )

    return jax.shard_map(per_device, mesh=split, in_specs=placed, out_specs=P(ALL, None), check_vma=False)
```

```python
import math

import jax
import jax.numpy as jnp
import numpy as np
from jax import lax
from jax.experimental import pallas as pl
from jax.experimental.pallas import tpu as pltpu
from jax.sharding import Mesh
from jax.sharding import PartitionSpec as P


SP = ("sp_z", "sp_x")
TP = ("tp_y", "tp_c")
ALL = SP + TP
bf16 = jnp.bfloat16
f32 = jnp.float32
residual_scale = 2.0**0.5
epsilon = 1e-05


def shifted(value, axis, steps):
    count = lax.axis_size(axis)
    return lax.ppermute(value, axis, [(i, (i + steps) % count) for i in range(count)])


def passed_along(value, axis, steps):
    count = lax.axis_size(axis)
    first, last = (max(0, -steps), min(count, count - steps))
    return lax.ppermute(value, axis, [(source, source + steps) for source in range(first, last)])


LOW = -1e30
CHUNK = 256
EXTRA = 32
STAT_ROWS = 16
RATE = 250e6


def in_pieces(value):
    high = value.astype(bf16).astype(f32)
    middle = (value - high).astype(bf16).astype(f32)
    return high, middle, value - high - middle


def cost_of(us):
    return pl.CostEstimate(flops=int(us * RATE), transcendentals=0, bytes_accessed=0)


def pack(slot, key_small, value_small, key_large, value_large, query_small, query_large, gates_small, gates_large):
    rows, width = key_small.shape
    half = rows // 2
    low = width // 2
    tiles = rows // width

    def body(slot_ref, ks, vs, kl, vl, qs, ql, gs, gl, kv, *q):
        lane = lax.broadcasted_iota(jnp.int32, (rows, width), 1)
        turn = lambda ref: pltpu.roll(ref[...].astype(f32), low, 1)
        for slot in range(2):
            part = slice(slot * half, (slot + 1) * half)
            kv[slot, :half] = kl[part]
            kv[slot, half:rows] = vl[part]
        kv[2, :rows] = jnp.where(lane < low, ks[...].astype(f32), turn(vs)).astype(bf16)
        kv[3, :rows] = jnp.where(lane < low, turn(ks), vs[...].astype(f32)).astype(bf16)
        for shift in range(4):
            target = lax.rem(slot_ref[0] + shift, 4)

            @pl.when(target < 2)
            def _():
                q[shift][...] = ql[...]

            @pl.when(target == 2)
            def _():
                q[shift][...] = qs[...]

            @pl.when(target == 3)
            def _():
                q[shift][...] = turn(qs).astype(bf16)

        for slot, gate in ((0, gl[0:1]), (1, gl[0:1]), (2, gs[0:1]), (3, gs[1:2])):
            blocks = []
            for piece in in_pieces(gate):
                blocks += [piece[:, i * width : (i + 1) * width] for i in range(tiles)]
                blocks.append(jnp.zeros((8 - tiles, width), f32))
            blocks.append(jnp.zeros((EXTRA - 24, width), f32))
            kv[slot, rows:] = jnp.concatenate(blocks, axis=0).astype(bf16)

    vm = pl.BlockSpec(memory_space=pltpu.VMEM)
    return pl.pallas_call(
        body,
        in_specs=[pl.BlockSpec(memory_space=pltpu.SMEM)] + [vm] * 8,
        out_specs=[vm] * 5,
        out_shape=[jax.ShapeDtypeStruct((4, rows + EXTRA, width), bf16)]
        + [jax.ShapeDtypeStruct((rows, width), bf16)] * 4,
        cost_estimate=cost_of(2.5),
    )(slot, key_small, value_small, key_large, value_large, query_small, query_large, gates_small, gates_large)


def work_tables(calls, depth, turns):
    tables = []
    for here in range(turns):
        row = []
        for shifts in calls:
            steps = []
            for z in range(depth):
                for n, shift in enumerate(shifts):
                    there = (here + shift) % turns
                    for w in range(depth):
                        key, query = w * turns + there, z * turns + here
                        if key < query:
                            steps.append((z, n * depth + w, 0))
                for n, shift in enumerate(shifts):
                    if shift == 0:
                        steps.append((z, n * depth + z, 1))
            row.append(steps)
        tables.append(row)
    longest = [max(len(tables[h][k]) for h in range(turns)) + 1 for k in range(len(calls))]
    out = []
    for k in range(len(calls)):
        table = np.zeros((turns, longest[k] * 3 + 1), np.int32)
        for h in range(turns):
            flat = np.array(tables[h][k] + [(0, 0, 0)] * (longest[k] - len(tables[h][k])), np.int32)
            table[h, :-1] = flat.reshape(-1)
            table[h, -1] = len(tables[h][k])
        out.append(table)
    return out


def attend(where, table, queries, chunks, state, final, tensor_parts, has_diagonal, cost):
    depth = len(queries)
    rows, width = queries[0].shape
    half = rows // 2
    low = width // 2
    tiles = rows // width
    blocks = sum(c.shape[0] for c in chunks)
    columns = rows // CHUNK
    tall = width + 16
    last = table.shape[1] - 1
    own = rows // tensor_parts
    fresh = state is None

    def body(*refs):
        where_ref, table_ref = refs[:2]
        q_refs = refs[2 : 2 + depth]
        chunk_refs = refs[2 + depth : 2 + depth + len(chunks)]
        at = 2 + depth + len(chunks) + (0 if fresh else 2)
        state_in = () if fresh else refs[at - 2 : at]
        if final:
            out_ref = refs[at]
            acc, peak = refs[at + 1 : at + 3]
            scratch = refs[at + 3 :]
        else:
            acc, peak = refs[at : at + 2]
            scratch = refs[at + 2 :]
        qa, ka_small, va_small, ka_large, va_large, first = scratch
        slot = where_ref[0]
        column = where_ref[1]
        count = table_ref[column, last]

        @pl.loop(0, depth)
        def _(z):
            if fresh:
                acc[z] = jnp.zeros(acc.shape[1:], f32)
                peak[z] = jnp.full(peak.shape[1:], LOW, f32)
            else:
                acc[z] = state_in[0][z]
                peak[z] = state_in[1][z]

        def attention(small):
            d = low if small else width
            ext = d + 16
            span = rows if small else half
            tile = CHUNK if small else half
            parts = span // tile
            root = d**0.5
            rate = math.log2(math.e) / root
            ka, va = (ka_small, va_small) if small else (ka_large, va_large)
            deep = width if small else 2 * width
            lane = lax.broadcasted_iota(jnp.int32, (rows, width), 1)

            for shift, q_ref in enumerate(q_refs):
                z = lax.rem(slot + depth - shift, depth)
                q = q_ref[...]
                if small:
                    one = ((lane >= d) & (lane < d + 3)).astype(f32)
                    qa[z, :, :width] = jnp.where(lane < d, q.astype(f32), one).astype(bf16)
                else:
                    qa[z, :, :width] = q
                    qa[z, :, width:] = (lane < 3).astype(f32).astype(bf16)

            def prepare(ref, n, block):
                pieces = ref[n, rows : rows + 24].astype(f32)
                gate = pieces[0:8] + pieces[8:16] + pieces[16:24]
                bias = jnp.concatenate([gate[i : i + 1] for i in range(tiles)], axis=1) * -root
                bias = jnp.broadcast_to(bias, (8, rows))
                if not small:
                    bias = jnp.where(slot == 0, bias[:, :half], bias[:, half:])
                high, middle, rest = in_pieces(bias)
                row = lax.broadcasted_iota(jnp.int32, (8, span), 0)
                zero = jnp.zeros((8, span), f32)
                picked = jnp.where(row == 0, high, jnp.where(row == 1, middle, jnp.where(row == 2, rest, zero)))
                before = d if small else 0
                stack = [picked, jnp.zeros((width - before - 8, span), f32)]
                if before:
                    stack = [jnp.zeros((before, span), f32)] + stack
                gate_columns = jnp.concatenate(stack, axis=0).astype(bf16).T
                if small:
                    kv = ref[n, :rows]
                    ka[block] = jnp.where(lane < d, kv, gate_columns)
                    va[block, :d] = kv.T[d:]
                else:
                    ka[block, :, :width] = ref[n, :half]
                    ka[block, :, width:] = gate_columns
                    va[block, :d] = ref[n, half:rows].T
                va[block, d:] = jnp.ones((16, span), bf16)

            offset = 0
            for ref in chunk_refs:
                base = offset

                @pl.loop(0, ref.shape[0])
                def _(n):
                    prepare(ref, n, base + n)

                offset += ref.shape[0]

            def scores(z, block, c, t):
                return lax.dot_general(
                    ka[block, t * tile : (t + 1) * tile],
                    qa[z, c * CHUNK : (c + 1) * CHUNK, :deep],
                    (((1,), (1,)), ((), ())),
                    preferred_element_type=f32,
                )

            def masked(s, c, t, flag):
                if small and t < c:
                    return s
                key = lax.broadcasted_iota(jnp.int32, (tile, CHUNK), 0) + t * tile
                if not small:
                    key = key + slot * half
                    key = jnp.where(flag == 0, 0, key)
                query = lax.broadcasted_iota(jnp.int32, (tile, CHUNK), 1) + c * CHUNK
                return jnp.where(key <= query, s, LOW)

            def step(n, diagonal):
                z, block = table_ref[column, 3 * n], table_ref[column, 3 * n + 1]
                next_z, next_block = table_ref[column, 3 * n + 3], table_ref[column, 3 * n + 4]
                held_count = lambda c: c + 1 if diagonal and small else parts
                held = [first[t * tile : (t + 1) * tile] for t in range(held_count(0))]
                for c in range(columns):
                    cols = slice(c * CHUNK, (c + 1) * CHUNK)
                    if diagonal:
                        held = [masked(s, c, t, table_ref[column, 3 * n + 2]) for t, s in enumerate(held)]
                    top = held[0]
                    for s in held[1:]:
                        top = jnp.maximum(top, s)
                    old = peak[z, 0:1, cols]
                    new = jnp.maximum(old, jnp.max(top, axis=0, keepdims=True))
                    scaled = new * rate
                    factor = jnp.exp2(old * rate - scaled)
                    peak[z, 0:1, cols] = new
                    coming = []
                    added = None
                    following = c + 1 < columns
                    ahead = held_count(c + 1) if following else parts
                    for t in range(max(len(held), ahead)):
                        if t < ahead:
                            if following:
                                coming.append(scores(z, block, c + 1, t))
                            else:
                                first[t * tile : (t + 1) * tile] = scores(next_z, next_block, 0, t)
                        if t < len(held):
                            w = jnp.exp2(held[t] * rate - scaled).astype(bf16)
                            add = jnp.dot(
                                va[block, :, t * tile : (t + 1) * tile], w, preferred_element_type=f32
                            )
                            added = add if added is None else added + add
                    acc[z, :ext, cols] = acc[z, :ext, cols] * factor + added
                    held = coming

            for t in range(parts):
                first[t * tile : (t + 1) * tile] = scores(table_ref[column, 0], table_ref[column, 1], 0, t)

            @pl.loop(0, count)
            def _(n):
                if not has_diagonal or not small:
                    step(n, has_diagonal)
                    return
                diagonal = table_ref[column, 3 * n + 2]

                @pl.when(diagonal == 0)
                def _():
                    step(n, False)

                @pl.when(diagonal == 1)
                def _():
                    step(n, True)

            if final:

                @pl.loop(0, depth)
                def _(z):
                    total = acc[z, d : d + 1]
                    out = acc[z, :d] / total
                    if small:
                        out = jnp.concatenate([out, jnp.zeros((width - d, rows), f32)], axis=0)
                    out = out.T.astype(bf16)
                    level = peak[z, 0:1] * rate + jnp.log2(total)
                    stat = jnp.concatenate([*in_pieces(level), jnp.zeros((STAT_ROWS - 3, rows), f32)], axis=0)
                    for r in range(tensor_parts):
                        out_ref[z * tensor_parts + r, :own] = out[r * own : (r + 1) * own]
                        if not small:
                            mine = stat[:, r * own : (r + 1) * own]
                            mine = jnp.concatenate([mine, jnp.zeros((STAT_ROWS, width - own), f32)], axis=1)
                            out_ref[z * tensor_parts + r, own:] = mine.astype(bf16)
                        else:
                            out_ref[z * tensor_parts + r, own:] = jnp.zeros((STAT_ROWS, width), bf16)

        @pl.when(slot < 2)
        def _():
            attention(False)

        @pl.when(slot >= 2)
        def _():
            attention(True)

    vm = pl.BlockSpec(memory_space=pltpu.VMEM)
    sm = pl.BlockSpec(memory_space=pltpu.SMEM)
    state_shapes = [((depth, tall, rows), f32), ((depth, 8, rows), f32)]
    scratch = [pltpu.VMEM(s, t) for s, t in state_shapes] if final else []
    scratch += [
        pltpu.VMEM((depth, rows, 2 * width), bf16),
        pltpu.VMEM((blocks, rows, width), bf16),
        pltpu.VMEM((blocks, low + 16, rows), bf16),
        pltpu.VMEM((blocks, half, 2 * width), bf16),
        pltpu.VMEM((blocks, tall, half), bf16),
        pltpu.VMEM((rows, CHUNK), f32),
    ]
    if final:
        out_shape = jax.ShapeDtypeStruct((depth * tensor_parts, own + STAT_ROWS, width), bf16)
        out_specs = vm
    else:
        out_shape = [jax.ShapeDtypeStruct(s, t) for s, t in state_shapes]
        out_specs = [vm, vm]
    args = [where, table, *queries, *chunks] + ([] if fresh else list(state))
    return pl.pallas_call(
        body,
        in_specs=[sm, sm] + [vm] * (len(args) - 2),
        out_specs=out_specs,
        scratch_shapes=scratch,
        out_shape=out_shape,
        compiler_params=pltpu.CompilerParams(vmem_limit_bytes=30 * 2**20),
        cost_estimate=cost_of(cost),
    )(*args)


def mix_rows(place, arrived, mixers, residual, gain):
    own, wide = residual.shape
    width = arrived.shape[2]
    cores = 2
    turns = arrived.shape[0] // 4 // cores
    parts = turns * cores

    def body(place_ref, arrived_ref, *refs):
        mixer_refs = refs[: len(mixers)]
        residual_ref, gain_ref, out_ref, acc = refs[len(mixers) :]
        lane = lax.broadcasted_iota(jnp.int32, (own, width), 1)

        def level(index):
            pieces = arrived_ref[index, own:].astype(f32)
            line = pieces[0:1] + pieces[1:2] + pieces[2:3]
            return jnp.broadcast_to(line, (8, width)).T[:own, 0:1]

        def rows_of(part):
            second = pltpu.roll(arrived_ref[3 * parts + part, :own].astype(f32), width // 2, 1)
            small = jnp.where(lane < width // 2, arrived_ref[2 * parts + part, :own].astype(f32), second)
            share = 1.0 / (1.0 + jnp.exp2(level(part) - level(parts + part)))
            large = arrived_ref[part, :own].astype(f32) * (1.0 - share) + arrived_ref[
                parts + part, :own
            ].astype(f32) * share
            return small.astype(bf16), large.astype(bf16)

        acc[...] = residual_ref[...].astype(f32) * residual_scale
        for ref, (_, shift, other) in zip(mixer_refs, mixers):
            y = lax.rem(place_ref[0] + shift + turns, turns)
            core = place_ref[1] if other == 0 else 1 - place_ref[1]
            both = rows_of(y * cores + core)
            acc[...] += jnp.dot(jnp.concatenate(both, axis=1), ref[...], preferred_element_type=f32)
        values = acc[...]
        center = jnp.mean(values, axis=-1, keepdims=True)
        values = values - center
        spread = jnp.mean(jnp.square(values), axis=-1, keepdims=True)
        out_ref[...] = (values * lax.rsqrt(spread + epsilon) * gain_ref[...]).astype(bf16)

    vm = pl.BlockSpec(memory_space=pltpu.VMEM)
    return pl.pallas_call(
        body,
        in_specs=[pl.BlockSpec(memory_space=pltpu.SMEM)] + [vm] * (len(mixers) + 3),
        out_specs=vm,
        scratch_shapes=[pltpu.VMEM((own, wide), f32)],
        out_shape=jax.ShapeDtypeStruct((own, wide), bf16),
        compiler_params=pltpu.CompilerParams(vmem_limit_bytes=24 * 2**20),
        cost_estimate=cost_of(5.0),
    )(place, arrived, *[m[0] for m in mixers], residual, gain.reshape(1, wide))


BLOCK = 768
LEAD = 16


def pack_weights(value_weight, gate_weight, down_weight):
    width, rows = value_weight.shape

    def body(v, g, d, out):
        for k, part in enumerate((v, g, d)):
            out[:, k * BLOCK : k * BLOCK + width] = part[...].T
            out[:, k * BLOCK + width : (k + 1) * BLOCK] = jnp.zeros((rows, BLOCK - width), bf16)

    vm = pl.BlockSpec(memory_space=pltpu.VMEM)
    return pl.pallas_call(
        body,
        in_specs=[vm] * 3,
        out_specs=vm,
        out_shape=jax.ShapeDtypeStruct((rows, 3 * BLOCK), bf16),
        cost_estimate=cost_of(1.5),
    )(value_weight, gate_weight, down_weight)


def window(array, k):
    return pl.BlockSpec((array.shape[0], BLOCK), lambda i: (0, k))


def whole(array):
    return pl.BlockSpec(array.shape, lambda i: (0,) * array.ndim)


def ups(chunks, weights, width, cost, earlier=(), place=None, spots=(), turns=0, cores=0):
    rows = sum(c.shape[0] for c in chunks)
    own = chunks[0].shape[0] * len(chunks) // 2 if earlier else 0
    flat = [a for pair in earlier for a in pair]

    def body(*refs):
        place_ref, chunk_refs = refs[0], refs[1 : 1 + len(chunks)]
        value_ref, gate_ref = refs[1 + len(chunks) : 3 + len(chunks)]
        done = refs[3 + len(chunks) : 3 + len(chunks) + len(flat)]
        outs = refs[3 + len(chunks) + len(flat) :]
        x = jnp.concatenate([r[...] for r in chunk_refs], axis=0)
        for ref, out in ((value_ref, outs[0]), (gate_ref, outs[1])):
            out[...] = jnp.dot(x, ref[:, :width], preferred_element_type=f32).astype(bf16)
        if not earlier:
            return
        tails, leaving = outs[2:4], outs[4]
        pieces = (*done, *outs[:2])
        spot = 0
        for k in range(0, len(pieces), 2):
            for i in range(pieces[k].shape[0] // own):
                shift, other = spots[spot]
                spot += 1
                y = lax.rem(place_ref[0] + shift + turns, turns)
                core = place_ref[1] if other == 0 else 1 - place_ref[1]
                for side in range(2):
                    tails[side][y * cores + core] = pieces[k + side][(i + 1) * own - LEAD : (i + 1) * own]
        for side in range(2):
            leaving[side * LEAD : (side + 1) * LEAD] = tails[side][turns * cores - 1]

    shapes = [jax.ShapeDtypeStruct((rows, width), bf16)] * 2
    if earlier:
        shapes += [jax.ShapeDtypeStruct((turns * cores, LEAD, width), bf16)] * 2
        shapes.append(jax.ShapeDtypeStruct((2 * LEAD, width), bf16))
    return pl.pallas_call(
        body,
        grid=(1,),
        in_specs=[pl.BlockSpec(memory_space=pltpu.SMEM)]
        + [whole(c) for c in chunks]
        + [window(weights, 0), window(weights, 1)]
        + [whole(a) for a in flat],
        out_specs=[whole(x) for x in shapes],
        out_shape=shapes,
        compiler_params=pltpu.CompilerParams(vmem_limit_bytes=24 * 2**20),
        cost_estimate=cost_of(cost),
    )(place, *chunks, weights, weights, *flat)


def downs(place, pieces, groups, tails, halo, value_taps, gate_taps, weights, own, turns, cores, cost):
    width = pieces[0][0].shape[1]
    wide = weights.shape[0]
    count = len(groups)

    def body(place_ref, *refs):
        vt_ref, gt_ref, down_ref, halo_ref = refs[:4]
        tail_refs = refs[4:6]
        up_refs = refs[6 : 6 + 2 * len(pieces)]
        theirs, mine, hidden, terms = refs[6 + 2 * len(pieces) :]

        def filtered(ref, taps, tail, side, at, part):
            halo_rows = halo_ref[side * LEAD : (side + 1) * LEAD].astype(f32)
            before = tail[jnp.maximum(part - 1, 0)].astype(f32)
            before = jnp.where(part == 0, halo_rows, before)
            here = ref[pl.ds(pl.multiple_of(at * own, LEAD), own)].astype(f32)
            rows = jnp.concatenate([before, here], axis=0)
            two = pltpu.roll(rows, 2, 0)[LEAD:]
            one = pltpu.roll(rows, 1, 0)[LEAD:]
            return taps[0:1] * two + taps[1:2] * one + taps[2:3] * rows[LEAD:]

        @pl.loop(0, 2)
        def _(turn):
            core = jnp.where(turn == 0, 1 - place_ref[1], place_ref[1])
            for i, (piece, at_own, at_other, shift) in enumerate(groups):
                at = jnp.where(turn == 0, at_other, at_own)
                part = lax.rem(place_ref[0] + shift + turns, turns) * cores + core
                value = filtered(up_refs[2 * piece], vt_ref, tail_refs[0], 0, at, part)
                gate = filtered(up_refs[2 * piece + 1], gt_ref, tail_refs[1], 1, at, part)
                hidden[i * own : (i + 1) * own] = (gate / (1.0 + jnp.exp(-gate)) * value).astype(bf16)
            terms[...] = lax.dot_general(
                hidden[...],
                down_ref[:, :width],
                (((1,), (1,)), ((), ())),
                preferred_element_type=f32,
            )
            for own_turn, out in enumerate((theirs, mine)):

                @pl.when(turn == own_turn)
                def _():
                    @pl.loop(0, count)
                    def _(i):
                        out[i] = terms[pl.ds(pl.multiple_of(i * own, LEAD), own)].astype(out.dtype)

    shapes = [jax.ShapeDtypeStruct((count, own, wide), t) for t in (bf16, f32)]
    flat = [a for pair in pieces for a in pair]
    return pl.pallas_call(
        body,
        grid=(1,),
        in_specs=[pl.BlockSpec(memory_space=pltpu.SMEM), whole(value_taps), whole(gate_taps)]
        + [window(weights, 2), whole(halo), whole(tails[0]), whole(tails[1])]
        + [whole(a) for a in flat],
        out_specs=[whole(x) for x in shapes],
        out_shape=shapes,
        scratch_shapes=[
            pltpu.VMEM((count * own, width), bf16),
            pltpu.VMEM((count * own, wide), f32),
        ],
        compiler_params=pltpu.CompilerParams(vmem_limit_bytes=24 * 2**20),
        cost_estimate=cost_of(cost),
    )(place, value_taps, gate_taps, weights, halo, *tails, *flat)


def paired(mine, theirs, kinds):
    count, own, wide = mine.shape

    def body(mine_ref, their_ref, *outs):
        for i, out in enumerate(outs):
            out[...] = (mine_ref[i] + their_ref[i].astype(f32)).astype(out.dtype)

    vm = pl.BlockSpec(memory_space=pltpu.VMEM)
    return pl.pallas_call(
        body,
        in_specs=[vm] * 2,
        out_specs=[vm] * count,
        out_shape=[jax.ShapeDtypeStruct((own, wide), kind) for kind in kinds],
        cost_estimate=cost_of(0.7 * count),
    )(mine, theirs)


def finish(mixed, own, shares, gain):
    rows, wide = mixed.shape

    def body(*refs):
        mixed_ref, own_ref = refs[:2]
        gain_ref, out_ref = refs[-2:]
        total = own_ref[...]
        for r in refs[2:-2]:
            total = total + r[...].astype(f32)
        values = residual_scale * mixed_ref[...].astype(f32) + total
        center = jnp.mean(values, axis=-1, keepdims=True)
        values = values - center
        spread = jnp.mean(jnp.square(values), axis=-1, keepdims=True)
        out_ref[...] = (values * lax.rsqrt(spread + epsilon) * gain_ref[...]).astype(bf16)

    vm = pl.BlockSpec(memory_space=pltpu.VMEM)
    return pl.pallas_call(
        body,
        in_specs=[vm] * (3 + len(shares)),
        out_specs=vm,
        out_shape=jax.ShapeDtypeStruct((rows, wide), bf16),
        cost_estimate=cost_of(2.0),
    )(mixed, own, *shares, gain.reshape(1, wide))


def per_device(
    query_small,
    key_small,
    value_small,
    gates_small,
    query_large,
    key_large,
    value_large,
    gates_large,
    residual,
    mixer_small,
    mixer_large,
    mix_gain,
    value_weight,
    gate_weight,
    value_taps,
    gate_taps,
    down_weight,
    final_gain,
):
    slot = lax.axis_index("sp_z").astype(jnp.int32)
    column = lax.axis_index("sp_x").astype(jnp.int32)
    depth, turns = lax.axis_size("sp_z"), lax.axis_size("sp_x")
    packed, *asked = pack(
        slot.reshape(1),
        key_small,
        value_small,
        key_large,
        value_large,
        query_small,
        query_large,
        gates_small.T,
        gates_large.T,
    )
    packed, value_turned, gate_turned, down_turned = lax.optimization_barrier(
        (packed, value_weight.T, gate_weight.T, down_weight)
    )
    pairs = lax.all_to_all(packed, "sp_z", split_axis=0, concat_axis=0, tiled=True)
    shards = pack_weights(value_turned, gate_turned, down_turned)
    pairs, shards, asked = lax.optimization_barrier((pairs, shards, asked))
    weights = lax.all_gather(shards, SP, axis=0, tiled=True)
    before = shifted(pairs, "sp_x", 1)
    after = shifted(pairs, "sp_x", -1)
    queries = [asked[0]] + [shifted(asked[k], "sp_z", k) for k in range(1, depth)]
    mixer = jnp.concatenate([mixer_small, mixer_large], axis=0)
    mixers = [mixer]
    for k in (1, -1, 2):
        mixers.append(shifted(mixer, "tp_y", k))
    calls = ((0,), (-1, 1), (2,))
    tables = work_tables(calls, depth, turns)
    place_here = jnp.stack([slot, column])
    call = lambda k, chunks, state: attend(
        place_here,
        jnp.asarray(tables[k]),
        queries,
        chunks,
        state,
        k + 1 == len(calls),
        lax.axis_size(TP),
        0 in calls[k],
        12.0 * len(calls[k]),
    )
    state = call(0, [pairs], None)
    pairs, before, after, state = lax.optimization_barrier((pairs, before, after, state))
    far = shifted(pairs, "sp_x", 2)
    state = call(1, [before, after], state)
    far_mixer = mixers.pop()
    far, state, mixers = lax.optimization_barrier((far, state, mixers))
    crossed = [shifted(a, "tp_c", 1) for a in mixers]
    state = call(2, [far], state)
    arrived = lax.all_to_all(state, ("sp_z",) + TP, split_axis=0, concat_axis=0, tiled=True)
    crossed.append(shifted(far_mixer, "tp_c", 1))
    shifts = (0, -1, 1, 2)
    mixers = [(a, k, 0) for a, k in zip(mixers + [far_mixer], shifts)]
    mixers += [(a, k, 1) for a, k in zip(crossed, shifts)]
    place = jnp.stack([lax.axis_index("tp_y"), lax.axis_index("tp_c")]).astype(jnp.int32)
    mixed = mix_rows(place, arrived, mixers, residual, mix_gain)
    turns_y, cores = lax.axis_size("tp_y"), lax.axis_size("tp_c")
    own_rows = mixed.shape[0]
    half = own_rows // 2
    width = value_weight.shape[1]
    spots = [(0, 0), (0, 1), (-1, 0), (1, 0), (-1, 1), (1, 1), (2, 0), (2, 1)]
    last_one, next_one = shifted(mixed, "tp_y", 1), shifted(mixed, "tp_y", -1)
    near = ups([mixed, shifted(mixed, "tp_c", 1)], weights, width, 3.0, place=place)
    opposite = [shifted(last_one[:half], "tp_y", 1), shifted(next_one[half:], "tp_y", -1)]
    beside = [last_one, next_one] + [shifted(a, "tp_c", 1) for a in (last_one, next_one)]
    beside = ups(beside, weights, width, 4.0, place=place)
    beside, opposite = lax.optimization_barrier((beside, opposite))
    opposite += [shifted(a, "tp_c", 1) for a in opposite]
    up_value, up_gate, *tails, leaving = ups(
        opposite, weights, width, 3.0, (near, beside), place, spots, turns_y, cores
    )
    opposite = [up_value, up_gate]
    halo = passed_along(leaving, SP, 1)
    down = lambda chosen, groups, cost: downs(
        place,
        chosen,
        groups,
        tails,
        halo,
        value_taps,
        gate_taps,
        weights,
        own_rows,
        turns_y,
        cores,
        cost,
    )
    theirs, mine = down([opposite], [(0, 0, 1, 2)], 4.0)
    (distant,) = paired(mine, shifted(theirs, "tp_c", 1), [bf16])
    near, beside, distant = lax.optimization_barrier((near, beside, distant))
    shares = [shifted(distant, "tp_y", 2)]
    theirs, mine = down([near, beside], [(0, 0, 1, 0), (1, 0, 2, -1), (1, 1, 3, 1)], 8.0)
    own, before, after = paired(mine, shifted(theirs, "tp_c", 1), [f32, bf16, bf16])
    shares += [shifted(before, "tp_y", -1), shifted(after, "tp_y", 1)]
    return finish(mixed, own, shares, final_gain)


def solution(mesh):
    split = Mesh(mesh.devices.reshape(4, 4, 4, 2), ALL)
    placed = (P(SP, TP),) * 8 + (
        P(ALL, None),
        P(TP, None),
        P(TP, None),
        P(),
        P(SP, TP),
        P(SP, TP),
        P(None, TP),
        P(None, TP),
        P(TP, SP),
        P(),
    )

    return jax.shard_map(per_device, mesh=split, in_specs=placed, out_specs=P(ALL, None), check_vma=False)
```

```python
import math

import jax
import jax.numpy as jnp
import numpy as np
from jax import lax
from jax.experimental import pallas as pl
from jax.experimental.pallas import tpu as pltpu
from jax.sharding import Mesh
from jax.sharding import PartitionSpec as P


SP = ("sp_z", "sp_x")
TP = ("tp_y", "tp_c")
ALL = SP + TP
bf16 = jnp.bfloat16
f32 = jnp.float32
residual_scale = 2.0**0.5
epsilon = 1e-05


def shifted(value, axis, steps):
    count = lax.axis_size(axis)
    return lax.ppermute(value, axis, [(i, (i + steps) % count) for i in range(count)])


def passed_along(value, axis, steps):
    count = lax.axis_size(axis)
    first, last = (max(0, -steps), min(count, count - steps))
    return lax.ppermute(value, axis, [(source, source + steps) for source in range(first, last)])


LOW = -1e30
CHUNK = 256
EXTRA = 32
STAT_ROWS = 16
RATE = 250e6


def in_pieces(value):
    high = value.astype(bf16).astype(f32)
    middle = (value - high).astype(bf16).astype(f32)
    return high, middle, value - high - middle


def cost_of(us):
    return pl.CostEstimate(flops=int(us * RATE), transcendentals=0, bytes_accessed=0)


def pack(slot, key_small, value_small, key_large, value_large, query_small, query_large, gates_small, gates_large):
    rows, width = key_small.shape
    half = rows // 2
    low = width // 2
    tiles = rows // width

    def body(slot_ref, ks, vs, kl, vl, qs, ql, gs, gl, kv, *q):
        lane = lax.broadcasted_iota(jnp.int32, (rows, width), 1)
        turn = lambda ref: pltpu.roll(ref[...].astype(f32), low, 1)
        for slot in range(2):
            part = slice(slot * half, (slot + 1) * half)
            kv[slot, :half] = kl[part]
            kv[slot, half:rows] = vl[part]
        kv[2, :rows] = jnp.where(lane < low, ks[...].astype(f32), turn(vs)).astype(bf16)
        kv[3, :rows] = jnp.where(lane < low, turn(ks), vs[...].astype(f32)).astype(bf16)
        for shift in range(4):
            target = lax.rem(slot_ref[0] + shift, 4)

            @pl.when(target < 2)
            def _():
                q[shift][...] = ql[...]

            @pl.when(target == 2)
            def _():
                q[shift][...] = qs[...]

            @pl.when(target == 3)
            def _():
                q[shift][...] = turn(qs).astype(bf16)

        for slot, gate in ((0, gl[0:1]), (1, gl[0:1]), (2, gs[0:1]), (3, gs[1:2])):
            blocks = []
            for piece in in_pieces(gate):
                blocks += [piece[:, i * width : (i + 1) * width] for i in range(tiles)]
                blocks.append(jnp.zeros((8 - tiles, width), f32))
            blocks.append(jnp.zeros((EXTRA - 24, width), f32))
            kv[slot, rows:] = jnp.concatenate(blocks, axis=0).astype(bf16)

    vm = pl.BlockSpec(memory_space=pltpu.VMEM)
    return pl.pallas_call(
        body,
        in_specs=[pl.BlockSpec(memory_space=pltpu.SMEM)] + [vm] * 8,
        out_specs=[vm] * 5,
        out_shape=[jax.ShapeDtypeStruct((4, rows + EXTRA, width), bf16)]
        + [jax.ShapeDtypeStruct((rows, width), bf16)] * 4,
        cost_estimate=cost_of(2.5),
    )(slot, key_small, value_small, key_large, value_large, query_small, query_large, gates_small, gates_large)


def work_tables(calls, depth, turns):
    tables = []
    for here in range(turns):
        row = []
        for shifts in calls:
            steps = []
            for z in range(depth):
                for n, shift in enumerate(shifts):
                    there = (here + shift) % turns
                    for w in range(depth):
                        key, query = w * turns + there, z * turns + here
                        if key < query:
                            steps.append((z, n * depth + w, 0))
                for n, shift in enumerate(shifts):
                    if shift == 0:
                        steps.append((z, n * depth + z, 1))
            row.append(steps)
        tables.append(row)
    longest = [max(len(tables[h][k]) for h in range(turns)) + 1 for k in range(len(calls))]
    out = []
    for k in range(len(calls)):
        table = np.zeros((turns, longest[k] * 3 + 1), np.int32)
        for h in range(turns):
            flat = np.array(tables[h][k] + [(0, 0, 0)] * (longest[k] - len(tables[h][k])), np.int32)
            table[h, :-1] = flat.reshape(-1)
            table[h, -1] = len(tables[h][k])
        out.append(table)
    return out


def attend(where, table, queries, chunks, state, final, tensor_parts, has_diagonal, cost):
    depth = len(queries)
    rows, width = queries[0].shape
    half = rows // 2
    low = width // 2
    tiles = rows // width
    blocks = sum(c.shape[0] for c in chunks)
    columns = rows // CHUNK
    tall = width + 16
    last = table.shape[1] - 1
    own = rows // tensor_parts
    fresh = state is None

    def body(*refs):
        where_ref, table_ref = refs[:2]
        q_refs = refs[2 : 2 + depth]
        chunk_refs = refs[2 + depth : 2 + depth + len(chunks)]
        at = 2 + depth + len(chunks) + (0 if fresh else 2)
        state_in = () if fresh else refs[at - 2 : at]
        if final:
            out_ref = refs[at]
            acc, peak = refs[at + 1 : at + 3]
            scratch = refs[at + 3 :]
        else:
            acc, peak = refs[at : at + 2]
            scratch = refs[at + 2 :]
        qa, ka_small, va_small, ka_large, va_large, first = scratch
        slot = where_ref[0]
        column = where_ref[1]
        count = table_ref[column, last]

        @pl.loop(0, depth)
        def _(z):
            if fresh:
                acc[z] = jnp.zeros(acc.shape[1:], f32)
                peak[z] = jnp.full(peak.shape[1:], LOW, f32)
            else:
                acc[z] = state_in[0][z]
                peak[z] = state_in[1][z]

        def attention(small):
            d = low if small else width
            ext = d + 16
            span = rows if small else half
            tile = CHUNK if small else half
            parts = span // tile
            root = d**0.5
            rate = math.log2(math.e) / root
            ka, va = (ka_small, va_small) if small else (ka_large, va_large)
            deep = width if small else 2 * width
            lane = lax.broadcasted_iota(jnp.int32, (rows, width), 1)

            for shift, q_ref in enumerate(q_refs):
                z = lax.rem(slot + depth - shift, depth)
                q = q_ref[...]
                if small:
                    one = ((lane >= d) & (lane < d + 3)).astype(f32)
                    qa[z, :, :width] = jnp.where(lane < d, q.astype(f32), one).astype(bf16)
                else:
                    qa[z, :, :width] = q
                    qa[z, :, width:] = (lane < 3).astype(f32).astype(bf16)

            def prepare(ref, n, block):
                pieces = ref[n, rows : rows + 24].astype(f32)
                gate = pieces[0:8] + pieces[8:16] + pieces[16:24]
                bias = jnp.concatenate([gate[i : i + 1] for i in range(tiles)], axis=1) * -root
                bias = jnp.broadcast_to(bias, (8, rows))
                if not small:
                    bias = jnp.where(slot == 0, bias[:, :half], bias[:, half:])
                high, middle, rest = in_pieces(bias)
                row = lax.broadcasted_iota(jnp.int32, (8, span), 0)
                zero = jnp.zeros((8, span), f32)
                picked = jnp.where(row == 0, high, jnp.where(row == 1, middle, jnp.where(row == 2, rest, zero)))
                before = d if small else 0
                stack = [picked, jnp.zeros((width - before - 8, span), f32)]
                if before:
                    stack = [jnp.zeros((before, span), f32)] + stack
                gate_columns = jnp.concatenate(stack, axis=0).astype(bf16).T
                if small:
                    kv = ref[n, :rows]
                    ka[block] = jnp.where(lane < d, kv, gate_columns)
                    va[block, :d] = kv.T[d:]
                else:
                    ka[block, :, :width] = ref[n, :half]
                    ka[block, :, width:] = gate_columns
                    va[block, :d] = ref[n, half:rows].T
                va[block, d:] = jnp.ones((16, span), bf16)

            offset = 0
            for ref in chunk_refs:
                base = offset

                @pl.loop(0, ref.shape[0])
                def _(n):
                    prepare(ref, n, base + n)

                offset += ref.shape[0]

            def scores(z, block, c, t):
                return lax.dot_general(
                    ka[block, t * tile : (t + 1) * tile],
                    qa[z, c * CHUNK : (c + 1) * CHUNK, :deep],
                    (((1,), (1,)), ((), ())),
                    preferred_element_type=f32,
                )

            def masked(s, c, t, flag):
                if small and t < c:
                    return s
                key = lax.broadcasted_iota(jnp.int32, (tile, CHUNK), 0) + t * tile
                if not small:
                    key = key + slot * half
                    key = jnp.where(flag == 0, 0, key)
                query = lax.broadcasted_iota(jnp.int32, (tile, CHUNK), 1) + c * CHUNK
                return jnp.where(key <= query, s, LOW)

            def step(n, diagonal):
                z, block = table_ref[column, 3 * n], table_ref[column, 3 * n + 1]
                next_z, next_block = table_ref[column, 3 * n + 3], table_ref[column, 3 * n + 4]
                held_count = lambda c: c + 1 if diagonal and small else parts
                held = [first[t * tile : (t + 1) * tile] for t in range(held_count(0))]
                for c in range(columns):
                    cols = slice(c * CHUNK, (c + 1) * CHUNK)
                    if diagonal:
                        held = [masked(s, c, t, table_ref[column, 3 * n + 2]) for t, s in enumerate(held)]
                    top = held[0]
                    for s in held[1:]:
                        top = jnp.maximum(top, s)
                    old = peak[z, 0:1, cols]
                    new = jnp.maximum(old, jnp.max(top, axis=0, keepdims=True))
                    scaled = new * rate
                    factor = jnp.exp2(old * rate - scaled)
                    peak[z, 0:1, cols] = new
                    coming = []
                    added = None
                    following = c + 1 < columns
                    ahead = held_count(c + 1) if following else parts
                    for t in range(max(len(held), ahead)):
                        if t < ahead:
                            if following:
                                coming.append(scores(z, block, c + 1, t))
                            else:
                                first[t * tile : (t + 1) * tile] = scores(next_z, next_block, 0, t)
                        if t < len(held):
                            w = jnp.exp2(held[t] * rate - scaled).astype(bf16)
                            add = jnp.dot(
                                va[block, :, t * tile : (t + 1) * tile], w, preferred_element_type=f32
                            )
                            added = add if added is None else added + add
                    acc[z, :ext, cols] = acc[z, :ext, cols] * factor + added
                    held = coming

            for t in range(parts):
                first[t * tile : (t + 1) * tile] = scores(table_ref[column, 0], table_ref[column, 1], 0, t)

            @pl.loop(0, count)
            def _(n):
                if not has_diagonal or not small:
                    step(n, has_diagonal)
                    return
                diagonal = table_ref[column, 3 * n + 2]

                @pl.when(diagonal == 0)
                def _():
                    step(n, False)

                @pl.when(diagonal == 1)
                def _():
                    step(n, True)

            if final:

                @pl.loop(0, depth)
                def _(z):
                    total = acc[z, d : d + 1]
                    out = acc[z, :d] / total
                    if small:
                        out = jnp.concatenate([out, jnp.zeros((width - d, rows), f32)], axis=0)
                    out = out.T.astype(bf16)
                    level = peak[z, 0:1] * rate + jnp.log2(total)
                    stat = jnp.concatenate([*in_pieces(level), jnp.zeros((STAT_ROWS - 3, rows), f32)], axis=0)
                    for r in range(tensor_parts):
                        out_ref[z * tensor_parts + r, :own] = out[r * own : (r + 1) * own]
                        if not small:
                            mine = stat[:, r * own : (r + 1) * own]
                            mine = jnp.concatenate([mine, jnp.zeros((STAT_ROWS, width - own), f32)], axis=1)
                            out_ref[z * tensor_parts + r, own:] = mine.astype(bf16)
                        else:
                            out_ref[z * tensor_parts + r, own:] = jnp.zeros((STAT_ROWS, width), bf16)

        @pl.when(slot < 2)
        def _():
            attention(False)

        @pl.when(slot >= 2)
        def _():
            attention(True)

    vm = pl.BlockSpec(memory_space=pltpu.VMEM)
    sm = pl.BlockSpec(memory_space=pltpu.SMEM)
    state_shapes = [((depth, tall, rows), f32), ((depth, 8, rows), f32)]
    scratch = [pltpu.VMEM(s, t) for s, t in state_shapes] if final else []
    scratch += [
        pltpu.VMEM((depth, rows, 2 * width), bf16),
        pltpu.VMEM((blocks, rows, width), bf16),
        pltpu.VMEM((blocks, low + 16, rows), bf16),
        pltpu.VMEM((blocks, half, 2 * width), bf16),
        pltpu.VMEM((blocks, tall, half), bf16),
        pltpu.VMEM((rows, CHUNK), f32),
    ]
    if final:
        out_shape = jax.ShapeDtypeStruct((depth * tensor_parts, own + STAT_ROWS, width), bf16)
        out_specs = vm
    else:
        out_shape = [jax.ShapeDtypeStruct(s, t) for s, t in state_shapes]
        out_specs = [vm, vm]
    args = [where, table, *queries, *chunks] + ([] if fresh else list(state))
    return pl.pallas_call(
        body,
        in_specs=[sm, sm] + [vm] * (len(args) - 2),
        out_specs=out_specs,
        scratch_shapes=scratch,
        out_shape=out_shape,
        compiler_params=pltpu.CompilerParams(vmem_limit_bytes=30 * 2**20),
        cost_estimate=cost_of(cost),
    )(*args)


def mix_rows(place, arrived, mixers, residual, gain):
    own, wide = residual.shape
    width = arrived.shape[2]
    cores = 2
    turns = arrived.shape[0] // 4 // cores
    parts = turns * cores

    def body(place_ref, arrived_ref, *refs):
        mixer_refs = refs[: len(mixers)]
        residual_ref, gain_ref, out_ref, acc = refs[len(mixers) :]
        lane = lax.broadcasted_iota(jnp.int32, (own, width), 1)

        def level(index):
            pieces = arrived_ref[index, own:].astype(f32)
            line = pieces[0:1] + pieces[1:2] + pieces[2:3]
            return jnp.broadcast_to(line, (8, width)).T[:own, 0:1]

        def rows_of(part):
            second = pltpu.roll(arrived_ref[3 * parts + part, :own].astype(f32), width // 2, 1)
            small = jnp.where(lane < width // 2, arrived_ref[2 * parts + part, :own].astype(f32), second)
            share = 1.0 / (1.0 + jnp.exp2(level(part) - level(parts + part)))
            large = arrived_ref[part, :own].astype(f32) * (1.0 - share) + arrived_ref[
                parts + part, :own
            ].astype(f32) * share
            return small.astype(bf16), large.astype(bf16)

        acc[...] = residual_ref[...].astype(f32) * residual_scale
        for ref, (_, shift, other) in zip(mixer_refs, mixers):
            y = lax.rem(place_ref[0] + shift + turns, turns)
            core = place_ref[1] if other == 0 else 1 - place_ref[1]
            both = rows_of(y * cores + core)
            acc[...] += jnp.dot(jnp.concatenate(both, axis=1), ref[...], preferred_element_type=f32)
        values = acc[...]
        center = jnp.mean(values, axis=-1, keepdims=True)
        values = values - center
        spread = jnp.mean(jnp.square(values), axis=-1, keepdims=True)
        out_ref[...] = (values * lax.rsqrt(spread + epsilon) * gain_ref[...]).astype(bf16)

    vm = pl.BlockSpec(memory_space=pltpu.VMEM)
    return pl.pallas_call(
        body,
        in_specs=[pl.BlockSpec(memory_space=pltpu.SMEM)] + [vm] * (len(mixers) + 3),
        out_specs=vm,
        scratch_shapes=[pltpu.VMEM((own, wide), f32)],
        out_shape=jax.ShapeDtypeStruct((own, wide), bf16),
        compiler_params=pltpu.CompilerParams(vmem_limit_bytes=24 * 2**20),
        cost_estimate=cost_of(5.0),
    )(place, arrived, *[m[0] for m in mixers], residual, gain.reshape(1, wide))


BLOCK = 768
LEAD = 16


def pack_weights(value_weight, gate_weight, down_weight):
    width, rows = value_weight.shape

    def body(v, g, d, out):
        for k, part in enumerate((v, g, d)):
            out[:, k * BLOCK : k * BLOCK + width] = part[...].T
            out[:, k * BLOCK + width : (k + 1) * BLOCK] = jnp.zeros((rows, BLOCK - width), bf16)

    vm = pl.BlockSpec(memory_space=pltpu.VMEM)
    return pl.pallas_call(
        body,
        in_specs=[vm] * 3,
        out_specs=vm,
        out_shape=jax.ShapeDtypeStruct((rows, 3 * BLOCK), bf16),
        cost_estimate=cost_of(1.5),
    )(value_weight, gate_weight, down_weight)


def window(array, k):
    return pl.BlockSpec((array.shape[0], BLOCK), lambda i: (0, k))


def whole(array):
    return pl.BlockSpec(array.shape, lambda i: (0,) * array.ndim)


def ups(chunks, weights, width, cost, earlier=(), place=None, spots=(), turns=0, cores=0):
    rows = sum(c.shape[0] for c in chunks)
    own = chunks[0].shape[0] * len(chunks) // 2 if earlier else 0
    flat = [a for pair in earlier for a in pair]

    def body(*refs):
        place_ref, chunk_refs = refs[0], refs[1 : 1 + len(chunks)]
        value_ref, gate_ref = refs[1 + len(chunks) : 3 + len(chunks)]
        done = refs[3 + len(chunks) : 3 + len(chunks) + len(flat)]
        outs = refs[3 + len(chunks) + len(flat) :]
        x = jnp.concatenate([r[...] for r in chunk_refs], axis=0)
        for ref, out in ((value_ref, outs[0]), (gate_ref, outs[1])):
            out[...] = jnp.dot(x, ref[:, :width], preferred_element_type=f32).astype(bf16)
        if not earlier:
            return
        tails, leaving = outs[2:4], outs[4]
        pieces = (*done, *outs[:2])
        spot = 0
        for k in range(0, len(pieces), 2):
            for i in range(pieces[k].shape[0] // own):
                shift, other = spots[spot]
                spot += 1
                y = lax.rem(place_ref[0] + shift + turns, turns)
                core = place_ref[1] if other == 0 else 1 - place_ref[1]
                for side in range(2):
                    tails[side][y * cores + core] = pieces[k + side][(i + 1) * own - LEAD : (i + 1) * own]
        for side in range(2):
            leaving[side * LEAD : (side + 1) * LEAD] = tails[side][turns * cores - 1]

    shapes = [jax.ShapeDtypeStruct((rows, width), bf16)] * 2
    if earlier:
        shapes += [jax.ShapeDtypeStruct((turns * cores, LEAD, width), bf16)] * 2
        shapes.append(jax.ShapeDtypeStruct((2 * LEAD, width), bf16))
    return pl.pallas_call(
        body,
        grid=(1,),
        in_specs=[pl.BlockSpec(memory_space=pltpu.SMEM)]
        + [whole(c) for c in chunks]
        + [window(weights, 0), window(weights, 1)]
        + [whole(a) for a in flat],
        out_specs=[whole(x) for x in shapes],
        out_shape=shapes,
        compiler_params=pltpu.CompilerParams(vmem_limit_bytes=24 * 2**20),
        cost_estimate=cost_of(cost),
    )(place, *chunks, weights, weights, *flat)


def downs(place, pieces, groups, tails, halo, value_taps, gate_taps, weights, own, turns, cores, cost):
    width = pieces[0][0].shape[1]
    wide = weights.shape[0]
    count = len(groups)

    def body(place_ref, *refs):
        vt_ref, gt_ref, down_ref, halo_ref = refs[:4]
        tail_refs = refs[4:6]
        up_refs = refs[6 : 6 + 2 * len(pieces)]
        theirs, mine, hidden, terms = refs[6 + 2 * len(pieces) :]

        def filtered(ref, taps, tail, side, at, part):
            halo_rows = halo_ref[side * LEAD : (side + 1) * LEAD].astype(f32)
            before = tail[jnp.maximum(part - 1, 0)].astype(f32)
            before = jnp.where(part == 0, halo_rows, before)
            here = ref[pl.ds(pl.multiple_of(at * own, LEAD), own)].astype(f32)
            rows = jnp.concatenate([before, here], axis=0)
            two = pltpu.roll(rows, 2, 0)[LEAD:]
            one = pltpu.roll(rows, 1, 0)[LEAD:]
            return taps[0:1] * two + taps[1:2] * one + taps[2:3] * rows[LEAD:]

        @pl.loop(0, 2)
        def _(turn):
            core = jnp.where(turn == 0, 1 - place_ref[1], place_ref[1])
            for i, (piece, at_own, at_other, shift) in enumerate(groups):
                at = jnp.where(turn == 0, at_other, at_own)
                part = lax.rem(place_ref[0] + shift + turns, turns) * cores + core
                value = filtered(up_refs[2 * piece], vt_ref, tail_refs[0], 0, at, part)
                gate = filtered(up_refs[2 * piece + 1], gt_ref, tail_refs[1], 1, at, part)
                hidden[i * own : (i + 1) * own] = (gate / (1.0 + jnp.exp(-gate)) * value).astype(bf16)
            terms[...] = lax.dot_general(
                hidden[...],
                down_ref[:, :width],
                (((1,), (1,)), ((), ())),
                preferred_element_type=f32,
            )
            for own_turn, out in enumerate((theirs, mine)):

                @pl.when(turn == own_turn)
                def _():
                    @pl.loop(0, count)
                    def _(i):
                        out[i] = terms[pl.ds(pl.multiple_of(i * own, LEAD), own)].astype(out.dtype)

    shapes = [jax.ShapeDtypeStruct((count, own, wide), t) for t in (bf16, f32)]
    flat = [a for pair in pieces for a in pair]
    return pl.pallas_call(
        body,
        grid=(1,),
        in_specs=[pl.BlockSpec(memory_space=pltpu.SMEM), whole(value_taps), whole(gate_taps)]
        + [window(weights, 2), whole(halo), whole(tails[0]), whole(tails[1])]
        + [whole(a) for a in flat],
        out_specs=[whole(x) for x in shapes],
        out_shape=shapes,
        scratch_shapes=[
            pltpu.VMEM((count * own, width), bf16),
            pltpu.VMEM((count * own, wide), f32),
        ],
        compiler_params=pltpu.CompilerParams(vmem_limit_bytes=24 * 2**20),
        cost_estimate=cost_of(cost),
    )(place, value_taps, gate_taps, weights, halo, *tails, *flat)


def paired(mine, theirs, kinds):
    count, own, wide = mine.shape

    def body(mine_ref, their_ref, *outs):
        for i, out in enumerate(outs):
            out[...] = (mine_ref[i] + their_ref[i].astype(f32)).astype(out.dtype)

    vm = pl.BlockSpec(memory_space=pltpu.VMEM)
    return pl.pallas_call(
        body,
        in_specs=[vm] * 2,
        out_specs=[vm] * count,
        out_shape=[jax.ShapeDtypeStruct((own, wide), kind) for kind in kinds],
        cost_estimate=cost_of(0.7 * count),
    )(mine, theirs)


def finish(mixed, own, shares, gain):
    rows, wide = mixed.shape

    def body(*refs):
        mixed_ref, own_ref = refs[:2]
        gain_ref, out_ref = refs[-2:]
        total = own_ref[...]
        for r in refs[2:-2]:
            total = total + r[...].astype(f32)
        values = residual_scale * mixed_ref[...].astype(f32) + total
        center = jnp.mean(values, axis=-1, keepdims=True)
        values = values - center
        spread = jnp.mean(jnp.square(values), axis=-1, keepdims=True)
        out_ref[...] = (values * lax.rsqrt(spread + epsilon) * gain_ref[...]).astype(bf16)

    vm = pl.BlockSpec(memory_space=pltpu.VMEM)
    return pl.pallas_call(
        body,
        in_specs=[vm] * (3 + len(shares)),
        out_specs=vm,
        out_shape=jax.ShapeDtypeStruct((rows, wide), bf16),
        cost_estimate=cost_of(2.0),
    )(mixed, own, *shares, gain.reshape(1, wide))


def per_device(
    query_small,
    key_small,
    value_small,
    gates_small,
    query_large,
    key_large,
    value_large,
    gates_large,
    residual,
    mixer_small,
    mixer_large,
    mix_gain,
    value_weight,
    gate_weight,
    value_taps,
    gate_taps,
    down_weight,
    final_gain,
):
    slot = lax.axis_index("sp_z").astype(jnp.int32)
    column = lax.axis_index("sp_x").astype(jnp.int32)
    depth, turns = lax.axis_size("sp_z"), lax.axis_size("sp_x")
    packed, *asked = pack(
        slot.reshape(1),
        key_small,
        value_small,
        key_large,
        value_large,
        query_small,
        query_large,
        gates_small.T,
        gates_large.T,
    )
    packed, value_turned, gate_turned, down_turned = lax.optimization_barrier(
        (packed, value_weight.T, gate_weight.T, down_weight)
    )
    pairs = lax.all_to_all(packed, "sp_z", split_axis=0, concat_axis=0, tiled=True)
    shards = pack_weights(value_turned, gate_turned, down_turned)
    pairs, shards, asked = lax.optimization_barrier((pairs, shards, asked))
    weights = lax.all_gather(shards, SP, axis=0, tiled=True)
    before = shifted(pairs, "sp_x", 1)
    after = shifted(pairs, "sp_x", -1)
    queries = [asked[0]] + [shifted(asked[k], "sp_z", k) for k in range(1, depth)]
    mixer = jnp.concatenate([mixer_small, mixer_large], axis=0)
    mixers = [mixer]
    for k in (1, -1, 2):
        mixers.append(shifted(mixer, "tp_y", k))
    calls = ((0,), (-1, 1), (2,))
    tables = work_tables(calls, depth, turns)
    place_here = jnp.stack([slot, column])
    call = lambda k, chunks, state: attend(
        place_here,
        jnp.asarray(tables[k]),
        queries,
        chunks,
        state,
        k + 1 == len(calls),
        lax.axis_size(TP),
        0 in calls[k],
        12.0 * len(calls[k]),
    )
    state = call(0, [pairs], None)
    pairs, before, after, state = lax.optimization_barrier((pairs, before, after, state))
    far = shifted(pairs, "sp_x", 2)
    state = call(1, [before, after], state)
    far_mixer = mixers.pop()
    far, state, mixers = lax.optimization_barrier((far, state, mixers))
    crossed = [shifted(a, "tp_c", 1) for a in mixers]
    state = call(2, [far], state)
    arrived = lax.all_to_all(state, ("sp_z",) + TP, split_axis=0, concat_axis=0, tiled=True)
    crossed.append(shifted(far_mixer, "tp_c", 1))
    shifts = (0, -1, 1, 2)
    mixers = [(a, k, 0) for a, k in zip(mixers + [far_mixer], shifts)]
    mixers += [(a, k, 1) for a, k in zip(crossed, shifts)]
    place = jnp.stack([lax.axis_index("tp_y"), lax.axis_index("tp_c")]).astype(jnp.int32)
    mixed = mix_rows(place, arrived, mixers, residual, mix_gain)
    turns_y, cores = lax.axis_size("tp_y"), lax.axis_size("tp_c")
    own_rows = mixed.shape[0]
    half = own_rows // 2
    width = value_weight.shape[1]
    spots = [(0, 0), (0, 1), (-1, 0), (1, 0), (-1, 1), (1, 1), (2, 0), (2, 1)]
    last_one, next_one = shifted(mixed, "tp_y", 1), shifted(mixed, "tp_y", -1)
    near = ups([mixed, shifted(mixed, "tp_c", 1)], weights, width, 3.0, place=place)
    opposite = [shifted(last_one[:half], "tp_y", 1), shifted(next_one[half:], "tp_y", -1)]
    beside = [last_one, next_one] + [shifted(a, "tp_c", 1) for a in (last_one, next_one)]
    beside = ups(beside, weights, width, 4.0, place=place)
    beside, opposite = lax.optimization_barrier((beside, opposite))
    opposite += [shifted(a, "tp_c", 1) for a in opposite]
    up_value, up_gate, *tails, leaving = ups(
        opposite, weights, width, 3.0, (near, beside), place, spots, turns_y, cores
    )
    opposite = [up_value, up_gate]
    halo = passed_along(leaving, SP, 1)
    down = lambda chosen, groups, cost: downs(
        place,
        chosen,
        groups,
        tails,
        halo,
        value_taps,
        gate_taps,
        weights,
        own_rows,
        turns_y,
        cores,
        cost,
    )
    theirs, mine = down([beside, opposite], [(0, 0, 2, -1), (0, 1, 3, 1), (1, 0, 1, 2)], 8.0)
    sums = paired(mine, shifted(theirs, "tp_c", 1), [bf16] * 3)
    near, sums = lax.optimization_barrier((near, sums))
    shares = []
    for part, steps in zip(sums, (-1, 1, 2)):
        shares.append(shifted(part, "tp_y", steps))
    theirs, mine = down([near], [(0, 0, 1, 0)], 4.0)
    (own,) = paired(mine, shifted(theirs, "tp_c", 1), [f32])
    return finish(mixed, own, shares, final_gain)


def solution(mesh):
    split = Mesh(mesh.devices.reshape(4, 4, 4, 2), ALL)
    placed = (P(SP, TP),) * 8 + (
        P(ALL, None),
        P(TP, None),
        P(TP, None),
        P(),
        P(SP, TP),
        P(SP, TP),
        P(None, TP),
        P(None, TP),
        P(TP, SP),
        P(),
    )

    return jax.shard_map(per_device, mesh=split, in_specs=placed, out_specs=P(ALL, None), check_vma=False)
```
